512 devices in a mesh: sp: 128 (over z, x, core), tp: 4 (over y).
Axes of the slice: x: 4, y: 4, z: 16, core: 2. Of those that a mesh axis runs over, the one named last changes fastest.
Arguments:
- tokens: bfloat16 [16384, 2048], P('sp', 'tp'), may hold values from -6 to 6
- conv_value_weight: bfloat16 [2048, 1024], P('sp', 'tp'), may hold values from -0.125 to 0.125
- conv_gate_weight: bfloat16 [2048, 1024], P('sp', 'tp'), may hold values from -0.125 to 0.125
- conv_kernel: bfloat16 [31, 1024], P(None, 'tp'), may hold values from -16 to 16
- conv_norm_gain: float32 [1024], P('tp'), may hold values from 0.1 to 1.9
- query_weight: bfloat16 [2048, 2048], P('sp', 'tp'), may hold values from -0.125 to 0.125
- key_weight: bfloat16 [2048, 2048], P('sp', 'tp'), may hold values from -0.125 to 0.125
- value_weight: bfloat16 [2048, 2048], P('sp', 'tp'), may hold values from -0.125 to 0.125
- input_gate_weight: bfloat16 [2048, 8], P(None, 'tp'), may hold values from -0.125 to 0.125
- forget_gate_weight: bfloat16 [2048, 8], P(None, 'tp'), may hold values from -0.125 to 0.125
- input_offset: float32 [16384, 8], P('sp', 'tp'), may hold values from -4 to 210
- forget_offset: float32 [16384, 8], P('sp', 'tp'), may hold values from 0 to 30
- memory_norm_gain: float32 [2048], P('tp'), may hold values from 0.1 to 1.9
- conv_out_weight: bfloat16 [1024, 2048], P('tp', 'sp'), may hold values from -0.3125 to 0.3125
- memory_out_weight: bfloat16 [2048, 2048], P('tp', 'sp'), may hold values from -0.125 to 0.125
Outputs:
- mixed: bfloat16 [16384, 2048], P('sp', 'tp')
The draws below stay inside these ranges and needn't reach their ends.
All inputs are finite; a program needn't handle non-finite values.
Results may differ from the reference program's by a relative error of at most 0.03.
Values may be sent and summed in bfloat16 or wider, within the bound.
No kernel may reach another device: no remote copies, remote signals or barrier semaphores. Data moves between devices by JAX's collectives and lax.ppermute only.
A program may use at most 128 MiB of HBM per device.

```python
import jax
import jax.numpy as jnp
from jax import lax

D = 2048
CONV = 1024
MEMORY_HEADS = 8
HEAD_DIM = 256
KERNEL = 31
BLOCK = 64
TOK_DEV = 128
SEQUENCE_TOKENS = 16384
GROUPS = 4


def draw_conv_kernel(key, part):
    key_rows = jax.random.split(jax.random.fold_in(key, 101), 2)
    channel = jnp.arange(CONV, dtype=jnp.float32) / CONV
    entries = jnp.clip(jax.random.normal(key_rows[0], (KERNEL, CONV), jnp.float32), -4.0, 4.0)
    rise = jnp.power(10.0, channel)
    factor = jnp.exp(jax.random.uniform(key_rows[1], (CONV,), jnp.float32, -0.35, 0.35))
    return (entries * rise * factor / jnp.sqrt(jnp.float32(KERNEL))).astype(jnp.bfloat16)


def draw_input_offset(key, part):
    key_rows = jax.random.split(jax.random.fold_in(key, 202), 1)
    position_offset = jnp.clip(jax.random.normal(key_rows[0], (SEQUENCE_TOKENS, MEMORY_HEADS), jnp.float32), -4.0, 4.0)
    return position_offset.astype(jnp.float32)


def draw_forget_offset(key, part):
    key_rows = jax.random.split(jax.random.fold_in(key, 303), 6)
    slow_head = jax.random.uniform(key_rows[0], (MEMORY_HEADS,)) < 0.5
    slow_level = jnp.log(jnp.float32(SEQUENCE_TOKENS)) + 3.0
    fast_level = jax.random.uniform(key_rows[1], (MEMORY_HEADS,), jnp.float32, 3.4, 4.6)
    level = jnp.where(slow_head, slow_level, fast_level)
    devices = SEQUENCE_TOKENS // TOK_DEV
    device_shift = jax.random.uniform(key_rows[2], (devices, 1, MEMORY_HEADS), jnp.float32, -0.7, 0.7)
    rough = 0.3 * jnp.clip(jax.random.normal(key_rows[3], (devices, TOK_DEV, MEMORY_HEADS), jnp.float32), -4.0, 4.0)
    position_offset = (level + device_shift + rough).reshape(SEQUENCE_TOKENS, MEMORY_HEADS)
    group_rows = jax.random.randint(key_rows[4], (3,), 0, SEQUENCE_TOKENS)
    token_positions = jnp.arange(SEQUENCE_TOKENS)
    token_group = jnp.any(token_positions[:, None] == group_rows[None, :], axis=1)
    group_level = jax.random.uniform(key_rows[5], (SEQUENCE_TOKENS, MEMORY_HEADS), jnp.float32, 0.9, 1.6)
    return jnp.where(token_group[:, None], group_level, position_offset).astype(jnp.float32)


def block_levels(key, dims, cuts, least, largest):
    level, own = 1.0, jax.random.fold_in(key, 6)
    for position, parts in cuts:
        draws = jnp.exp(jax.random.uniform(jax.random.fold_in(own, position), (parts,), jnp.float32, least / len(cuts), largest / len(cuts)))
        level = level * jnp.repeat(draws, dims[position] // parts).reshape([-1 if axis == position else 1 for axis in range(len(dims))])
    return level


def centred(stream_key, dims, width, limit, cuts=(), kind=jnp.bfloat16):
    drawn = width * jax.random.normal(stream_key, dims, jnp.float32)
    if cuts:
        drawn = drawn * block_levels(stream_key, dims, cuts, -0.22, 0.18)
    return jnp.clip(drawn, -limit, limit).astype(kind)


def setup_inputs(seed: int = 0) -> dict:
    keys = jax.random.split(jax.random.key(seed), 16)
    tokens = centred(keys[0], (SEQUENCE_TOKENS, D), 1.0, 6.0, ((0, 128), (1, 4)))
    conv_value_weight = centred(keys[1], (D, CONV), D ** -0.5, 0.125, ((0, 128), (1, 4)))
    conv_gate_weight = centred(keys[2], (D, CONV), D ** -0.5, 0.125, ((0, 128), (1, 4)))
    conv_kernel = draw_conv_kernel(jax.random.fold_in(keys[15], 71), 0)
    conv_norm_gain = jnp.clip(1.0 + 0.18 * jax.random.normal(keys[4], (CONV,), jnp.float32), 0.1, 1.9)
    query_weight = centred(keys[5], (D, MEMORY_HEADS * HEAD_DIM), D ** -0.5, 0.125, ((0, 128), (1, 4)))
    key_weight = centred(keys[6], (D, MEMORY_HEADS * HEAD_DIM), D ** -0.5, 0.125, ((0, 128), (1, 4)))
    value_weight = centred(keys[7], (D, MEMORY_HEADS * HEAD_DIM), D ** -0.5, 0.125, ((0, 128), (1, 4)))
    input_gate_weight = centred(keys[8], (D, MEMORY_HEADS), D ** -0.5, 0.125, ((1, 4),))
    forget_gate_weight = centred(keys[9], (D, MEMORY_HEADS), D ** -0.5, 0.125, ((1, 4),))
    input_offset = draw_input_offset(jax.random.fold_in(keys[15], 71), 0)
    forget_offset = draw_forget_offset(jax.random.fold_in(keys[15], 71), 0)
    memory_norm_gain = jnp.clip(1.0 + 0.18 * jax.random.normal(keys[12], (MEMORY_HEADS * HEAD_DIM,), jnp.float32), 0.1, 1.9)
    conv_out_weight = centred(keys[13], (CONV, D), (CONV // 3) ** -0.5, 0.3125, ((0, 4), (1, 128)))
    memory_out_weight = centred(keys[14], (MEMORY_HEADS * HEAD_DIM, D), (MEMORY_HEADS * HEAD_DIM) ** -0.5, 0.125, ((0, 4), (1, 128)))
    return {"tokens": tokens, "conv_value_weight": conv_value_weight, "conv_gate_weight": conv_gate_weight, "conv_kernel": conv_kernel, "conv_norm_gain": conv_norm_gain, "query_weight": query_weight, "key_weight": key_weight, "value_weight": value_weight, "input_gate_weight": input_gate_weight, "forget_gate_weight": forget_gate_weight, "input_offset": input_offset, "forget_offset": forget_offset, "memory_norm_gain": memory_norm_gain, "conv_out_weight": conv_out_weight, "memory_out_weight": memory_out_weight}


EPS = 1e-06

def block_step(carry, inputs):
    state, normal, level = carry
    query, key, value, gate_in, forget_log = inputs
    length = gate_in.shape[-1]
    scale = query.shape[-1] ** (-0.5)
    causal = jnp.tril(jnp.ones((length, length), dtype=bool))
    within = jnp.cumsum(forget_log, axis=-1)
    log_weight = within[:, :, None] - within[:, None, :] + gate_in[:, None, :]
    log_weight = jnp.where(causal, log_weight, -jnp.inf)
    carried = within + level[:, None]
    top = jnp.maximum(carried, lax.optimization_barrier(jnp.max(log_weight, axis=-1)))
    weight = jnp.exp(log_weight - top[:, :, None])
    carried_weight = jnp.exp(carried - top) * scale
    scores = jnp.einsum('htd,hsd->hts', query, key, preferred_element_type=jnp.float32) * (scale * weight)
    numer = jnp.einsum('hts,hse->hte', scores.astype(jnp.bfloat16), value, preferred_element_type=jnp.float32)
    numer = numer + carried_weight[:, :, None] * jnp.einsum('hed,htd->hte', state.astype(jnp.bfloat16), query, preferred_element_type=jnp.float32)
    denom = lax.optimization_barrier(jnp.sum(scores, axis=-1)) + carried_weight * jnp.einsum('hd,htd->ht', normal.astype(jnp.bfloat16), query, preferred_element_type=jnp.float32)
    result = numer / jnp.maximum(jnp.abs(denom), 1.0)[:, :, None]
    last = within[:, -1]
    end_log = last[:, None] - within + gate_in
    new_level = jnp.maximum(last + level, lax.optimization_barrier(jnp.max(end_log, axis=-1)))
    keep = jnp.exp(last + level - new_level)
    fresh = jnp.exp(end_log - new_level[:, None])
    scaled_key = (fresh[:, :, None] * key).astype(jnp.bfloat16)
    new_state = keep[:, None, None] * state + jnp.einsum('hse,hsd->hed', value, scaled_key, preferred_element_type=jnp.float32)
    new_normal = keep[:, None] * normal + lax.optimization_barrier(jnp.sum(scaled_key.astype(jnp.float32), axis=1))
    return ((new_state, new_normal, new_level), result)

def depthwise(extended, kernel):
    taps = kernel.shape[0]
    length = extended.shape[0] - taps + 1
    total = extended[0:length] * kernel[0]
    for index in range(1, taps):
        total = total + extended[index:index + length] * kernel[index]
    return total

def reference(tokens, conv_value_weight, conv_gate_weight, conv_kernel, conv_norm_gain, query_weight, key_weight, value_weight, input_gate_weight, forget_gate_weight, input_offset, forget_offset, memory_norm_gain, conv_out_weight, memory_out_weight):

    def project(weight):
        return jnp.dot(tokens, weight, preferred_element_type=jnp.float32)
    glu = (project(conv_value_weight) * jax.nn.sigmoid(project(conv_gate_weight))).astype(jnp.bfloat16)
    extended = jnp.concatenate([jnp.zeros((KERNEL - 1, CONV), jnp.float32), glu.astype(jnp.float32)], axis=0)
    conv = depthwise(extended, conv_kernel.astype(jnp.float32))
    mean = lax.optimization_barrier(jnp.mean(conv, axis=1, keepdims=True))
    variance = lax.optimization_barrier(jnp.mean(conv * conv, axis=1, keepdims=True)) - mean * mean
    conv_branch = jax.nn.silu((conv - mean) * lax.rsqrt(variance + EPS) * conv_norm_gain).astype(jnp.bfloat16)

    def to_heads(weight):
        return project(weight).astype(jnp.bfloat16).reshape(SEQUENCE_TOKENS, MEMORY_HEADS, HEAD_DIM).transpose(1, 0, 2)
    query = to_heads(query_weight)
    key = to_heads(key_weight)
    value = to_heads(value_weight)
    gate_in = (project(input_gate_weight) + input_offset).T
    forget_log = jax.nn.log_sigmoid(project(forget_gate_weight) + forget_offset).T
    blocks = SEQUENCE_TOKENS // BLOCK

    def split(array):
        return jnp.moveaxis(array.reshape((MEMORY_HEADS, blocks, BLOCK) + array.shape[2:]), 1, 0)
    start_state = (jnp.zeros((MEMORY_HEADS, HEAD_DIM, HEAD_DIM), jnp.float32), jnp.zeros((MEMORY_HEADS, HEAD_DIM), jnp.float32), jnp.full((MEMORY_HEADS,), -1e+30, jnp.float32))
    _, hidden = lax.scan(block_step, start_state, (split(query), split(key), split(value), split(gate_in), split(forget_log)))
    hidden = jnp.moveaxis(hidden, 0, 1).reshape(MEMORY_HEADS, SEQUENCE_TOKENS, HEAD_DIM)
    hidden = hidden * lax.rsqrt(lax.optimization_barrier(jnp.mean(hidden * hidden, axis=(0, 2), keepdims=True)) + EPS)
    hidden = hidden * memory_norm_gain.reshape(MEMORY_HEADS, 1, HEAD_DIM)
    memory_branch = hidden.transpose(1, 0, 2).reshape(SEQUENCE_TOKENS, MEMORY_HEADS * HEAD_DIM).astype(jnp.bfloat16)
    conv_share = CONV // GROUPS
    memory_share = MEMORY_HEADS * HEAD_DIM // GROUPS
    mixed = jnp.zeros((SEQUENCE_TOKENS, D), jnp.float32)
    for group in range(GROUPS):
        conv_rows = slice(group * conv_share, (group + 1) * conv_share)
        memory_rows = slice(group * memory_share, (group + 1) * memory_share)
        partial_value = jnp.dot(conv_branch[:, conv_rows], conv_out_weight[conv_rows], preferred_element_type=jnp.float32)
        partial_value = partial_value + jnp.dot(memory_branch[:, memory_rows], memory_out_weight[memory_rows], preferred_element_type=jnp.float32)
        rounded = lax.optimization_barrier(partial_value.astype(jnp.bfloat16))
        mixed = mixed + rounded.astype(jnp.float32)
    return mixed.astype(jnp.bfloat16)
```

```python
import jax
import jax.numpy as jnp
from jax import lax
from jax.experimental import pallas as pl
from jax.experimental.pallas import tpu as pltpu
from jax.sharding import Mesh
from jax.sharding import PartitionSpec as P

AXES = ("zh", "zl", "x", "c", "tp")
Z = ("zh", "zl")
SP = ("zh", "zl", "x", "c")
EPS = 1e-06
LOW = -1e30
F32 = jnp.float32
BF16 = jnp.bfloat16
INTERPRET = False


def size(axis):
    return lax.axis_size(axis)


def exchange(pieces, axes):
    return lax.all_to_all(pieces, axes, split_axis=0, concat_axis=0, tiled=True)


def copies(shard, axes):
    return exchange(jnp.broadcast_to(shard, (lax.axis_size(axes), *shard.shape)), axes)


def swapped(value, axis):
    return lax.ppermute(value, axis, [(0, 1), (1, 0)])


def three(value):
    high = lax.reduce_precision(value, 8, 7)
    rest = value - high
    mid = lax.reduce_precision(rest, 8, 7)
    return high.astype(BF16), mid.astype(BF16), (rest - mid).astype(BF16)


def lane_cumsum(rows):
    lane = lax.broadcasted_iota(jnp.int32, rows.shape, 1)
    step = 1
    while step < rows.shape[1]:
        moved = pltpu.roll(rows, step, 1)
        rows = rows + jnp.where(lane >= step, moved, 0.0)
        step *= 2
    return rows


def columns_of(rows):
    count, length = rows.shape
    square = jnp.concatenate([rows, jnp.zeros((length - count, length), F32)], axis=0)
    return square.T


def dot(a, b, dims):
    return lax.dot_general(a, b, (dims, ((), ())), preferred_element_type=F32)


NN = ((1,), (0,))
NT = ((1,), (1,))
TN = ((0,), (0,))


def joined(parts_ref, start, width, chunk, length):
    picked = [
        parts_ref[j, chunk * length : (chunk + 1) * length, start : start + width]
        for j in range(parts_ref.shape[0])
    ]
    return jnp.concatenate(picked, axis=1)


def slab_kernel(qk_ref, v_ref, gate_ref, out_ref, q_ref, k_ref):
    chunks, length = gate_ref.shape[1], gate_ref.shape[2]
    width = qk_ref.shape[2] // 2
    gate, forget = gate_ref[0], gate_ref[1]
    within = lane_cumsum(forget)
    ends = [within[r : r + 1, length - 1 :] for r in range(chunks)]
    after = [jnp.zeros((1, 1), F32)]
    for r in range(chunks - 1, 0, -1):
        after.insert(0, after[0] + ends[r])
    total = after[0] + ends[0]
    to_end = jnp.concatenate([e + a for e, a in zip(ends, after)], axis=0)
    end_log = to_end - within + gate
    level = jnp.max(jnp.max(end_log, axis=1, keepdims=True), axis=0, keepdims=True)
    fresh = columns_of(jnp.exp(end_log - level))
    state = jnp.zeros((2 * width, width * qk_ref.shape[0]), F32)
    for r in range(chunks):
        q_ref[r * length : (r + 1) * length] = joined(qk_ref, 0, width, r, length)
        key = joined(qk_ref, width, width, r, length)
        k_ref[r * length : (r + 1) * length] = key
        scaled = (fresh[:, r : r + 1] * key.astype(F32)).astype(BF16)
        state = state + dot(v_ref[r * length : (r + 1) * length], scaled, TN)
    rows = out_ref.shape[0]
    kept = state[:rows]
    row = lax.broadcasted_iota(jnp.int32, kept.shape, 0)
    lane = lax.broadcasted_iota(jnp.int32, kept.shape, 1)
    for at, value in ((0, level), (3, total)):
        high = value.astype(BF16).astype(F32)
        mid = (value - high).astype(BF16).astype(F32)
        low = value - high - mid
        for k, part in enumerate((high, mid, low)):
            kept = jnp.where((row == width + 1) & (lane == at + k), part, kept)
    out_ref[...] = kept.astype(BF16)


def cell_kernel(place_ref, in_ref, q_ref, k_ref, v_ref, gate_ref, out_ref):
    chunks, length = gate_ref.shape[1], gate_ref.shape[2]
    members, rows, head = in_ref.shape
    width = out_ref.shape[1]
    scale = head ** (-0.5)
    place = place_ref[0]
    acc = jnp.zeros((1, 1), F32)
    logs = [None] * members
    for j in range(members - 1, -1, -1):
        line = in_ref[j, width + 1 : width + 2, :128].astype(F32)
        level_j = line[:, 0:1] + line[:, 1:2] + line[:, 2:3]
        total_j = line[:, 3:4] + line[:, 4:5] + line[:, 5:6]
        before = j < place
        logs[j] = jnp.where(before, level_j + acc, LOW)
        acc = acc + jnp.where(before, total_j, 0.0)
    level = logs[0]
    for j in range(1, members):
        level = jnp.maximum(level, logs[j])
    state = jnp.zeros((rows, head), F32)
    for j in range(members):
        weight = jnp.where(j < place, jnp.exp(logs[j] - level), 0.0)
        state = state + weight * in_ref[j].astype(F32)
    state = jnp.concatenate([state, jnp.zeros((2 * width - rows, head), F32)], axis=0)
    gate, forget = gate_ref[0], gate_ref[1]
    within = lane_cumsum(forget)
    turned = columns_of(jnp.concatenate([within, gate], axis=0))
    causal = lax.broadcasted_iota(jnp.int32, (length, length), 0) >= lax.broadcasted_iota(
        jnp.int32, (length, length), 1
    )
    for r in range(chunks):
        here = slice(r * length, (r + 1) * length)
        query, key, value = q_ref[here], k_ref[here], v_ref[here]
        within_row, gate_row = within[r : r + 1], gate[r : r + 1]
        within_col = turned[:, r : r + 1]
        gate_col = turned[:, chunks + r : chunks + r + 1]
        log_weight = jnp.where(causal, within_col - within_row + gate_row, -jnp.inf)
        carried = within_col + level
        top = jnp.maximum(carried, jnp.max(log_weight, axis=1, keepdims=True))
        weight = jnp.exp(log_weight - top)
        carried_weight = jnp.exp(carried - top) * scale
        scores = dot(query, key, NT) * (scale * weight)
        older = dot(query, state.astype(BF16), NT)
        numer = dot(scores.astype(BF16), value, NN) + carried_weight * older
        denom = jnp.sum(scores, axis=1, keepdims=True) + carried_weight * older[:, width : width + 1]
        result = numer[:, :width] / jnp.maximum(jnp.abs(denom), 1.0)
        out_ref[here] = result.astype(BF16)
        last = within_row[:, length - 1 :]
        end_row = last - within_row + gate_row
        new_level = jnp.maximum(last + level, jnp.max(end_row, axis=1, keepdims=True))
        keep = jnp.exp(last + level - new_level)
        fresh = jnp.exp(last - within_col + gate_col - new_level)
        scaled = (fresh * key.astype(F32)).astype(BF16)
        state = keep * state + dot(value, scaled, TN)
        level = new_level


def vmem(count):
    return [pl.BlockSpec(memory_space=pltpu.VMEM)] * count


def depthwise(extended, kernel):
    taps = kernel.shape[0]
    length = extended.shape[0] - taps + 1
    total = extended[0:length] * kernel[0]
    for index in range(1, taps):
        total = total + extended[index : index + length] * kernel[index]
    return total


def on_device(
    tokens,
    conv_value_weight,
    conv_gate_weight,
    conv_kernel,
    conv_norm_gain,
    query_weight,
    key_weight,
    value_weight,
    input_gate_weight,
    forget_gate_weight,
    input_offset,
    forget_offset,
    memory_norm_gain,
    conv_out_weight,
    memory_out_weight,
):
    nzh, nzl, nx, nc, ny = (size(a) for a in AXES)
    xi, ci = lax.axis_index("x"), lax.axis_index("c")
    length, part = tokens.shape
    slab = length * nx * nc
    head = query_weight.shape[1] // nc
    width = head // nx
    chan = conv_value_weight.shape[1] // nc // nx
    rows = query_weight.shape[0]
    features = part * ny

    out_rows = jnp.concatenate([memory_out_weight, conv_out_weight], axis=0).T
    turned = lax.ppermute(
        out_rows, ("zh", "tp"), [(a * ny + b, b * ny + a) for a in range(nzh) for b in range(ny)]
    )
    out_weight = lax.all_gather(turned, SP, axis=0, tiled=True).reshape(ny, part, -1)

    def cut(weight, each):
        return weight.reshape(rows, nc, nx, each)

    pieces = jnp.concatenate(
        [cut(w, width) for w in (query_weight, key_weight, value_weight)]
        + [cut(w, chan) for w in (conv_value_weight, conv_gate_weight)],
        axis=3,
    )
    wide = pieces.shape[3]
    pieces = pieces.transpose(2, 1, 0, 3).reshape(nx * nc, rows, wide)
    mine = exchange(pieces, ("x", "c")).reshape(nx * nc * rows, wide)
    mine = copies(mine, "zh").reshape(nzh, nx * nc * rows, wide)
    whole = copies(mine, "zl").reshape(nzl, nzh, nx * nc * rows, wide)
    weight = whole.transpose(1, 0, 2, 3).reshape(features, wide)

    extra = jnp.concatenate(
        [input_offset.T.reshape(-1), forget_offset.T.reshape(-1), conv_norm_gain, memory_norm_gain]
    )
    extra = jnp.concatenate(three(extra))
    extra_rows = -(-extra.shape[0] // part)
    extra_rows = -(-extra_rows // 8) * 8
    extra = jnp.pad(extra, (0, extra_rows * part - extra.shape[0])).reshape(extra_rows, part)
    sent = jnp.concatenate([tokens, extra], axis=0)
    own = copies(sent, ("x", "tp")).reshape(nx, ny, length + extra_rows, part)
    other = swapped(own, "c")
    first = ci == 0
    both = jnp.stack([jnp.where(first, own, other), jnp.where(first, other, own)], axis=1)
    slab_tokens = both[:, :, :, :length].transpose(0, 1, 3, 2, 4).reshape(slab, features)
    split_values = 4 * length + conv_norm_gain.shape[0] + memory_norm_gain.shape[0]
    extras = both[:, :, :, length:].reshape(nx, nc, ny, -1)[..., : 3 * split_values]
    extras = extras.reshape(nx, nc, ny, 3, split_values).astype(F32).sum(axis=3)
    gains = extras[0, 0, :, 4 * length :]
    conv_gain = gains[:, : conv_norm_gain.shape[0]].reshape(-1)
    memory_gain = gains[:, conv_norm_gain.shape[0] :].reshape(-1)
    yi = lax.axis_index("tp")
    offsets = lax.dynamic_index_in_dim(extras[..., : 4 * length], yi, 2, keepdims=False)
    offsets = offsets.reshape(nx * nc, 2, nc, length)
    offsets = lax.dynamic_index_in_dim(offsets, ci, 2, keepdims=False)

    projected = jnp.dot(slab_tokens, weight, preferred_element_type=F32)
    gate_weight = jnp.stack([input_gate_weight, forget_gate_weight], axis=0)
    gate_weight = lax.dynamic_index_in_dim(gate_weight, ci, 2, keepdims=False)
    gate_pre = lax.dot_general(
        gate_weight, slab_tokens, (((1,), (1,)), ((), ())), preferred_element_type=F32
    ).reshape(2, nx * nc, length)
    gates = jnp.stack(
        [gate_pre[0] + offsets[:, 0], jax.nn.log_sigmoid(gate_pre[1] + offsets[:, 1])], axis=0
    )
    qk = projected[:, : 2 * width].astype(BF16)
    value = projected[:, 2 * width : 3 * width].astype(BF16)
    lane = lax.broadcasted_iota(jnp.int32, (slab, width), 1)
    value = jnp.concatenate([value, jnp.where(lane == 0, 1.0, 0.0).astype(BF16)], axis=1)
    conv_value = projected[:, 3 * width : 3 * width + chan]
    conv_gate = projected[:, 3 * width + chan :]
    glu = (conv_value * jax.nn.sigmoid(conv_gate)).astype(BF16)

    taps = conv_kernel.shape[0]
    members = nzh * nzl
    prior = lax.ppermute(glu[slab - (taps - 1) :], Z, [(j, j + 1) for j in range(members - 1)])
    all_qk = copies(qk, "x")

    group = slab // nx
    packed = glu.reshape(nx, group, chan).transpose(1, 0, 2).reshape(group, nx * chan)
    lead = jnp.concatenate([prior, packed[group - (taps - 1) :, : (nx - 1) * chan]], axis=1)
    extended = jnp.concatenate([lead, packed], axis=0).astype(F32)
    own_kernel = lax.dynamic_slice_in_dim(conv_kernel, (ci * nx + xi) * chan, chan, 1).astype(F32)
    conv = depthwise(extended, jnp.tile(own_kernel, (1, nx)))
    conv_high = lax.reduce_precision(conv, 8, 7)
    conv_low = (conv - conv_high).astype(BF16).reshape(group, nx, chan)
    conv_high = conv_high.astype(BF16).reshape(group, nx, chan)
    conv_sent = jnp.concatenate([conv_high, conv_low], axis=2).transpose(1, 0, 2)

    state_rows = width + 8
    packed_state, query, key = pl.pallas_call(
        slab_kernel,
        out_shape=(
            jax.ShapeDtypeStruct((state_rows, head), BF16),
            jax.ShapeDtypeStruct((slab, head), BF16),
            jax.ShapeDtypeStruct((slab, head), BF16),
        ),
        in_specs=vmem(3),
        out_specs=vmem(3),
        interpret=INTERPRET,
        name="slab_state",
    )(all_qk.reshape(nx, slab, 2 * width), value, gates)
    states = copies(packed_state, Z).reshape(members, state_rows, head)
    place = (lax.axis_index("zh") * nzl + lax.axis_index("zl")).reshape(1)
    hidden = pl.pallas_call(
        cell_kernel,
        out_shape=jax.ShapeDtypeStruct((slab, width), BF16),
        in_specs=[pl.BlockSpec(memory_space=pltpu.SMEM)] + vmem(5),
        out_specs=pl.BlockSpec(memory_space=pltpu.VMEM),
        interpret=INTERPRET,
        name="cell",
    )(place, states, query, key, value, gates)

    last = jnp.concatenate([hidden.reshape(nx, group, width), conv_sent], axis=2)
    last = last.reshape(nx, nc, 1, length, width + 2 * chan)
    last = jnp.broadcast_to(last, (nx, nc, ny, length, width + 2 * chan))
    arrived = exchange(last.reshape(nx * nc * ny, length, -1), ("x", "c", "tp"))
    arrived = arrived.reshape(nx, nc, ny, length, -1).transpose(3, 2, 1, 0, 4)
    memory = arrived[..., :width].reshape(length, -1).astype(F32)
    conv = (
        arrived[..., width : width + chan].astype(F32) + arrived[..., width + chan :].astype(F32)
    ).reshape(length, -1)
    mean = jnp.mean(conv, axis=1, keepdims=True)
    variance = jnp.mean(conv * conv, axis=1, keepdims=True) - mean * mean
    conv_branch = jax.nn.silu((conv - mean) * lax.rsqrt(variance + EPS) * conv_gain).astype(BF16)
    memory_scale = lax.rsqrt(jnp.mean(memory * memory, axis=1, keepdims=True) + EPS)
    memory_branch = (memory * memory_scale * memory_gain).astype(BF16)
    heads_part = memory_out_weight.shape[0]
    total = jnp.zeros((length, part), F32)
    conv_part = conv_out_weight.shape[0]
    for b in range(ny):
        total = total + dot(
            memory_branch[:, b * heads_part : (b + 1) * heads_part], out_weight[b, :, :heads_part], NT
        )
        total = total + dot(
            conv_branch[:, b * conv_part : (b + 1) * conv_part], out_weight[b, :, heads_part:], NT
        )
    return total.astype(BF16)


def solution(mesh):
    shape = mesh.shape
    depth = shape["sp"] // 32
    split = Mesh(mesh.devices.reshape(4, depth, 4, 2, shape["tp"]), AXES)
    in_specs = (
        P(SP, "tp"),
        P(SP, "tp"),
        P(SP, "tp"),
        P(None, "tp"),
        P("tp"),
        P(SP, "tp"),
        P(SP, "tp"),
        P(SP, "tp"),
        P(None, "tp"),
        P(None, "tp"),
        P(SP, "tp"),
        P(SP, "tp"),
        P("tp"),
        P("tp", SP),
        P("tp", SP),
    )
    return jax.shard_map(
        on_device, mesh=split, in_specs=in_specs, out_specs=P(SP, "tp"), check_vma=False
    )
```

```python
import jax
import jax.numpy as jnp
from jax import lax
from jax.experimental import pallas as pl
from jax.experimental.pallas import tpu as pltpu
from jax.sharding import Mesh
from jax.sharding import PartitionSpec as P

AXES = ("zh", "zl", "x", "c", "tp")
Z = ("zh", "zl")
SP = ("zh", "zl", "x", "c")
EPS = 1e-06
LOW = -1e30
F32 = jnp.float32
BF16 = jnp.bfloat16
INTERPRET = False


def size(axis):
    return lax.axis_size(axis)


def exchange(pieces, axes):
    return lax.all_to_all(pieces, axes, split_axis=0, concat_axis=0, tiled=True)


def swapped(value, axis):
    return lax.ppermute(value, axis, [(0, 1), (1, 0)])


def lane_cumsum(rows):
    lane = lax.broadcasted_iota(jnp.int32, rows.shape, 1)
    step = 1
    while step < rows.shape[1]:
        moved = pltpu.roll(rows, step, 1)
        rows = rows + jnp.where(lane >= step, moved, 0.0)
        step *= 2
    return rows


def columns_of(rows):
    count, length = rows.shape
    square = jnp.concatenate([rows, jnp.zeros((length - count, length), F32)], axis=0)
    return square.T


def dot(a, b, dims):
    return lax.dot_general(a, b, (dims, ((), ())), preferred_element_type=F32)


NN = ((1,), (0,))
NT = ((1,), (1,))
TN = ((0,), (0,))


def joined(parts_ref, start, width, chunk, length):
    picked = [
        parts_ref[j, chunk * length : (chunk + 1) * length, start : start + width]
        for j in range(parts_ref.shape[0])
    ]
    return jnp.concatenate(picked, axis=1)


def three_parts(value):
    high = value.astype(BF16).astype(F32)
    mid = (value - high).astype(BF16).astype(F32)
    return high, mid, value - high - mid


def pack_kernel(tokens_ref, offsets_ref, conv_gain_ref, memory_gain_ref, out_ref):
    length = tokens_ref.shape[0]
    offsets = three_parts(offsets_ref[...])
    conv_gain = three_parts(conv_gain_ref[...])
    memory_gain = three_parts(memory_gain_ref[...])
    rows = [jnp.concatenate([p[k : k + 1] for k in range(p.shape[0])], axis=1) for p in offsets]
    rows += memory_gain
    rows.append(jnp.concatenate(conv_gain[:2], axis=1))
    rows.append(jnp.concatenate([conv_gain[2], jnp.zeros_like(conv_gain[2])], axis=1))
    extra = jnp.concatenate(rows, axis=0).astype(BF16)
    tokens = tokens_ref[...]
    for j in range(out_ref.shape[0]):
        out_ref[j, :length] = tokens
        out_ref[j, length:] = extra


def piece_kernel(query_ref, key_ref, value_ref, left_ref, right_ref, out_weight_ref, out_ref):
    rows = query_ref.shape[0]
    nx, nc = out_ref.shape[0], out_ref.shape[1]
    wide = out_ref.shape[3]
    chunks = out_weight_ref.shape[1] // wide
    for x in range(nx):
        for c in range(nc):
            at = c * nx + x
            parts = []
            for ref in (query_ref, key_ref, value_ref, left_ref, right_ref):
                width = ref.shape[1] // (nx * nc)
                parts.append(ref[:, at * width : (at + 1) * width])
            out_ref[x, c, :rows] = jnp.concatenate(parts, axis=1)
            for k in range(chunks):
                out_ref[x, c, rows * (k + 1) : rows * (k + 2)] = out_weight_ref[
                    :, k * wide : (k + 1) * wide
                ]


def project_kernel(
    place_ref, own_ref, other_ref, w0_ref, w1_ref, w2_ref, w3_ref, gate_ref,
    qk_ref, v_ref, glu_ref, gates_ref, conv_gain_ref, memory_gain_ref,
):
    nx, ny, _, part = own_ref.shape
    block = w0_ref.shape[1]
    length = glu_ref.shape[1]
    blocks = part * ny // block
    per_part = part // block
    place, core, column = place_ref[0], place_ref[1], place_ref[2]
    groups = ((w0_ref, 0, w1_ref, 1), (w2_ref, 2, w3_ref, blocks - 1))
    tokens_rows = nx * length
    width = qk_ref.shape[4] // 2
    chan = glu_ref.shape[2] // nx
    lane = lax.broadcasted_iota(jnp.int32, (length, width), 1)
    ones = jnp.where(lane == 0, 1.0, 0.0).astype(BF16)
    row = lax.broadcasted_iota(jnp.int32, (2 * nx, length), 0)
    gate_in = jnp.zeros((2 * nx, length), F32)
    forget = jnp.zeros((2 * nx, length), F32)
    for half, ref in enumerate((own_ref, other_ref)):
        home = core if half == 0 else 1 - core
        acc = jnp.zeros((tokens_rows, w0_ref.shape[2]), F32)
        pre = jnp.zeros((tokens_rows, gate_ref.shape[1]), F32)
        for first_ref, first_at, second_ref, second_at in groups:
            for k in range(w0_ref.shape[0]):
                left, right, gate_rows = [], [], []
                for w_ref, at in ((first_ref, first_at), (second_ref, second_at)):
                    kb = lax.rem(place + at + k * (blocks // w0_ref.shape[0]), blocks)
                    lanes = pl.ds(pl.multiple_of(lax.rem(kb, per_part) * block, block), block)
                    left.append(
                        ref[:, lax.div(kb, per_part), :length, lanes].reshape(tokens_rows, block)
                    )
                    right.append(w_ref[k])
                    gate_rows.append(gate_ref[pl.ds(pl.multiple_of(kb * block, block), block)])
                lhs = jnp.concatenate(left, axis=1)
                acc = acc + dot(lhs, jnp.concatenate(right, axis=0), NN)
                pre = pre + dot(lhs, jnp.concatenate(gate_rows, axis=0), NN)
        packed = []
        for x in range(nx):
            here = slice(x * length, (x + 1) * length)
            mine = acc[here]
            qk = mine[:, : 2 * width].astype(BF16)[None]
            for j in range(qk_ref.shape[0]):
                qk_ref[j, x, pl.ds(home, 1)] = qk
            v_ref[x, pl.ds(home, 1)] = jnp.concatenate(
                [mine[:, 2 * width : 3 * width].astype(BF16), ones], axis=1
            )[None]
            left = mine[:, 3 * width : 3 * width + chan]
            right = mine[:, 3 * width + chan :]
            packed.append(left / (1.0 + jnp.exp(-right)))
            turned = pre[here].T
            extra = ref[x, column, length : length + 8].astype(F32)
            values = extra[0:1] + extra[1:2] + extra[2:3]
            offsets = jnp.where(core == 0, values[:, :length], values[:, length : 2 * length])
            offsets_f = jnp.where(
                core == 0, values[:, 2 * length : 3 * length], values[:, 3 * length : 4 * length]
            )
            at = row == 2 * x + home
            gate_pre = jnp.where(core == 0, turned[0:1], turned[1:2])
            forget_pre = jnp.where(core == 0, turned[2:3], turned[3:4])
            gate_in = jnp.where(at, gate_pre + offsets, gate_in)
            forget = jnp.where(at, forget_pre + offsets_f, forget)
        glu_ref[pl.ds(home, 1)] = jnp.concatenate(packed, axis=1).astype(BF16)[None]
    for b in range(ny):
        extra = own_ref[0, b, length : length + 8].astype(F32)
        memory_gain_ref[b : b + 1] = extra[3:4] + extra[4:5] + extra[5:6]
        half = part // 2
        conv_gain_ref[b : b + 1] = extra[6:7, :half] + extra[6:7, half:] + extra[7:8, :half]
    y = jnp.exp(-jnp.abs(forget))
    small = y * (1.0 - y * (1 / 2 - y * (1 / 3 - y * (1 / 4 - y * (1 / 5)))))
    gates_ref[0] = gate_in
    gates_ref[1] = jnp.minimum(forget, 0.0) - jnp.where(y < 0.03, small, jnp.log(1.0 + y))


def finish_kernel(arrived_ref, weight_ref, conv_gain_ref, memory_gain_ref, out_ref):
    nx, nc, ny, length, lanes = arrived_ref.shape
    width = lanes // 2
    chan = width // 2
    rows = weight_ref.shape[2] // 3
    depth = weight_ref.shape[0] // ny
    conv, memory = [], []
    for b in range(ny):
        pairs = [(x, c) for c in range(nc) for x in range(nx)]
        blocks = [arrived_ref[x, c, b].astype(F32) for x, c in pairs]
        memory.append(jnp.concatenate([t[:, :width] for t in blocks], axis=1))
        conv.append(
            jnp.concatenate(
                [t[:, width : width + chan] + t[:, width + chan :] for t in blocks], axis=1
            )
        )
    squares = sum(jnp.sum(m * m, axis=1, keepdims=True) for m in memory)
    scale = lax.rsqrt(squares / (ny * memory[0].shape[1]) + EPS)
    channels = ny * conv[0].shape[1]
    mean = sum(jnp.sum(t, axis=1, keepdims=True) for t in conv) / channels
    second = sum(jnp.sum(t * t, axis=1, keepdims=True) for t in conv) / channels
    spread = lax.rsqrt(second - mean * mean + EPS)
    total = jnp.zeros((length, out_ref.shape[1]), F32)
    for b in range(ny):
        scaled = (memory[b] * scale * memory_gain_ref[b : b + 1]).astype(BF16)
        normed = (conv[b] - mean) * spread * conv_gain_ref[b : b + 1]
        branch = (normed / (1.0 + jnp.exp(-normed))).astype(BF16)
        wide = branch.shape[1]
        for k, lhs in enumerate((scaled[:, :wide], scaled[:, wide:], branch)):
            rhs = weight_ref[b * depth : (b + 1) * depth, :, k * rows : (k + 1) * rows]
            total = total + dot(lhs, rhs.reshape(out_ref.shape[1], wide), NT)
    out_ref[...] = total.astype(BF16)


def convolve(glu_ref, prior_ref, taps_ref, out_ref, core, x_at):
    nc, length, lanes = glu_ref.shape
    nx, chan = out_ref.shape[0], out_ref.shape[2] // 2
    group = nc * length
    glu = glu_ref[...].reshape(group, lanes).astype(F32)
    taps = taps_ref.shape[0]
    hold = 32
    lane = lax.broadcasted_iota(jnp.int32, (hold, lanes), 1)
    before = pltpu.roll(glu[group - hold :], chan, 1)
    prior = jnp.concatenate([prior_ref[...].astype(F32), jnp.zeros((hold, lanes - chan), F32)], axis=1)
    extended = jnp.concatenate([jnp.where(lane < chan, prior, before), glu], axis=0)
    weights = taps_ref[...].astype(F32)
    weights = jnp.where(core == 0, weights[:, :lanes], weights[:, lanes:])
    weights = pltpu.roll(weights, lax.rem(lanes - chan * x_at, lanes), 1)
    weights = jnp.where(lax.broadcasted_iota(jnp.int32, weights.shape, 1) < chan, weights, 0.0)
    weights = sum(pltpu.roll(weights, chan * k, 1) for k in range(1, nx)) + weights
    total = jnp.zeros((group, lanes), F32)
    first = hold - (taps - 1)
    for shift in range(8):
        moved = extended[shift : shift + group + hold - 8] if shift else extended
        for j in range(taps):
            at = first + j
            if at % 8 == shift:
                total = total + moved[at - shift : at - shift + group] * weights[j : j + 1]
    high = total.astype(BF16)
    low = (total - high.astype(F32)).astype(BF16)
    for x in range(nx):
        mine = slice(x * chan, (x + 1) * chan)
        out_ref[x] = jnp.concatenate([high[:, mine], low[:, mine]], axis=1)


def slab_kernel(
    place_ref, qk_ref, v_ref, gate_ref, glu_ref, prior_ref, taps_ref,
    out_ref, q_ref, k_ref, conv_ref,
):
    convolve(glu_ref, prior_ref, taps_ref, conv_ref, place_ref[1], place_ref[3])
    chunks, length = gate_ref.shape[1], gate_ref.shape[2]
    width = qk_ref.shape[2] // 2
    gate, forget = gate_ref[0], gate_ref[1]
    within = lane_cumsum(forget)
    ends = [within[r : r + 1, length - 1 :] for r in range(chunks)]
    after = [jnp.zeros((1, 1), F32)]
    for r in range(chunks - 1, 0, -1):
        after.insert(0, after[0] + ends[r])
    total = after[0] + ends[0]
    to_end = jnp.concatenate([e + a for e, a in zip(ends, after)], axis=0)
    end_log = to_end - within + gate
    level = jnp.max(jnp.max(end_log, axis=1, keepdims=True), axis=0, keepdims=True)
    fresh = columns_of(jnp.exp(end_log - level))
    state = jnp.zeros((2 * width, width * qk_ref.shape[0]), F32)
    for r in range(chunks):
        q_ref[r * length : (r + 1) * length] = joined(qk_ref, 0, width, r, length)
        key = joined(qk_ref, width, width, r, length)
        k_ref[r * length : (r + 1) * length] = key
        scaled = (fresh[:, r : r + 1] * key.astype(F32)).astype(BF16)
        state = state + dot(v_ref[r * length : (r + 1) * length], scaled, TN)
    rows = out_ref.shape[1]
    kept = state[:rows]
    row = lax.broadcasted_iota(jnp.int32, kept.shape, 0)
    lane = lax.broadcasted_iota(jnp.int32, kept.shape, 1)
    for at, value in ((0, level), (3, total)):
        high = value.astype(BF16).astype(F32)
        mid = (value - high).astype(BF16).astype(F32)
        low = value - high - mid
        for k, part in enumerate((high, mid, low)):
            kept = jnp.where((row == width + 1) & (lane == at + k), part, kept)
    kept = kept.astype(BF16)
    for j in range(out_ref.shape[0]):
        out_ref[j] = kept


def cell_kernel(place_ref, in_ref, q_ref, k_ref, v_ref, gate_ref, conv_ref, out_ref):
    chunks, length = gate_ref.shape[1], gate_ref.shape[2]
    members, rows, head = in_ref.shape
    width = out_ref.shape[4] // 2
    nc, ny = out_ref.shape[1], out_ref.shape[2]
    scale = head ** (-0.5)
    place = place_ref[0]
    acc = jnp.zeros((1, 1), F32)
    logs = [None] * members
    for j in range(members - 1, -1, -1):
        line = in_ref[j, width + 1 : width + 2, :128].astype(F32)
        level_j = line[:, 0:1] + line[:, 1:2] + line[:, 2:3]
        total_j = line[:, 3:4] + line[:, 4:5] + line[:, 5:6]
        before = j < place
        logs[j] = jnp.where(before, level_j + acc, LOW)
        acc = acc + jnp.where(before, total_j, 0.0)
    level = logs[0]
    for j in range(1, members):
        level = jnp.maximum(level, logs[j])
    state = jnp.zeros((rows, head), F32)
    for j in range(members):
        weight = jnp.where(j < place, jnp.exp(logs[j] - level), 0.0)
        state = state + weight * in_ref[j].astype(F32)
    state = jnp.concatenate([state, jnp.zeros((2 * width - rows, head), F32)], axis=0)
    gate, forget = gate_ref[0], gate_ref[1]
    within = lane_cumsum(forget)
    turned = columns_of(jnp.concatenate([within, gate], axis=0))
    causal = lax.broadcasted_iota(jnp.int32, (length, length), 0) >= lax.broadcasted_iota(
        jnp.int32, (length, length), 1
    )
    for r in range(chunks):
        here = slice(r * length, (r + 1) * length)
        query, key, value = q_ref[here], k_ref[here], v_ref[here]
        within_row, gate_row = within[r : r + 1], gate[r : r + 1]
        within_col = turned[:, r : r + 1]
        gate_col = turned[:, chunks + r : chunks + r + 1]
        log_weight = jnp.where(causal, within_col - within_row + gate_row, -jnp.inf)
        carried = within_col + level
        top = jnp.maximum(carried, jnp.max(log_weight, axis=1, keepdims=True))
        weight = jnp.exp(log_weight - top)
        carried_weight = jnp.exp(carried - top) * scale
        scores = dot(query, key, NT) * (scale * weight)
        older = dot(query, state.astype(BF16), NT)
        numer = dot(scores.astype(BF16), value, NN) + carried_weight * older
        denom = jnp.sum(scores, axis=1, keepdims=True) + carried_weight * older[:, width : width + 1]
        result = numer[:, :width] / jnp.maximum(jnp.abs(denom), 1.0)
        x, c = r // nc, r % nc
        sent = jnp.concatenate(
            [result.astype(BF16), conv_ref[x, c * length : (c + 1) * length]], axis=1
        )
        for y in range(ny):
            out_ref[x, c, y] = sent
        last = within_row[:, length - 1 :]
        end_row = last - within_row + gate_row
        new_level = jnp.maximum(last + level, jnp.max(end_row, axis=1, keepdims=True))
        keep = jnp.exp(last + level - new_level)
        fresh = jnp.exp(last - within_col + gate_col - new_level)
        scaled = (fresh * key.astype(F32)).astype(BF16)
        state = keep * state + dot(value, scaled, TN)
        level = new_level


def vmem(count):
    return [pl.BlockSpec(memory_space=pltpu.VMEM)] * count


def layer(
    tokens,
    conv_value_weight,
    conv_gate_weight,
    conv_kernel,
    conv_norm_gain,
    query_weight,
    key_weight,
    value_weight,
    input_gate_weight,
    forget_gate_weight,
    input_offset,
    forget_offset,
    memory_norm_gain,
    conv_out_weight,
    memory_out_weight,
):
    nzh, nzl, nx, nc, ny = (size(a) for a in AXES)
    xi, ci, yi = lax.axis_index("x"), lax.axis_index("c"), lax.axis_index("tp")
    members = nzh * nzl
    zi = lax.axis_index("zh") * nzl + lax.axis_index("zl")
    length, part = tokens.shape
    slab = length * nx * nc
    head = query_weight.shape[1] // nc
    width = head // nx
    chan = conv_value_weight.shape[1] // nc // nx
    rows = query_weight.shape[0]
    wide = 3 * width + 2 * chan

    def from_z(value, ahead):
        return lax.ppermute(value, Z, [(j, (j - ahead) % members) for j in range(members)])

    out_rows = jnp.concatenate([memory_out_weight, conv_out_weight], axis=0).T
    pieces = pl.pallas_call(
        piece_kernel,
        out_shape=jax.ShapeDtypeStruct((nx, nc, 4 * rows, wide), BF16),
        in_specs=vmem(6),
        out_specs=pl.BlockSpec(memory_space=pltpu.VMEM),
        interpret=INTERPRET,
        name="pieces",
    )(query_weight, key_weight, value_weight, conv_value_weight, conv_gate_weight, out_rows)
    pieces = exchange(pieces.reshape(nx * nc, 4 * rows, wide), ("x", "c"))
    mine = pieces[:, :rows].reshape(nx * nc * rows, wide)
    turned = lax.ppermute(
        pieces[:, rows:],
        ("zh", "tp"),
        [(a * ny + b, b * ny + a) for a in range(nzh) for b in range(ny)],
    )
    step = members // 4
    far = [from_z(mine, k * step) for k in (1, 2, 3)]

    offsets = jnp.concatenate([input_offset.T, forget_offset.T], axis=0)
    offsets, turned = lax.optimization_barrier((offsets, turned))
    tall = length + 8
    sent = pl.pallas_call(
        pack_kernel,
        out_shape=jax.ShapeDtypeStruct((nx * ny, tall, part), BF16),
        in_specs=vmem(4),
        out_specs=pl.BlockSpec(memory_space=pltpu.VMEM),
        interpret=INTERPRET,
        name="pack",
    )(tokens, offsets, conv_norm_gain[None], memory_norm_gain[None])
    own = exchange(sent, ("x", "tp")).reshape(nx, ny, tall, part)
    other = swapped(own, "c")
    near = jnp.stack([mine, *far], axis=0)
    sets = [near, from_z(near, 1), from_z(near, 2), from_z(near, -1)]
    out_weight = lax.all_gather(turned, Z, axis=0, tiled=False)
    out_weight = out_weight.reshape(members, nx * nc, 3 * rows, wide)

    gate_weight = jnp.pad(
        jnp.concatenate([input_gate_weight, forget_gate_weight], axis=1), ((0, 0), (0, 124))
    )
    place = jnp.stack([zi, ci, yi, xi])
    smem = pl.BlockSpec(memory_space=pltpu.SMEM)
    qk, value, packed, gates, conv_gain, memory_gain = pl.pallas_call(
        project_kernel,
        out_shape=(
            jax.ShapeDtypeStruct((nx, nx, nc, length, 2 * width), BF16),
            jax.ShapeDtypeStruct((nx, nc, length, 2 * width), BF16),
            jax.ShapeDtypeStruct((nc, length, nx * chan), BF16),
            jax.ShapeDtypeStruct((2, nx * nc, length), F32),
            jax.ShapeDtypeStruct((ny, conv_norm_gain.shape[0]), F32),
            jax.ShapeDtypeStruct((ny, memory_norm_gain.shape[0]), F32),
        ),
        in_specs=[smem] + vmem(7),
        out_specs=vmem(6),
        interpret=INTERPRET,
        name="project",
    )(place, own, other, *sets, gate_weight)
    value = value.reshape(slab, 2 * width)
    group = slab // nx
    hold = 32
    prior = lax.ppermute(
        packed[nc - 1, length - hold :, (nx - 1) * chan :],
        Z,
        [(j, j + 1) for j in range(members - 1)],
    )
    all_qk = exchange(qk.reshape(nx, slab, 2 * width), "x")

    state_rows = width + 8
    states, query, key, conv_sent = pl.pallas_call(
        slab_kernel,
        out_shape=(
            jax.ShapeDtypeStruct((members, state_rows, head), BF16),
            jax.ShapeDtypeStruct((slab, head), BF16),
            jax.ShapeDtypeStruct((slab, head), BF16),
            jax.ShapeDtypeStruct((nx, group, 2 * chan), BF16),
        ),
        in_specs=[smem] + vmem(6),
        out_specs=vmem(4),
        interpret=INTERPRET,
        name="slab_state",
    )(place, all_qk, value, gates, packed, prior, conv_kernel)
    states = exchange(states, Z)
    last = pl.pallas_call(
        cell_kernel,
        out_shape=jax.ShapeDtypeStruct((nx, nc, ny, length, 2 * width), BF16),
        in_specs=[smem] + vmem(6),
        out_specs=pl.BlockSpec(memory_space=pltpu.VMEM),
        interpret=INTERPRET,
        name="cell",
    )(place, states, query, key, value, gates, conv_sent)
    arrived = exchange(last.reshape(nx * nc * ny, length, -1), ("x", "c", "tp"))
    arrived = arrived.reshape(nx, nc, ny, length, -1)
    return pl.pallas_call(
        finish_kernel,
        out_shape=jax.ShapeDtypeStruct((length, part), BF16),
        in_specs=vmem(4),
        out_specs=pl.BlockSpec(memory_space=pltpu.VMEM),
        interpret=INTERPRET,
        name="finish",
    )(arrived, out_weight, conv_gain, memory_gain)


def solution(mesh):
    shape = mesh.shape
    depth = shape["sp"] // 32
    split = Mesh(mesh.devices.reshape(4, depth, 4, 2, shape["tp"]), AXES)
    in_specs = (
        P(SP, "tp"),
        P(SP, "tp"),
        P(SP, "tp"),
        P(None, "tp"),
        P("tp"),
        P(SP, "tp"),
        P(SP, "tp"),
        P(SP, "tp"),
        P(None, "tp"),
        P(None, "tp"),
        P(SP, "tp"),
        P(SP, "tp"),
        P("tp"),
        P("tp", SP),
        P("tp", SP),
    )
    return jax.shard_map(
        layer, mesh=split, in_specs=in_specs, out_specs=P(SP, "tp"), check_vma=False
    )
```

```python
import jax
import jax.numpy as jnp
from jax import lax
from jax.experimental import pallas as pl
from jax.experimental.pallas import tpu as pltpu
from jax.sharding import Mesh
from jax.sharding import PartitionSpec as P

AXES = ("zh", "zl", "x", "c", "tp")
Z = ("zh", "zl")
SP = ("zh", "zl", "x", "c")
EPS = 1e-06
LOW = -1e30
F32 = jnp.float32
BF16 = jnp.bfloat16
INTERPRET = False


def size(axis):
    return lax.axis_size(axis)


def exchange(pieces, axes):
    return lax.all_to_all(pieces, axes, split_axis=0, concat_axis=0, tiled=True)


def swapped(value, axis):
    return lax.ppermute(value, axis, [(0, 1), (1, 0)])


def lane_cumsum(rows):
    lane = lax.broadcasted_iota(jnp.int32, rows.shape, 1)
    step = 1
    while step < rows.shape[1]:
        moved = pltpu.roll(rows, step, 1)
        rows = rows + jnp.where(lane >= step, moved, 0.0)
        step *= 2
    return rows


def columns_of(rows):
    count, length = rows.shape
    square = jnp.concatenate([rows, jnp.zeros((length - count, length), F32)], axis=0)
    return square.T


def dot(a, b, dims):
    return lax.dot_general(a, b, (dims, ((), ())), preferred_element_type=F32)


NN = ((1,), (0,))
NT = ((1,), (1,))
TN = ((0,), (0,))


def joined(parts_ref, start, width, chunk, length):
    picked = [
        parts_ref[j, chunk * length : (chunk + 1) * length, start : start + width]
        for j in range(parts_ref.shape[0])
    ]
    return jnp.concatenate(picked, axis=1)


def three_parts(value):
    high = value.astype(BF16).astype(F32)
    mid = (value - high).astype(BF16).astype(F32)
    return high, mid, value - high - mid


def pack_kernel(tokens_ref, offsets_ref, conv_gain_ref, memory_gain_ref, out_ref):
    length = tokens_ref.shape[0]
    offsets = three_parts(offsets_ref[...])
    conv_gain = three_parts(conv_gain_ref[...])
    memory_gain = three_parts(memory_gain_ref[...])
    rows = [jnp.concatenate([p[k : k + 1] for k in range(p.shape[0])], axis=1) for p in offsets]
    rows += memory_gain
    rows.append(jnp.concatenate(conv_gain[:2], axis=1))
    rows.append(jnp.concatenate([conv_gain[2], jnp.zeros_like(conv_gain[2])], axis=1))
    extra = jnp.concatenate(rows, axis=0).astype(BF16)
    tokens = tokens_ref[...]
    for j in range(out_ref.shape[0]):
        out_ref[j, :length] = tokens
        out_ref[j, length:] = extra


def piece_kernel(query_ref, key_ref, value_ref, left_ref, right_ref, out_weight_ref, out_ref):
    rows = query_ref.shape[0]
    copies, nx, nc, _, half = out_ref.shape
    for x in range(nx):
        for c in range(nc):
            at = c * nx + x
            parts = []
            for ref in (query_ref, key_ref, value_ref, left_ref, right_ref):
                width = ref.shape[1] // (nx * nc)
                parts.append(ref[:, at * width : (at + 1) * width])
            whole = jnp.concatenate(parts, axis=1)
            for j in range(copies):
                out_ref[j, x, c, :rows] = whole[:, :half]
                out_ref[j, x, c, rows : 2 * rows] = whole[:, half:]
                out_ref[j, x, c, 2 * rows :] = out_weight_ref[x, c]


def project_kernel(
    place_ref, own_ref, other_ref, w0_ref, w1_ref, w3_ref, low_ref, high_ref, gate_ref,
    qk_ref, v_ref, glu_ref, gates_ref, gain_ref, out_weight_ref,
):
    nx, ny, _, part = own_ref.shape
    far, senders, tall_piece, side = w0_ref.shape
    rows = tall_piece // 3
    block = senders * rows
    close = part // block
    length = glu_ref.shape[1]
    at_close, core, column = place_ref[0], place_ref[1], place_ref[2]
    tokens_rows = nx * length
    width = qk_ref.shape[4] // 2
    chan = glu_ref.shape[2] // nx
    lane = lax.broadcasted_iota(jnp.int32, (length, width), 1)
    ones = jnp.where(lane == 0, 1.0, 0.0).astype(BF16)
    row = lax.broadcasted_iota(jnp.int32, (2 * nx, length), 0)
    gate_in = jnp.zeros((2 * nx, length), F32)
    forget = jnp.zeros((2 * nx, length), F32)

    def piece(distance, k):
        if distance == 2:
            return low_ref[k] if k < far // 2 else high_ref[k - far // 2]
        return (w0_ref, w1_ref, None, w3_ref)[distance][k]

    homes = [lax.rem(at_close + distance, close) for distance in range(close)]
    for distance in range(close):
        for k in range(far):
            out_weight_ref[k, pl.ds(homes[distance], 1)] = piece(distance, k)[:, 2 * rows :][None]

    def weight_block(distance, k):
        mine = piece(distance, k)
        return jnp.concatenate(
            [
                mine[:, :rows].reshape(block, side),
                mine[:, rows : 2 * rows].reshape(block, side),
            ],
            axis=1,
        )

    for half, ref in enumerate((own_ref, other_ref)):
        home = core if half == 0 else 1 - core
        acc = jnp.zeros((tokens_rows, 2 * side), F32)
        pre = jnp.zeros((tokens_rows, gate_ref.shape[1]), F32)
        for k in range(far):
            for pair in ((0, 1), (2, 3)):
                left, right, gate_rows = [], [], []
                for distance in pair:
                    start = pl.multiple_of(homes[distance] * block, block)
                    lanes = pl.ds(start, block)
                    left.append(ref[:, k, :length, lanes].reshape(tokens_rows, block))
                    right.append(weight_block(distance, k))
                    gate_rows.append(gate_ref[pl.ds(k * part + start, block)])
                lhs = jnp.concatenate(left, axis=1)
                acc = acc + dot(lhs, jnp.concatenate(right, axis=0), NN)
                pre = pre + dot(lhs, jnp.concatenate(gate_rows, axis=0), NN)
        packed = []
        for x in range(nx):
            here = slice(x * length, (x + 1) * length)
            mine = acc[here]
            qk = mine[:, : 2 * width].astype(BF16)[None]
            for j in range(qk_ref.shape[0]):
                qk_ref[j, x, pl.ds(home, 1)] = qk
            v_ref[x, pl.ds(home, 1)] = jnp.concatenate(
                [mine[:, 2 * width : 3 * width].astype(BF16), ones], axis=1
            )[None]
            left = mine[:, 3 * width : 3 * width + chan]
            right = mine[:, 3 * width + chan :]
            packed.append(left / (1.0 + jnp.exp(-right)))
            turned = pre[here].T
            extra = ref[x, column, length : length + 8].astype(F32)
            values = extra[0:1] + extra[1:2] + extra[2:3]
            offsets = jnp.where(core == 0, values[:, :length], values[:, length : 2 * length])
            offsets_f = jnp.where(
                core == 0, values[:, 2 * length : 3 * length], values[:, 3 * length : 4 * length]
            )
            at = row == 2 * x + home
            gate_pre = jnp.where(core == 0, turned[0:1], turned[1:2])
            forget_pre = jnp.where(core == 0, turned[2:3], turned[3:4])
            gate_in = jnp.where(at, gate_pre + offsets, gate_in)
            forget = jnp.where(at, forget_pre + offsets_f, forget)
        glu_ref[pl.ds(home, 1)] = jnp.concatenate(packed, axis=1).astype(BF16)[None]
    for b in range(ny):
        extra = own_ref[0, b, length : length + 8].astype(F32)
        memory_gain = extra[3:4] + extra[4:5] + extra[5:6]
        half = part // 2
        conv_gain = extra[6:7, :half] + extra[6:7, half:] + extra[7:8, :half]
        for at in range(2 * nx):
            gain_ref[b, at : at + 1] = jnp.concatenate(
                [
                    memory_gain[:, at * width : (at + 1) * width],
                    conv_gain[:, at * chan : (at + 1) * chan],
                    jnp.zeros((1, width - chan), F32),
                ],
                axis=1,
            )
    y = jnp.exp(-jnp.abs(forget))
    small = y * (1.0 - y * (1 / 2 - y * (1 / 3 - y * (1 / 4 - y * (1 / 5)))))
    gates_ref[0] = gate_in
    gates_ref[1] = jnp.minimum(forget, 0.0) - jnp.where(y < 0.03, small, jnp.log(1.0 + y))


def finish_kernel(place_ref, arrived_ref, own_ref, other_ref, gain_ref, out_ref):
    nx, nc, ny, length, lanes = arrived_ref.shape
    core, x_at = place_ref[1], place_ref[3]
    width = lanes // 2
    chan = width // 2
    part = out_ref.shape[1]
    lane = lax.broadcasted_iota(jnp.int32, (length, lanes), 1)
    is_memory = lane < width
    is_conv = (lane >= width) & (lane < width + chan)

    def block(x, c, b):
        got = arrived_ref[x, c, b].astype(F32)
        both = got + pltpu.roll(got, lanes - chan, 1)
        return jnp.where(is_memory, got, jnp.where(is_conv, both, 0.0))

    first = jnp.zeros((length, lanes), F32)
    second = jnp.zeros((length, lanes), F32)
    for x in range(nx):
        for c in range(nc):
            for b in range(ny):
                got = block(x, c, b)
                first = first + got
                second = second + got * got
    senders = nx * nc * ny
    memory_mean = jnp.sum(jnp.where(is_memory, second, 0.0), axis=1, keepdims=True)
    scale = lax.rsqrt(memory_mean / (senders * width) + EPS)
    mean = jnp.sum(jnp.where(is_conv, first, 0.0), axis=1, keepdims=True) / (senders * chan)
    power = jnp.sum(jnp.where(is_conv, second, 0.0), axis=1, keepdims=True) / (senders * chan)
    spread = lax.rsqrt(power - mean * mean + EPS)
    shift = jnp.where(is_memory, 0.0, mean)
    factor = jnp.where(is_memory, scale, spread)
    total = jnp.zeros((length, part), F32)
    for b in range(ny):
        for ahead in range(nx):
            x = lax.rem(x_at + ahead, nx)
            left, right = [], []
            for c, ref in ((core, own_ref), (1 - core, other_ref)):
                gain = gain_ref[b, pl.ds(c * nx + x, 1)]
                normed = (block(x, c, b) - shift) * factor * gain
                branch = normed / (1.0 + jnp.exp(-normed))
                used = jnp.where(is_memory, normed, jnp.where(is_conv, branch, 0.0))
                left.append(used.astype(BF16))
                right.append(ref[ahead, b].reshape(part, lanes))
            total = total + dot(
                jnp.concatenate(left, axis=1), jnp.concatenate(right, axis=1), NT
            )
    out_ref[...] = total.astype(BF16)


def convolve(glu_ref, prior_ref, taps_ref, out_ref, core, x_at):
    nc, length, lanes = glu_ref.shape
    nx, chan = out_ref.shape[0], out_ref.shape[2] // 2
    group = nc * length
    glu = glu_ref[...].reshape(group, lanes).astype(F32)
    taps = taps_ref.shape[0]
    hold = 32
    lane = lax.broadcasted_iota(jnp.int32, (hold, lanes), 1)
    before = pltpu.roll(glu[group - hold :], chan, 1)
    prior = jnp.concatenate([prior_ref[...].astype(F32), jnp.zeros((hold, lanes - chan), F32)], axis=1)
    extended = jnp.concatenate([jnp.where(lane < chan, prior, before), glu], axis=0)
    weights = taps_ref[...].astype(F32)
    weights = jnp.where(core == 0, weights[:, :lanes], weights[:, lanes:])
    weights = pltpu.roll(weights, lax.rem(lanes - chan * x_at, lanes), 1)
    weights = jnp.where(lax.broadcasted_iota(jnp.int32, weights.shape, 1) < chan, weights, 0.0)
    weights = sum(pltpu.roll(weights, chan * k, 1) for k in range(1, nx)) + weights
    total = jnp.zeros((group, lanes), F32)
    first = hold - (taps - 1)
    for shift in range(8):
        moved = extended[shift : shift + group + hold - 8] if shift else extended
        for j in range(taps):
            at = first + j
            if at % 8 == shift:
                total = total + moved[at - shift : at - shift + group] * weights[j : j + 1]
    high = total.astype(BF16)
    low = (total - high.astype(F32)).astype(BF16)
    for x in range(nx):
        mine = slice(x * chan, (x + 1) * chan)
        out_ref[x] = jnp.concatenate([high[:, mine], low[:, mine]], axis=1)


def slab_kernel(
    place_ref, qk_ref, v_ref, gate_ref, glu_ref, prior_ref, taps_ref,
    out_ref, q_ref, k_ref, conv_ref,
):
    convolve(glu_ref, prior_ref, taps_ref, conv_ref, place_ref[1], place_ref[3])
    chunks, length = gate_ref.shape[1], gate_ref.shape[2]
    width = qk_ref.shape[2] // 2
    gate, forget = gate_ref[0], gate_ref[1]
    within = lane_cumsum(forget)
    ends = [within[r : r + 1, length - 1 :] for r in range(chunks)]
    after = [jnp.zeros((1, 1), F32)]
    for r in range(chunks - 1, 0, -1):
        after.insert(0, after[0] + ends[r])
    total = after[0] + ends[0]
    to_end = jnp.concatenate([e + a for e, a in zip(ends, after)], axis=0)
    end_log = to_end - within + gate
    level = jnp.max(jnp.max(end_log, axis=1, keepdims=True), axis=0, keepdims=True)
    fresh = columns_of(jnp.exp(end_log - level))
    state = jnp.zeros((2 * width, width * qk_ref.shape[0]), F32)
    for r in range(chunks):
        q_ref[r * length : (r + 1) * length] = joined(qk_ref, 0, width, r, length)
        key = joined(qk_ref, width, width, r, length)
        k_ref[r * length : (r + 1) * length] = key
        scaled = (fresh[:, r : r + 1] * key.astype(F32)).astype(BF16)
        state = state + dot(v_ref[r * length : (r + 1) * length], scaled, TN)
    rows = out_ref.shape[1]
    kept = state[:rows]
    row = lax.broadcasted_iota(jnp.int32, kept.shape, 0)
    lane = lax.broadcasted_iota(jnp.int32, kept.shape, 1)
    for at, value in ((0, level), (3, total)):
        high = value.astype(BF16).astype(F32)
        mid = (value - high).astype(BF16).astype(F32)
        low = value - high - mid
        for k, part in enumerate((high, mid, low)):
            kept = jnp.where((row == width + 1) & (lane == at + k), part, kept)
    kept = kept.astype(BF16)
    for j in range(out_ref.shape[0]):
        out_ref[j] = kept


def cell_kernel(place_ref, in_ref, q_ref, k_ref, v_ref, gate_ref, conv_ref, out_ref):
    chunks, length = gate_ref.shape[1], gate_ref.shape[2]
    members, rows, head = in_ref.shape
    width = out_ref.shape[4] // 2
    nc, ny = out_ref.shape[1], out_ref.shape[2]
    scale = head ** (-0.5)
    place = place_ref[4]
    acc = jnp.zeros((1, 1), F32)
    logs = [None] * members
    for j in range(members - 1, -1, -1):
        line = in_ref[j, width + 1 : width + 2, :128].astype(F32)
        level_j = line[:, 0:1] + line[:, 1:2] + line[:, 2:3]
        total_j = line[:, 3:4] + line[:, 4:5] + line[:, 5:6]
        before = j < place
        logs[j] = jnp.where(before, level_j + acc, LOW)
        acc = acc + jnp.where(before, total_j, 0.0)
    level = logs[0]
    for j in range(1, members):
        level = jnp.maximum(level, logs[j])
    state = jnp.zeros((rows, head), F32)
    for j in range(members):
        weight = jnp.where(j < place, jnp.exp(logs[j] - level), 0.0)
        state = state + weight * in_ref[j].astype(F32)
    state = jnp.concatenate([state, jnp.zeros((2 * width - rows, head), F32)], axis=0)
    gate, forget = gate_ref[0], gate_ref[1]
    within = lane_cumsum(forget)
    turned = columns_of(jnp.concatenate([within, gate], axis=0))
    causal = lax.broadcasted_iota(jnp.int32, (length, length), 0) >= lax.broadcasted_iota(
        jnp.int32, (length, length), 1
    )
    for r in range(chunks):
        here = slice(r * length, (r + 1) * length)
        query, key, value = q_ref[here], k_ref[here], v_ref[here]
        within_row, gate_row = within[r : r + 1], gate[r : r + 1]
        within_col = turned[:, r : r + 1]
        gate_col = turned[:, chunks + r : chunks + r + 1]
        log_weight = jnp.where(causal, within_col - within_row + gate_row, -jnp.inf)
        carried = within_col + level
        top = jnp.maximum(carried, jnp.max(log_weight, axis=1, keepdims=True))
        weight = jnp.exp(log_weight - top)
        carried_weight = jnp.exp(carried - top) * scale
        scores = dot(query, key, NT) * (scale * weight)
        older = dot(query, state.astype(BF16), NT)
        numer = dot(scores.astype(BF16), value, NN) + carried_weight * older
        denom = jnp.sum(scores, axis=1, keepdims=True) + carried_weight * older[:, width : width + 1]
        result = numer[:, :width] / jnp.maximum(jnp.abs(denom), 1.0)
        x, c = r // nc, r % nc
        sent = jnp.concatenate(
            [result.astype(BF16), conv_ref[x, c * length : (c + 1) * length]], axis=1
        )
        for y in range(ny):
            out_ref[x, c, y] = sent
        last = within_row[:, length - 1 :]
        end_row = last - within_row + gate_row
        new_level = jnp.maximum(last + level, jnp.max(end_row, axis=1, keepdims=True))
        keep = jnp.exp(last + level - new_level)
        fresh = jnp.exp(last - within_col + gate_col - new_level)
        scaled = (fresh * key.astype(F32)).astype(BF16)
        state = keep * state + dot(value, scaled, TN)
        level = new_level


def vmem(count):
    return [pl.BlockSpec(memory_space=pltpu.VMEM)] * count


def layer(
    tokens,
    conv_value_weight,
    conv_gate_weight,
    conv_kernel,
    conv_norm_gain,
    query_weight,
    key_weight,
    value_weight,
    input_gate_weight,
    forget_gate_weight,
    input_offset,
    forget_offset,
    memory_norm_gain,
    conv_out_weight,
    memory_out_weight,
):
    nzh, nzl, nx, nc, ny = (size(a) for a in AXES)
    xi, ci, yi = lax.axis_index("x"), lax.axis_index("c"), lax.axis_index("tp")
    members = nzh * nzl
    zi = lax.axis_index("zh") * nzl + lax.axis_index("zl")
    length, part = tokens.shape
    slab = length * nx * nc
    head = query_weight.shape[1] // nc
    width = head // nx
    chan = conv_value_weight.shape[1] // nc // nx
    rows = query_weight.shape[0]
    wide = 3 * width + 2 * chan

    def from_z(value, ahead):
        return lax.ppermute(value, Z, [(j, (j - ahead) % members) for j in range(members)])

    out_rows = jnp.concatenate(
        [
            memory_out_weight.reshape(nc, nx, width, rows),
            conv_out_weight.reshape(nc, nx, chan, rows),
            jnp.zeros((nc, nx, width - chan, rows), BF16),
        ],
        axis=2,
    ).transpose(1, 0, 3, 2)
    turned = lax.ppermute(
        out_rows,
        ("zh", "tp"),
        [(a * ny + b, b * ny + a) for a in range(nzh) for b in range(ny)],
    )
    offsets = jnp.concatenate([input_offset.T, forget_offset.T], axis=0)
    tall = length + 8
    sent = pl.pallas_call(
        pack_kernel,
        out_shape=jax.ShapeDtypeStruct((nx * ny, tall, part), BF16),
        in_specs=vmem(4),
        out_specs=pl.BlockSpec(memory_space=pltpu.VMEM),
        interpret=INTERPRET,
        name="pack",
    )(tokens, offsets, conv_norm_gain[None], memory_norm_gain[None])
    own = exchange(sent, ("x", "tp")).reshape(nx, ny, tall, part)
    other = swapped(own, "c")
    own, turned = lax.optimization_barrier((own, turned))
    pieces = pl.pallas_call(
        piece_kernel,
        out_shape=jax.ShapeDtypeStruct((nzh, nx, nc, 3 * rows, wide // 2), BF16),
        in_specs=vmem(6),
        out_specs=pl.BlockSpec(memory_space=pltpu.VMEM),
        interpret=INTERPRET,
        name="pieces",
    )(query_weight, key_weight, value_weight, conv_value_weight, conv_gate_weight, turned)
    near = exchange(pieces.reshape(nzh * nx * nc, 3 * rows, wide // 2), ("zh", "x", "c"))
    near = near.reshape(nzh, nx * nc, 3 * rows, wide // 2)
    sets = [near, from_z(near, 1), from_z(near, -1)]
    sets += [from_z(near[: nzh // 2], 2), from_z(near[nzh // 2 :], -2)]

    gate_weight = jnp.pad(
        jnp.concatenate([input_gate_weight, forget_gate_weight], axis=1), ((0, 0), (0, 124))
    )
    place = jnp.stack([lax.axis_index("zl"), ci, yi, xi, zi])
    smem = pl.BlockSpec(memory_space=pltpu.SMEM)
    qk, value, packed, gates, gain, out_part = pl.pallas_call(
        project_kernel,
        out_shape=(
            jax.ShapeDtypeStruct((nx, nx, nc, length, 2 * width), BF16),
            jax.ShapeDtypeStruct((nx, nc, length, 2 * width), BF16),
            jax.ShapeDtypeStruct((nc, length, nx * chan), BF16),
            jax.ShapeDtypeStruct((2, nx * nc, length), F32),
            jax.ShapeDtypeStruct((ny, nc * nx, 2 * width), F32),
            jax.ShapeDtypeStruct((nzh, nzl, nx * nc, rows, wide // 2), BF16),
        ),
        in_specs=[smem] + vmem(8),
        out_specs=vmem(6),
        interpret=INTERPRET,
        name="project",
    )(place, own, other, *sets, gate_weight)
    value = value.reshape(slab, 2 * width)
    group = slab // nx
    hold = 32
    prior = lax.ppermute(
        packed[nc - 1, length - hold :, (nx - 1) * chan :],
        Z,
        [(j, j + 1) for j in range(members - 1)],
    )
    all_qk = exchange(qk.reshape(nx, slab, 2 * width), "x")
    out_part, all_qk = lax.optimization_barrier((out_part, all_qk))
    out_parts = [out_part] + [
        lax.ppermute(out_part, "x", [(j, (j - ahead) % nx) for j in range(nx)])
        for ahead in range(1, nx)
    ]
    own_out = jnp.stack(out_parts, axis=0)
    other_out = swapped(own_out, "c")

    state_rows = width + 8
    states, query, key, conv_sent = pl.pallas_call(
        slab_kernel,
        out_shape=(
            jax.ShapeDtypeStruct((members, state_rows, head), BF16),
            jax.ShapeDtypeStruct((slab, head), BF16),
            jax.ShapeDtypeStruct((slab, head), BF16),
            jax.ShapeDtypeStruct((nx, group, 2 * chan), BF16),
        ),
        in_specs=[smem] + vmem(6),
        out_specs=vmem(4),
        interpret=INTERPRET,
        name="slab_state",
    )(place, all_qk, value, gates, packed, prior, conv_kernel)
    states = exchange(states, Z)
    last = pl.pallas_call(
        cell_kernel,
        out_shape=jax.ShapeDtypeStruct((nx, nc, ny, length, 2 * width), BF16),
        in_specs=[smem] + vmem(6),
        out_specs=pl.BlockSpec(memory_space=pltpu.VMEM),
        interpret=INTERPRET,
        name="cell",
    )(place, states, query, key, value, gates, conv_sent)
    arrived = exchange(last.reshape(nx * nc * ny, length, -1), ("x", "c", "tp"))
    arrived = arrived.reshape(nx, nc, ny, length, -1)
    return pl.pallas_call(
        finish_kernel,
        out_shape=jax.ShapeDtypeStruct((length, part), BF16),
        in_specs=[smem] + vmem(4),
        out_specs=pl.BlockSpec(memory_space=pltpu.VMEM),
        interpret=INTERPRET,
        name="finish",
    )(place, arrived, own_out, other_out, gain)


def solution(mesh):
    shape = mesh.shape
    depth = shape["sp"] // 32
    split = Mesh(mesh.devices.reshape(4, depth, 4, 2, shape["tp"]), AXES)
    in_specs = (
        P(SP, "tp"),
        P(SP, "tp"),
        P(SP, "tp"),
        P(None, "tp"),
        P("tp"),
        P(SP, "tp"),
        P(SP, "tp"),
        P(SP, "tp"),
        P(None, "tp"),
        P(None, "tp"),
        P(SP, "tp"),
        P(SP, "tp"),
        P("tp"),
        P("tp", SP),
        P("tp", SP),
    )
    return jax.shard_map(
        layer, mesh=split, in_specs=in_specs, out_specs=P(SP, "tp"), check_vma=False
    )
```

```python
import jax
import jax.numpy as jnp
from jax import lax
from jax.experimental import pallas as pl
from jax.experimental.pallas import tpu as pltpu
from jax.sharding import Mesh
from jax.sharding import PartitionSpec as P

AXES = ("zh", "zl", "x", "c", "tp")
Z = ("zh", "zl")
SP = ("zh", "zl", "x", "c")
EPS = 1e-06
LOW = -1e30
F32 = jnp.float32
BF16 = jnp.bfloat16
INTERPRET = False


def size(axis):
    return lax.axis_size(axis)


def exchange(pieces, axes):
    return lax.all_to_all(pieces, axes, split_axis=0, concat_axis=0, tiled=True)


def swapped(value, axis):
    return lax.ppermute(value, axis, [(0, 1), (1, 0)])


def lane_cumsum(rows):
    lane = lax.broadcasted_iota(jnp.int32, rows.shape, 1)
    step = 1
    while step < rows.shape[1]:
        moved = pltpu.roll(rows, step, 1)
        rows = rows + jnp.where(lane >= step, moved, 0.0)
        step *= 2
    return rows


def columns_of(rows):
    count, length = rows.shape
    square = jnp.concatenate([rows, jnp.zeros((length - count, length), F32)], axis=0)
    return square.T


def dot(a, b, dims):
    return lax.dot_general(a, b, (dims, ((), ())), preferred_element_type=F32)


NN = ((1,), (0,))
NT = ((1,), (1,))
TN = ((0,), (0,))


def joined(parts_ref, start, width, chunk, length):
    picked = [
        parts_ref[j, chunk * length : (chunk + 1) * length, start : start + width]
        for j in range(parts_ref.shape[0])
    ]
    return jnp.concatenate(picked, axis=1)


def three_parts(value):
    high = value.astype(BF16).astype(F32)
    mid = (value - high).astype(BF16).astype(F32)
    return high, mid, value - high - mid


def pack_kernel(tokens_ref, offsets_ref, conv_gain_ref, memory_gain_ref, upper_ref, lower_ref):
    length = tokens_ref.shape[0] // 2
    offsets = three_parts(offsets_ref[...])
    conv_gain = three_parts(conv_gain_ref[...])
    memory_gain = three_parts(memory_gain_ref[...])
    rows = [jnp.concatenate([p[k : k + 1] for k in range(p.shape[0])], axis=1) for p in offsets]
    rows += memory_gain
    rows.append(jnp.concatenate(conv_gain[:2], axis=1))
    rows.append(jnp.concatenate([conv_gain[2], jnp.zeros_like(conv_gain[2])], axis=1))
    extra = jnp.concatenate(rows, axis=0).astype(BF16)
    upper, lower = tokens_ref[:length], tokens_ref[length:]
    for j in range(upper_ref.shape[0]):
        upper_ref[j, :length] = upper
        upper_ref[j, length:] = extra
        lower_ref[j] = lower


def piece_kernel(
    query_ref, key_ref, value_ref, left_ref, right_ref, memory_ref, conv_ref, out_ref, turn_ref
):
    nx, nc = out_ref.shape[0], out_ref.shape[1]
    rows = turn_ref.shape[0]
    width, chan = memory_ref.shape[0] // (nx * nc), conv_ref.shape[0] // (nx * nc)
    parts = []
    for at in range(nx * nc):
        parts.append(memory_ref[at * width : (at + 1) * width].astype(F32))
        parts.append(conv_ref[at * chan : (at + 1) * chan].astype(F32))
    whole = jnp.concatenate(parts, axis=0)
    lanes = 128
    for j in range(whole.shape[0] // lanes):
        tile = whole[j * lanes : (j + 1) * lanes]
        tile = jnp.concatenate([tile, jnp.zeros((lanes, lanes - rows), F32)], axis=1)
        turn_ref[:, j * lanes : (j + 1) * lanes] = tile.T[:rows].astype(BF16)
    for x in range(nx):
        for c in range(nc):
            at = c * nx + x
            parts = []
            for ref in (query_ref, key_ref, value_ref, left_ref, right_ref):
                width = ref.shape[1] // (nx * nc)
                parts.append(ref[:, at * width : (at + 1) * width])
            out_ref[x, c] = jnp.concatenate(parts, axis=1)


def project_kernel(
    place_ref, own_a_ref, own_b_ref, other_a_ref, other_b_ref,
    w0_ref, w1_ref, w3_ref, low_ref, high_ref, gate_ref,
    qk_ref, v_ref, glu_ref, gates_ref, gain_ref, out_weight_ref,
):
    nx, ny, _, part = own_a_ref.shape
    far, tall, wide = w0_ref.shape
    depth, chunks = out_weight_ref.shape[2], out_weight_ref.shape[3] // wide
    rows = tall - depth * chunks
    close = part // rows
    members = far * close
    length = glu_ref.shape[1]
    half_length = length // 2
    place, core, column = place_ref[0], place_ref[1], place_ref[2]
    tokens_rows = nx * half_length
    width = qk_ref.shape[4] // 2
    chan = glu_ref.shape[2] // nx
    lane = lax.broadcasted_iota(jnp.int32, (half_length, width), 1)
    ones = jnp.where(lane == 0, 1.0, 0.0).astype(BF16)
    row = lax.broadcasted_iota(jnp.int32, (2 * nx, length), 0)
    gate_in = jnp.zeros((2 * nx, length), F32)
    forget = jnp.zeros((2 * nx, length), F32)

    blocks = [(ref, i, ahead + close * (i - 1)) for ref, ahead in ((w0_ref, 0), (w1_ref, 1), (w3_ref, -1)) for i in range(far)]
    blocks += [(low_ref, i, 2 + close * i) for i in range(far // 2)]
    blocks += [(high_ref, i, -2 + close * (i - 1)) for i in range(far // 2)]
    homes = []
    for ref, i, ahead in blocks:
        home = lax.rem(place + (ahead + members), members)
        homes.append((lax.div(home, close), lax.rem(home, close)))
        out_weight_ref[pl.ds(homes[-1][0], 1), pl.ds(homes[-1][1], 1)] = jnp.concatenate(
            [ref[i, rows + j * depth : rows + (j + 1) * depth] for j in range(chunks)], axis=1
        )[None, None]
    packed = [[None, None], [None, None]]
    for half, refs in enumerate(((own_a_ref, own_b_ref), (other_a_ref, other_b_ref))):
        home = core if half == 0 else 1 - core
        for side, ref in enumerate(refs):
            acc = jnp.zeros((tokens_rows, wide), F32)
            pre = jnp.zeros((tokens_rows, gate_ref.shape[1]), F32)
            for pair in range(0, len(blocks), 2):
                left, right, gate_rows = [], [], []
                for at in (pair, pair + 1):
                    w_ref, i, _ = blocks[at]
                    y, z = homes[at]
                    start = pl.multiple_of(z * rows, rows)
                    lanes = pl.ds(start, rows)
                    left.append(ref[:, pl.ds(y, 1), :half_length, lanes].reshape(tokens_rows, rows))
                    right.append(w_ref[i, :rows])
                    gate_rows.append(gate_ref[pl.ds(y * part + start, rows)])
                lhs = jnp.concatenate(left, axis=1)
                acc = acc + dot(lhs, jnp.concatenate(right, axis=0), NN)
                pre = pre + dot(lhs, jnp.concatenate(gate_rows, axis=0), NN)
            glu = []
            span = slice(side * half_length, (side + 1) * half_length)
            for x in range(nx):
                here = slice(x * half_length, (x + 1) * half_length)
                mine = acc[here]
                qk = mine[:, : 2 * width].astype(BF16)[None]
                for j in range(qk_ref.shape[0]):
                    qk_ref[j, x, pl.ds(home, 1), span] = qk
                v_ref[x, pl.ds(home, 1), span] = jnp.concatenate(
                    [mine[:, 2 * width : 3 * width].astype(BF16), ones], axis=1
                )[None]
                left = mine[:, 3 * width : 3 * width + chan]
                right = mine[:, 3 * width + chan :]
                glu.append(left / (1.0 + jnp.exp(-right)))
            glu_ref[pl.ds(home, 1), span] = jnp.concatenate(glu, axis=1).astype(BF16)[None]
            packed[half][side] = pre
        for x in range(nx):
            here = slice(x * half_length, (x + 1) * half_length)
            turned = jnp.concatenate([packed[half][0][here], packed[half][1][here]], axis=0).T
            extra = refs[0][x, column, half_length : half_length + 8].astype(F32)
            values = extra[0:1] + extra[1:2] + extra[2:3]
            offsets = jnp.where(core == 0, values[:, :length], values[:, length : 2 * length])
            offsets_f = jnp.where(
                core == 0, values[:, 2 * length : 3 * length], values[:, 3 * length : 4 * length]
            )
            at = row == 2 * x + home
            gate_pre = jnp.where(core == 0, turned[0:1], turned[1:2])
            forget_pre = jnp.where(core == 0, turned[2:3], turned[3:4])
            gate_in = jnp.where(at, gate_pre + offsets, gate_in)
            forget = jnp.where(at, forget_pre + offsets_f, forget)
    for b in range(ny):
        extra = own_a_ref[0, b, half_length : half_length + 8].astype(F32)
        memory_gain = extra[3:4] + extra[4:5] + extra[5:6]
        half = part // 2
        conv_gain = extra[6:7, :half] + extra[6:7, half:] + extra[7:8, :half]
        for at in range(2 * nx):
            gain_ref[b, at : at + 1] = jnp.concatenate(
                [
                    memory_gain[:, at * width : (at + 1) * width],
                    conv_gain[:, at * chan : (at + 1) * chan],
                    jnp.zeros((1, width - chan), F32),
                ],
                axis=1,
            )
    y = jnp.exp(-jnp.abs(forget))
    small = y * (1.0 - y * (1 / 2 - y * (1 / 3 - y * (1 / 4 - y * (1 / 5)))))
    gates_ref[0] = gate_in
    gates_ref[1] = jnp.minimum(forget, 0.0) - jnp.where(y < 0.03, small, jnp.log(1.0 + y))


def finish_kernel(place_ref, arrived_ref, own_ref, other_ref, gain_ref, out_ref, weight_ref):
    nx, nc, ny, length, lanes = arrived_ref.shape
    core, x_at = place_ref[1], place_ref[3]
    width = lanes // 2
    chan = width // 2
    part = out_ref.shape[1]
    lane = lax.broadcasted_iota(jnp.int32, (length, lanes), 1)
    is_memory = lane < width
    is_conv = (lane >= width) & (lane < width + chan)

    def block(x, c, b):
        got = arrived_ref[x, c, b].astype(F32)
        both = got + pltpu.roll(got, lanes - chan, 1)
        return jnp.where(is_memory, got, jnp.where(is_conv, both, 0.0))

    first = jnp.zeros((length, lanes), F32)
    second = jnp.zeros((length, lanes), F32)
    for x in range(nx):
        for c in range(nc):
            for b in range(ny):
                got = block(x, c, b)
                first = first + got
                second = second + got * got
    senders = nx * nc * ny
    memory_mean = jnp.sum(jnp.where(is_memory, second, 0.0), axis=1, keepdims=True)
    scale = lax.rsqrt(memory_mean / (senders * width) + EPS)
    mean = jnp.sum(jnp.where(is_conv, first, 0.0), axis=1, keepdims=True) / (senders * chan)
    power = jnp.sum(jnp.where(is_conv, second, 0.0), axis=1, keepdims=True) / (senders * chan)
    spread = lax.rsqrt(power - mean * mean + EPS)
    shift = jnp.where(is_memory, 0.0, mean)
    factor = jnp.where(is_memory, scale, spread)
    deep = weight_ref.shape[5]
    for ahead in range(nx):
        x = lax.rem(x_at + ahead, nx)
        for c, ref in ((core, own_ref), (1 - core, other_ref)):
            for b in range(ny):
                for near in range(ref.shape[2]):
                    weight_ref[b, near, pl.ds(x, 1), pl.ds(c, 1)] = ref[ahead, b, near][None, None]
    total = jnp.zeros((length, part), F32)
    for b in range(ny):
        left = []
        for c in range(nc):
            for x in range(nx):
                gain = gain_ref[b, c * nx + x : c * nx + x + 1]
                normed = (block(x, c, b) - shift) * factor * gain
                branch = normed / (1.0 + jnp.exp(-normed))
                used = jnp.where(is_memory, normed, branch).astype(BF16)
                left.append(used[:, : width + chan])
        total = total + dot(
            jnp.concatenate(left, axis=1), weight_ref[b].reshape(part, deep), NT
        )
    out_ref[...] = total.astype(BF16)


def convolve(glu_ref, prior, taps_ref, nx, core, x_at):
    nc, length, lanes = glu_ref.shape
    chan = lanes // nx
    group = nc * length
    glu = glu_ref[...].reshape(group, lanes).astype(F32)
    taps = taps_ref.shape[0]
    hold = 32
    lane = lax.broadcasted_iota(jnp.int32, (hold, lanes), 1)
    before = pltpu.roll(glu[group - hold :], chan, 1)
    prior = jnp.concatenate([prior, jnp.zeros((hold, lanes - chan), F32)], axis=1)
    extended = jnp.concatenate([jnp.where(lane < chan, prior, before), glu], axis=0)
    weights = taps_ref[...].astype(F32)
    weights = jnp.where(core == 0, weights[:, :lanes], weights[:, lanes:])
    weights = pltpu.roll(weights, lax.rem(lanes - chan * x_at, lanes), 1)
    weights = jnp.where(lax.broadcasted_iota(jnp.int32, weights.shape, 1) < chan, weights, 0.0)
    weights = sum(pltpu.roll(weights, chan * k, 1) for k in range(1, nx)) + weights
    total = jnp.zeros((group, lanes), F32)
    first = hold - (taps - 1)
    for shift in range(8):
        moved = extended[shift : shift + group + hold - 8] if shift else extended
        for j in range(taps):
            at = first + j
            if at % 8 == shift:
                total = total + moved[at - shift : at - shift + group] * weights[j : j + 1]
    high = total.astype(BF16)
    low = (total - high.astype(F32)).astype(BF16)
    sides = [slice(x * chan, (x + 1) * chan) for x in range(nx)]
    return [jnp.concatenate([high[:, mine], low[:, mine]], axis=1) for mine in sides]


def slab_kernel(
    qk_ref, v_ref, gate_ref, glu_ref, out_ref, q_ref, k_ref,
):
    chunks, length = gate_ref.shape[1], gate_ref.shape[2]
    width = qk_ref.shape[2] // 2
    gate, forget = gate_ref[0], gate_ref[1]
    within = lane_cumsum(forget)
    ends = [within[r : r + 1, length - 1 :] for r in range(chunks)]
    after = [jnp.zeros((1, 1), F32)]
    for r in range(chunks - 1, 0, -1):
        after.insert(0, after[0] + ends[r])
    total = after[0] + ends[0]
    to_end = jnp.concatenate([e + a for e, a in zip(ends, after)], axis=0)
    end_log = to_end - within + gate
    level = jnp.max(jnp.max(end_log, axis=1, keepdims=True), axis=0, keepdims=True)
    fresh = columns_of(jnp.exp(end_log - level))
    state = jnp.zeros((2 * width, width * qk_ref.shape[0]), F32)
    for r in range(chunks):
        q_ref[r * length : (r + 1) * length] = joined(qk_ref, 0, width, r, length)
        key = joined(qk_ref, width, width, r, length)
        k_ref[r * length : (r + 1) * length] = key
        scaled = (fresh[:, r : r + 1] * key.astype(F32)).astype(BF16)
        state = state + dot(v_ref[r * length : (r + 1) * length], scaled, TN)
    rows, head_lanes = out_ref.shape[1], out_ref.shape[2]
    kept = state[:rows]
    row = lax.broadcasted_iota(jnp.int32, kept.shape, 0)
    lane = lax.broadcasted_iota(jnp.int32, kept.shape, 1)
    for at, value in ((0, level), (3, total)):
        high = value.astype(BF16).astype(F32)
        mid = (value - high).astype(BF16).astype(F32)
        low = value - high - mid
        for k, part in enumerate((high, mid, low)):
            kept = jnp.where((row == width + 1) & (lane == at + k), part, kept)
    chan = glu_ref.shape[2] // qk_ref.shape[0]
    hold = 32
    tail = glu_ref[glu_ref.shape[0] - 1, length - hold :].astype(F32)[:, glu_ref.shape[2] - chan :]
    group = head_lanes // chan
    each = hold // group
    tail = jnp.concatenate([tail[g * each : (g + 1) * each] for g in range(group)], axis=1)
    kept = jnp.concatenate([kept[: width + 2], tail, kept[width + 2 + each :]], axis=0)
    kept = kept.astype(BF16)
    for j in range(out_ref.shape[0]):
        out_ref[j] = kept


def cell_kernel(place_ref, in_ref, q_ref, k_ref, v_ref, gate_ref, glu_ref, taps_ref, out_ref):
    chunks, length = gate_ref.shape[1], gate_ref.shape[2]
    members, rows, head = in_ref.shape
    width = out_ref.shape[4] // 2
    nc, ny = out_ref.shape[1], out_ref.shape[2]
    scale = head ** (-0.5)
    place = place_ref[0]
    chan = glu_ref.shape[2] // out_ref.shape[0]
    hold, group = 32, head // chan
    each = hold // group
    last_rows = in_ref[jnp.maximum(place - 1, 0), width : width + 8].astype(F32)
    last_rows = jnp.where(place > 0, last_rows[2 : 2 + each], 0.0)
    prior = jnp.concatenate([last_rows[:, g * chan : (g + 1) * chan] for g in range(group)], axis=0)
    conv = convolve(glu_ref, prior, taps_ref, out_ref.shape[0], place_ref[1], place_ref[3])
    acc = jnp.zeros((1, 1), F32)
    logs = [None] * members
    for j in range(members - 1, -1, -1):
        line = in_ref[j, width + 1 : width + 2, :128].astype(F32)
        level_j = line[:, 0:1] + line[:, 1:2] + line[:, 2:3]
        total_j = line[:, 3:4] + line[:, 4:5] + line[:, 5:6]
        before = j < place
        logs[j] = jnp.where(before, level_j + acc, LOW)
        acc = acc + jnp.where(before, total_j, 0.0)
    level = logs[0]
    for j in range(1, members):
        level = jnp.maximum(level, logs[j])
    state = jnp.zeros((rows, head), F32)
    for j in range(members):
        weight = jnp.where(j < place, jnp.exp(logs[j] - level), 0.0)
        state = state + weight * in_ref[j].astype(F32)
    state = jnp.concatenate([state, jnp.zeros((2 * width - rows, head), F32)], axis=0)
    gate, forget = gate_ref[0], gate_ref[1]
    within = lane_cumsum(forget)
    turned = columns_of(jnp.concatenate([within, gate], axis=0))
    causal = lax.broadcasted_iota(jnp.int32, (length, length), 0) >= lax.broadcasted_iota(
        jnp.int32, (length, length), 1
    )
    for r in range(chunks):
        here = slice(r * length, (r + 1) * length)
        query, key, value = q_ref[here], k_ref[here], v_ref[here]
        within_row, gate_row = within[r : r + 1], gate[r : r + 1]
        within_col = turned[:, r : r + 1]
        gate_col = turned[:, chunks + r : chunks + r + 1]
        log_weight = jnp.where(causal, within_col - within_row + gate_row, -jnp.inf)
        carried = within_col + level
        top = jnp.maximum(carried, jnp.max(log_weight, axis=1, keepdims=True))
        weight = jnp.exp(log_weight - top)
        carried_weight = jnp.exp(carried - top) * scale
        scores = dot(query, key, NT) * (scale * weight)
        older = dot(query, state.astype(BF16), NT)
        numer = dot(scores.astype(BF16), value, NN) + carried_weight * older
        denom = jnp.sum(scores, axis=1, keepdims=True) + carried_weight * older[:, width : width + 1]
        result = numer[:, :width] / jnp.maximum(jnp.abs(denom), 1.0)
        x, c = r // nc, r % nc
        sent = jnp.concatenate(
            [result.astype(BF16), conv[x][c * length : (c + 1) * length]], axis=1
        )
        for y in range(ny):
            out_ref[x, c, y] = sent
        last = within_row[:, length - 1 :]
        end_row = last - within_row + gate_row
        new_level = jnp.maximum(last + level, jnp.max(end_row, axis=1, keepdims=True))
        keep = jnp.exp(last + level - new_level)
        fresh = jnp.exp(last - within_col + gate_col - new_level)
        scaled = (fresh * key.astype(F32)).astype(BF16)
        state = keep * state + dot(value, scaled, TN)
        level = new_level


def vmem(count):
    return [pl.BlockSpec(memory_space=pltpu.VMEM)] * count


def layer(
    tokens,
    conv_value_weight,
    conv_gate_weight,
    conv_kernel,
    conv_norm_gain,
    query_weight,
    key_weight,
    value_weight,
    input_gate_weight,
    forget_gate_weight,
    input_offset,
    forget_offset,
    memory_norm_gain,
    conv_out_weight,
    memory_out_weight,
):
    nzh, nzl, nx, nc, ny = (size(a) for a in AXES)
    xi, ci, yi = lax.axis_index("x"), lax.axis_index("c"), lax.axis_index("tp")
    members = nzh * nzl
    zi = lax.axis_index("zh") * nzl + lax.axis_index("zl")
    length, part = tokens.shape
    slab = length * nx * nc
    head = query_weight.shape[1] // nc
    width = head // nx
    chan = conv_value_weight.shape[1] // nc // nx
    rows = query_weight.shape[0]
    wide = 3 * width + 2 * chan

    def from_z(value, ahead):
        return lax.ppermute(value, Z, [(j, (j - ahead) % members) for j in range(members)])

    deep = memory_out_weight.shape[0] + conv_out_weight.shape[0]
    pieces, out_rows = pl.pallas_call(
        piece_kernel,
        out_shape=(
            jax.ShapeDtypeStruct((nx, nc, rows, wide), BF16),
            jax.ShapeDtypeStruct((rows, deep), BF16),
        ),
        in_specs=vmem(7),
        out_specs=vmem(2),
        interpret=INTERPRET,
        name="pieces",
    )(
        query_weight,
        key_weight,
        value_weight,
        conv_value_weight,
        conv_gate_weight,
        memory_out_weight,
        conv_out_weight,
    )
    turned = lax.ppermute(
        out_rows,
        ("zh", "tp"),
        [(a * ny + b, b * ny + a) for a in range(nzh) for b in range(ny)],
    )
    offsets = jnp.concatenate([input_offset.T, forget_offset.T], axis=0)
    half = length // 2
    upper, lower = pl.pallas_call(
        pack_kernel,
        out_shape=(
            jax.ShapeDtypeStruct((nx * ny, half + 8, part), BF16),
            jax.ShapeDtypeStruct((nx * ny, half, part), BF16),
        ),
        in_specs=vmem(4),
        out_specs=vmem(2),
        interpret=INTERPRET,
        name="pack",
    )(tokens, offsets, conv_norm_gain[None], memory_norm_gain[None])
    mine = exchange(pieces.reshape(nx * nc, rows, wide), ("x", "c"))
    mine = mine.reshape(nx * nc * rows, wide)
    upper, lower, mine = lax.optimization_barrier((upper, lower, mine))
    own_a = exchange(upper, ("x", "tp"))
    turned = jnp.concatenate([turned[:, j * wide : (j + 1) * wide] for j in range(deep // wide)], 0)
    mine = jnp.concatenate([mine, turned], axis=0)
    step, cut = members // 4, mine.shape[0] // 2
    far = [
        from_z(mine, -step),
        from_z(mine, step),
        from_z(mine[:cut], 2 * step),
        from_z(mine[cut:], -2 * step),
    ]
    near = jnp.stack([far[0], mine, far[1], jnp.concatenate(far[2:], axis=0)], axis=0)
    near, lower, own_a = lax.optimization_barrier((near, lower, own_a))
    own_b = exchange(lower, ("x", "tp"))
    sets = [near, from_z(near, 1), from_z(near, -1)]
    sets += [from_z(near[1:3], 2), from_z(near[:2], -2)]
    own_a = own_a.reshape(nx, ny, half + 8, part)
    own_b = own_b.reshape(nx, ny, half, part)
    others = [swapped(own_a, "c")]
    others.append(swapped(own_b, "c"))

    gate_weight = jnp.pad(
        jnp.concatenate([input_gate_weight, forget_gate_weight], axis=1), ((0, 0), (0, 124))
    )
    place = jnp.stack([zi, ci, yi, xi])
    smem = pl.BlockSpec(memory_space=pltpu.SMEM)
    qk, value, packed, gates, gain, out_part = pl.pallas_call(
        project_kernel,
        out_shape=(
            jax.ShapeDtypeStruct((nx, nx, nc, length, 2 * width), BF16),
            jax.ShapeDtypeStruct((nx, nc, length, 2 * width), BF16),
            jax.ShapeDtypeStruct((nc, length, nx * chan), BF16),
            jax.ShapeDtypeStruct((2, nx * nc, length), F32),
            jax.ShapeDtypeStruct((ny, nc * nx, 2 * width), F32),
            jax.ShapeDtypeStruct((nzh, nzl, rows, deep), BF16),
        ),
        in_specs=[smem] + vmem(10),
        out_specs=vmem(6),
        interpret=INTERPRET,
        name="project",
    )(place, own_a, own_b, *others, *sets, gate_weight)
    value = value.reshape(slab, 2 * width)
    all_qk = exchange(qk.reshape(nx, slab, 2 * width), "x")
    out_part, all_qk = lax.optimization_barrier((out_part, all_qk))
    out_parts = [out_part] + [
        lax.ppermute(out_part, "x", [(j, (j - ahead) % nx) for j in range(nx)])
        for ahead in range(1, nx)
    ]
    own_out = jnp.stack(out_parts, axis=0)
    other_out = swapped(own_out, "c")

    state_rows = width + 8
    states, query, key = pl.pallas_call(
        slab_kernel,
        out_shape=(
            jax.ShapeDtypeStruct((members, state_rows, head), BF16),
            jax.ShapeDtypeStruct((slab, head), BF16),
            jax.ShapeDtypeStruct((slab, head), BF16),
        ),
        in_specs=vmem(4),
        out_specs=vmem(3),
        interpret=INTERPRET,
        name="slab_state",
    )(all_qk, value, gates, packed)
    states = exchange(states, Z)
    last = pl.pallas_call(
        cell_kernel,
        out_shape=jax.ShapeDtypeStruct((nx, nc, ny, length, 2 * width), BF16),
        in_specs=[smem] + vmem(7),
        out_specs=pl.BlockSpec(memory_space=pltpu.VMEM),
        interpret=INTERPRET,
        name="cell",
    )(place, states, query, key, value, gates, packed, conv_kernel)
    arrived = exchange(last.reshape(nx * nc * ny, length, -1), ("x", "c", "tp"))
    arrived = arrived.reshape(nx, nc, ny, length, -1)
    return pl.pallas_call(
        finish_kernel,
        out_shape=jax.ShapeDtypeStruct((length, part), BF16),
        in_specs=[smem] + vmem(4),
        out_specs=pl.BlockSpec(memory_space=pltpu.VMEM),
        scratch_shapes=[pltpu.VMEM((ny, nzl, nx, nc, rows, deep), BF16)],
        interpret=INTERPRET,
        name="finish",
    )(place, arrived, own_out, other_out, gain)


def solution(mesh):
    shape = mesh.shape
    depth = shape["sp"] // 32
    split = Mesh(mesh.devices.reshape(4, depth, 4, 2, shape["tp"]), AXES)
    in_specs = (
        P(SP, "tp"),
        P(SP, "tp"),
        P(SP, "tp"),
        P(None, "tp"),
        P("tp"),
        P(SP, "tp"),
        P(SP, "tp"),
        P(SP, "tp"),
        P(None, "tp"),
        P(None, "tp"),
        P(SP, "tp"),
        P(SP, "tp"),
        P("tp"),
        P("tp", SP),
        P("tp", SP),
    )
    return jax.shard_map(
        layer, mesh=split, in_specs=in_specs, out_specs=P(SP, "tp"), check_vma=False
    )
```

```python
import jax
import jax.numpy as jnp
from jax import lax
from jax.experimental import pallas as pl
from jax.experimental.pallas import tpu as pltpu
from jax.sharding import Mesh
from jax.sharding import PartitionSpec as P

AXES = ("zh", "zl", "x", "c", "tp")
Z = ("zh", "zl")
SP = ("zh", "zl", "x", "c")
EPS = 1e-06
LOW = -1e30
F32 = jnp.float32
BF16 = jnp.bfloat16
INTERPRET = False


def size(axis):
    return lax.axis_size(axis)


def exchange(pieces, axes):
    return lax.all_to_all(pieces, axes, split_axis=0, concat_axis=0, tiled=True)


def swapped(value, axis):
    return lax.ppermute(value, axis, [(0, 1), (1, 0)])


def lane_cumsum(rows):
    lane = lax.broadcasted_iota(jnp.int32, rows.shape, 1)
    step = 1
    while step < rows.shape[1]:
        moved = pltpu.roll(rows, step, 1)
        rows = rows + jnp.where(lane >= step, moved, 0.0)
        step *= 2
    return rows


def columns_of(rows):
    count, length = rows.shape
    square = jnp.concatenate([rows, jnp.zeros((length - count, length), F32)], axis=0)
    return square.T


def dot(a, b, dims):
    return lax.dot_general(a, b, (dims, ((), ())), preferred_element_type=F32)


NN = ((1,), (0,))
NT = ((1,), (1,))
TN = ((0,), (0,))


def joined(parts_ref, start, width, chunk, length):
    picked = [
        parts_ref[j, chunk * length : (chunk + 1) * length, start : start + width]
        for j in range(parts_ref.shape[0])
    ]
    return jnp.concatenate(picked, axis=1)


def three_parts(value):
    high = value.astype(BF16).astype(F32)
    mid = (value - high).astype(BF16).astype(F32)
    return high, mid, value - high - mid


def pack_kernel(tokens_ref, offsets_ref, conv_gain_ref, memory_gain_ref, out_ref):
    length = tokens_ref.shape[0]
    offsets = three_parts(offsets_ref[...])
    conv_gain = three_parts(conv_gain_ref[...])
    memory_gain = three_parts(memory_gain_ref[...])
    rows = [jnp.concatenate([p[k : k + 1] for k in range(p.shape[0])], axis=1) for p in offsets]
    rows += memory_gain
    rows.append(jnp.concatenate(conv_gain[:2], axis=1))
    rows.append(jnp.concatenate([conv_gain[2], jnp.zeros_like(conv_gain[2])], axis=1))
    extra = jnp.concatenate(rows, axis=0).astype(BF16)
    tokens = tokens_ref[...]
    for j in range(out_ref.shape[0]):
        out_ref[j, :length] = tokens
        out_ref[j, length:] = extra


def piece_kernel(
    query_ref, key_ref, value_ref, left_ref, right_ref, memory_ref, conv_ref, out_ref, turn_ref
):
    nx, nc = out_ref.shape[0], out_ref.shape[1]
    rows = memory_ref.shape[0]
    width, chan = memory_ref.shape[1] // (nx * nc), conv_ref.shape[1] // (nx * nc)
    parts = []
    for at in range(nx * nc):
        parts.append(memory_ref[:, at * width : (at + 1) * width])
        parts.append(conv_ref[:, at * chan : (at + 1) * chan])
    whole = jnp.concatenate(parts, axis=1)
    wide = out_ref.shape[3]
    for j in range(whole.shape[1] // wide):
        turn_ref[j * rows : (j + 1) * rows] = whole[:, j * wide : (j + 1) * wide]
    for x in range(nx):
        for c in range(nc):
            at = c * nx + x
            parts = []
            for ref in (query_ref, key_ref, value_ref, left_ref, right_ref):
                width = ref.shape[1] // (nx * nc)
                parts.append(ref[:, at * width : (at + 1) * width])
            out_ref[x, c] = jnp.concatenate(parts, axis=1)


def project_kernel(
    place_ref, own_ref, other_ref,
    w0_ref, w1_ref, w3_ref, low_ref, high_ref, gate_ref,
    qk_ref, v_ref, glu_ref, gates_ref, gain_ref, out_weight_ref,
):
    nx, ny, _, part = own_ref.shape
    far, tall, wide = w0_ref.shape
    depth, chunks = out_weight_ref.shape[2], out_weight_ref.shape[3] // wide
    rows = tall - depth * chunks
    close = part // rows
    length = glu_ref.shape[1]
    place, core, column = place_ref[0], place_ref[1], place_ref[2]
    tokens_rows = nx * length
    width = qk_ref.shape[4] // 2
    chan = glu_ref.shape[2] // nx
    lane = lax.broadcasted_iota(jnp.int32, (length, width), 1)
    ones = jnp.where(lane == 0, 1.0, 0.0).astype(BF16)
    row = lax.broadcasted_iota(jnp.int32, (2 * nx, length), 0)
    gate_in = jnp.zeros((2 * nx, length), F32)
    forget = jnp.zeros((2 * nx, length), F32)

    blocks = [
        (ref, i, ahead, i)
        for ref, ahead in ((w0_ref, 0), (w1_ref, 1), (w3_ref, close - 1))
        for i in range(far)
    ]
    blocks += [(low_ref, i, 2, i) for i in range(far // 2)]
    blocks += [(high_ref, i, 2, i + far // 2) for i in range(far // 2)]
    homes = []
    for ref, i, ahead, y in blocks:
        homes.append((y, lax.rem(place + ahead, close)))
        out_weight_ref[y, pl.ds(homes[-1][1], 1)] = jnp.concatenate(
            [ref[i, rows + j * depth : rows + (j + 1) * depth] for j in range(chunks)], axis=1
        )[None]
    for half, ref in enumerate((own_ref, other_ref)):
        home = core if half == 0 else 1 - core
        acc = jnp.zeros((tokens_rows, wide), F32)
        pre = jnp.zeros((tokens_rows, gate_ref.shape[1]), F32)
        for pair in range(0, len(blocks), 2):
            left, right, gate_rows = [], [], []
            for at in (pair, pair + 1):
                w_ref, i, _, _ = blocks[at]
                y, z = homes[at]
                start = pl.multiple_of(z * rows, rows)
                left.append(ref[:, y, :length, pl.ds(start, rows)].reshape(tokens_rows, rows))
                right.append(w_ref[i, :rows])
                gate_rows.append(gate_ref[pl.ds(y * part + start, rows)])
            lhs = jnp.concatenate(left, axis=1)
            acc = acc + dot(lhs, jnp.concatenate(right, axis=0), NN)
            pre = pre + dot(lhs, jnp.concatenate(gate_rows, axis=0), NN)
        glu = []
        for x in range(nx):
            mine = acc[x * length : (x + 1) * length]
            qk = mine[:, : 2 * width].astype(BF16)[None]
            for j in range(qk_ref.shape[0]):
                qk_ref[j, x, pl.ds(home, 1)] = qk
            v_ref[x, pl.ds(home, 1)] = jnp.concatenate(
                [mine[:, 2 * width : 3 * width].astype(BF16), ones], axis=1
            )[None]
            left = mine[:, 3 * width : 3 * width + chan]
            right = mine[:, 3 * width + chan :]
            glu.append(left / (1.0 + jnp.exp(-right)))
        glu_ref[pl.ds(home, 1)] = jnp.concatenate(glu, axis=1).astype(BF16)[None]
        for x in range(nx):
            turned = pre[x * length : (x + 1) * length].T
            extra = ref[x, column, length : length + 8].astype(F32)
            values = extra[0:1] + extra[1:2] + extra[2:3]
            offsets = jnp.where(core == 0, values[:, :length], values[:, length : 2 * length])
            offsets_f = jnp.where(
                core == 0, values[:, 2 * length : 3 * length], values[:, 3 * length : 4 * length]
            )
            at = row == 2 * x + home
            gate_pre = jnp.where(core == 0, turned[0:1], turned[1:2])
            forget_pre = jnp.where(core == 0, turned[2:3], turned[3:4])
            gate_in = jnp.where(at, gate_pre + offsets, gate_in)
            forget = jnp.where(at, forget_pre + offsets_f, forget)
    for b in range(ny):
        extra = own_ref[0, b, length : length + 8].astype(F32)
        memory_gain = extra[3:4] + extra[4:5] + extra[5:6]
        half = part // 2
        conv_gain = extra[6:7, :half] + extra[6:7, half:] + extra[7:8, :half]
        for at in range(2 * nx):
            gain_ref[b, at : at + 1] = jnp.concatenate(
                [
                    memory_gain[:, at * width : (at + 1) * width],
                    conv_gain[:, at * chan : (at + 1) * chan],
                    jnp.zeros((1, width - chan), F32),
                ],
                axis=1,
            )
    y = jnp.exp(-jnp.abs(forget))
    small = y * (1.0 - y * (1 / 2 - y * (1 / 3 - y * (1 / 4 - y * (1 / 5)))))
    gates_ref[0] = gate_in
    gates_ref[1] = jnp.minimum(forget, 0.0) - jnp.where(y < 0.03, small, jnp.log(1.0 + y))


def finish_kernel(place_ref, arrived_ref, own_ref, other_ref, gain_ref, out_ref, weight_ref):
    nx, nc, ny, length, lanes = arrived_ref.shape
    core, x_at = place_ref[1], place_ref[3]
    width = lanes // 2
    chan = width // 2
    part = out_ref.shape[1]
    lane = lax.broadcasted_iota(jnp.int32, (length, lanes), 1)
    is_memory = lane < width
    is_conv = (lane >= width) & (lane < width + chan)

    def block(x, c, b):
        got = arrived_ref[x, c, b].astype(F32)
        both = got + pltpu.roll(got, lanes - chan, 1)
        return jnp.where(is_memory, got, jnp.where(is_conv, both, 0.0))

    first = jnp.zeros((length, lanes), F32)
    second = jnp.zeros((length, lanes), F32)
    for x in range(nx):
        for c in range(nc):
            for b in range(ny):
                got = block(x, c, b)
                first = first + got
                second = second + got * got
    senders = nx * nc * ny
    memory_mean = jnp.sum(jnp.where(is_memory, second, 0.0), axis=1, keepdims=True)
    scale = lax.rsqrt(memory_mean / (senders * width) + EPS)
    mean = jnp.sum(jnp.where(is_conv, first, 0.0), axis=1, keepdims=True) / (senders * chan)
    power = jnp.sum(jnp.where(is_conv, second, 0.0), axis=1, keepdims=True) / (senders * chan)
    spread = lax.rsqrt(power - mean * mean + EPS)
    shift = jnp.where(is_memory, 0.0, mean)
    factor = jnp.where(is_memory, scale, spread)
    deep = weight_ref.shape[5]
    for ahead in range(nx):
        x = lax.rem(x_at + ahead, nx)
        for c, ref in ((core, own_ref), (1 - core, other_ref)):
            for b in range(ny):
                for near in range(ref.shape[2]):
                    weight_ref[b, near, pl.ds(x, 1), pl.ds(c, 1)] = ref[ahead, b, near][None, None]
    total = jnp.zeros((length, part), F32)
    for b in range(ny):
        left = []
        for c in range(nc):
            for x in range(nx):
                gain = gain_ref[b, c * nx + x : c * nx + x + 1]
                normed = (block(x, c, b) - shift) * factor * gain
                branch = normed / (1.0 + jnp.exp(-normed))
                used = jnp.where(is_memory, normed, branch).astype(BF16)
                left.append(used[:, : width + chan])
        total = total + dot(
            jnp.concatenate(left, axis=1), weight_ref[b].reshape(part, deep), NT
        )
    out_ref[...] = total.astype(BF16)


def convolve(glu_ref, prior, taps_ref, nx, core, x_at):
    nc, length, lanes = glu_ref.shape
    chan = lanes // nx
    group = nc * length
    glu = glu_ref[...].reshape(group, lanes).astype(F32)
    taps = taps_ref.shape[0]
    hold = 32
    lane = lax.broadcasted_iota(jnp.int32, (hold, lanes), 1)
    before = pltpu.roll(glu[group - hold :], chan, 1)
    prior = jnp.concatenate([prior, jnp.zeros((hold, lanes - chan), F32)], axis=1)
    extended = jnp.concatenate([jnp.where(lane < chan, prior, before), glu], axis=0)
    weights = taps_ref[...].astype(F32)
    weights = jnp.where(core == 0, weights[:, :lanes], weights[:, lanes:])
    weights = pltpu.roll(weights, lax.rem(lanes - chan * x_at, lanes), 1)
    weights = jnp.where(lax.broadcasted_iota(jnp.int32, weights.shape, 1) < chan, weights, 0.0)
    weights = sum(pltpu.roll(weights, chan * k, 1) for k in range(1, nx)) + weights
    total = jnp.zeros((group, lanes), F32)
    first = hold - (taps - 1)
    for shift in range(8):
        moved = extended[shift : shift + group + hold - 8] if shift else extended
        for j in range(taps):
            at = first + j
            if at % 8 == shift:
                total = total + moved[at - shift : at - shift + group] * weights[j : j + 1]
    high = total.astype(BF16)
    low = (total - high.astype(F32)).astype(BF16)
    sides = [slice(x * chan, (x + 1) * chan) for x in range(nx)]
    return [jnp.concatenate([high[:, mine], low[:, mine]], axis=1) for mine in sides]


def slab_kernel(
    qk_ref, v_ref, gate_ref, glu_ref, out_ref, q_ref, k_ref,
):
    chunks, length = gate_ref.shape[1], gate_ref.shape[2]
    width = qk_ref.shape[2] // 2
    gate, forget = gate_ref[0], gate_ref[1]
    within = lane_cumsum(forget)
    ends = [within[r : r + 1, length - 1 :] for r in range(chunks)]
    after = [jnp.zeros((1, 1), F32)]
    for r in range(chunks - 1, 0, -1):
        after.insert(0, after[0] + ends[r])
    total = after[0] + ends[0]
    to_end = jnp.concatenate([e + a for e, a in zip(ends, after)], axis=0)
    end_log = to_end - within + gate
    level = jnp.max(jnp.max(end_log, axis=1, keepdims=True), axis=0, keepdims=True)
    fresh = columns_of(jnp.exp(end_log - level))
    state = jnp.zeros((2 * width, width * qk_ref.shape[0]), F32)
    for r in range(chunks):
        q_ref[r * length : (r + 1) * length] = joined(qk_ref, 0, width, r, length)
        key = joined(qk_ref, width, width, r, length)
        k_ref[r * length : (r + 1) * length] = key
        scaled = (fresh[:, r : r + 1] * key.astype(F32)).astype(BF16)
        state = state + dot(v_ref[r * length : (r + 1) * length], scaled, TN)
    rows, head_lanes = out_ref.shape[1], out_ref.shape[2]
    kept = state[:rows]
    row = lax.broadcasted_iota(jnp.int32, kept.shape, 0)
    lane = lax.broadcasted_iota(jnp.int32, kept.shape, 1)
    for at, value in ((0, level), (3, total)):
        high = value.astype(BF16).astype(F32)
        mid = (value - high).astype(BF16).astype(F32)
        low = value - high - mid
        for k, part in enumerate((high, mid, low)):
            kept = jnp.where((row == width + 1) & (lane == at + k), part, kept)
    chan = glu_ref.shape[2] // qk_ref.shape[0]
    hold = 32
    tail = glu_ref[glu_ref.shape[0] - 1, length - hold :].astype(F32)[:, glu_ref.shape[2] - chan :]
    group = head_lanes // chan
    each = hold // group
    tail = jnp.concatenate([tail[g * each : (g + 1) * each] for g in range(group)], axis=1)
    kept = jnp.concatenate([kept[: width + 2], tail, kept[width + 2 + each :]], axis=0)
    kept = kept.astype(BF16)
    for j in range(out_ref.shape[0]):
        out_ref[j] = kept


def cell_kernel(place_ref, in_ref, q_ref, k_ref, v_ref, gate_ref, glu_ref, taps_ref, out_ref):
    chunks, length = gate_ref.shape[1], gate_ref.shape[2]
    members, rows, head = in_ref.shape
    width = out_ref.shape[4] // 2
    nc, ny = out_ref.shape[1], out_ref.shape[2]
    scale = head ** (-0.5)
    place = place_ref[0]
    chan = glu_ref.shape[2] // out_ref.shape[0]
    hold, group = 32, head // chan
    each = hold // group
    last_rows = in_ref[jnp.maximum(place - 1, 0), width : width + 8].astype(F32)
    last_rows = jnp.where(place > 0, last_rows[2 : 2 + each], 0.0)
    prior = jnp.concatenate([last_rows[:, g * chan : (g + 1) * chan] for g in range(group)], axis=0)
    conv = convolve(glu_ref, prior, taps_ref, out_ref.shape[0], place_ref[1], place_ref[3])
    acc = jnp.zeros((1, 1), F32)
    logs = [None] * members
    for j in range(members - 1, -1, -1):
        line = in_ref[j, width + 1 : width + 2, :128].astype(F32)
        level_j = line[:, 0:1] + line[:, 1:2] + line[:, 2:3]
        total_j = line[:, 3:4] + line[:, 4:5] + line[:, 5:6]
        before = j < place
        logs[j] = jnp.where(before, level_j + acc, LOW)
        acc = acc + jnp.where(before, total_j, 0.0)
    level = logs[0]
    for j in range(1, members):
        level = jnp.maximum(level, logs[j])
    state = jnp.zeros((rows, head), F32)
    for j in range(members):
        weight = jnp.where(j < place, jnp.exp(logs[j] - level), 0.0)
        state = state + weight * in_ref[j].astype(F32)
    state = jnp.concatenate([state, jnp.zeros((2 * width - rows, head), F32)], axis=0)
    gate, forget = gate_ref[0], gate_ref[1]
    within = lane_cumsum(forget)
    turned = columns_of(jnp.concatenate([within, gate], axis=0))
    causal = lax.broadcasted_iota(jnp.int32, (length, length), 0) >= lax.broadcasted_iota(
        jnp.int32, (length, length), 1
    )
    for r in range(chunks):
        here = slice(r * length, (r + 1) * length)
        query, key, value = q_ref[here], k_ref[here], v_ref[here]
        within_row, gate_row = within[r : r + 1], gate[r : r + 1]
        within_col = turned[:, r : r + 1]
        gate_col = turned[:, chunks + r : chunks + r + 1]
        log_weight = jnp.where(causal, within_col - within_row + gate_row, -jnp.inf)
        carried = within_col + level
        top = jnp.maximum(carried, jnp.max(log_weight, axis=1, keepdims=True))
        weight = jnp.exp(log_weight - top)
        carried_weight = jnp.exp(carried - top) * scale
        scores = dot(query, key, NT) * (scale * weight)
        older = dot(query, state.astype(BF16), NT)
        numer = dot(scores.astype(BF16), value, NN) + carried_weight * older
        denom = jnp.sum(scores, axis=1, keepdims=True) + carried_weight * older[:, width : width + 1]
        result = numer[:, :width] / jnp.maximum(jnp.abs(denom), 1.0)
        x, c = r // nc, r % nc
        sent = jnp.concatenate(
            [result.astype(BF16), conv[x][c * length : (c + 1) * length]], axis=1
        )
        for y in range(ny):
            out_ref[x, c, y] = sent
        last = within_row[:, length - 1 :]
        end_row = last - within_row + gate_row
        new_level = jnp.maximum(last + level, jnp.max(end_row, axis=1, keepdims=True))
        keep = jnp.exp(last + level - new_level)
        fresh = jnp.exp(last - within_col + gate_col - new_level)
        scaled = (fresh * key.astype(F32)).astype(BF16)
        state = keep * state + dot(value, scaled, TN)
        level = new_level


def vmem(count):
    return [pl.BlockSpec(memory_space=pltpu.VMEM)] * count


def layer(
    tokens,
    conv_value_weight,
    conv_gate_weight,
    conv_kernel,
    conv_norm_gain,
    query_weight,
    key_weight,
    value_weight,
    input_gate_weight,
    forget_gate_weight,
    input_offset,
    forget_offset,
    memory_norm_gain,
    conv_out_weight,
    memory_out_weight,
):
    nzh, nzl, nx, nc, ny = (size(a) for a in AXES)
    xi, ci, yi = lax.axis_index("x"), lax.axis_index("c"), lax.axis_index("tp")
    members = nzh * nzl
    zi = lax.axis_index("zh") * nzl + lax.axis_index("zl")
    length, part = tokens.shape
    slab = length * nx * nc
    head = query_weight.shape[1] // nc
    width = head // nx
    chan = conv_value_weight.shape[1] // nc // nx
    rows = query_weight.shape[0]
    wide = 3 * width + 2 * chan

    def from_z(value, ahead):
        return lax.ppermute(value, Z, [(j, (j - ahead) % members) for j in range(members)])

    deep = memory_out_weight.shape[0] + conv_out_weight.shape[0]
    pieces, out_rows = pl.pallas_call(
        piece_kernel,
        out_shape=(
            jax.ShapeDtypeStruct((nx, nc, rows, wide), BF16),
            jax.ShapeDtypeStruct((deep // wide * rows, wide), BF16),
        ),
        in_specs=vmem(7),
        out_specs=vmem(2),
        interpret=INTERPRET,
        name="pieces",
    )(
        query_weight,
        key_weight,
        value_weight,
        conv_value_weight,
        conv_gate_weight,
        memory_out_weight.T,
        conv_out_weight.T,
    )
    turned = lax.ppermute(
        out_rows,
        ("zh", "tp"),
        [(a * ny + b, b * ny + a) for a in range(nzh) for b in range(ny)],
    )
    offsets = jnp.concatenate([input_offset.T, forget_offset.T], axis=0)
    sent = pl.pallas_call(
        pack_kernel,
        out_shape=jax.ShapeDtypeStruct((nx * ny, length + 8, part), BF16),
        in_specs=vmem(4),
        out_specs=pl.BlockSpec(memory_space=pltpu.VMEM),
        interpret=INTERPRET,
        name="pack",
    )(tokens, offsets, conv_norm_gain[None], memory_norm_gain[None])
    mine = exchange(pieces.reshape(nx * nc, rows, wide), ("x", "c"))
    mine = mine.reshape(nx * nc * rows, wide)
    mine = jnp.concatenate([mine, turned], axis=0)
    near = exchange(jnp.broadcast_to(mine, (nzh, *mine.shape)), "zh")
    own = exchange(sent, ("x", "tp")).reshape(nx, ny, length + 8, part)
    sets = [near, from_z(near, 1), from_z(near, -1)]
    sets += [from_z(near[: nzh // 2], 2), from_z(near[nzh // 2 :], -2)]
    other = swapped(own, "c")

    gate_weight = jnp.pad(
        jnp.concatenate([input_gate_weight, forget_gate_weight], axis=1), ((0, 0), (0, 124))
    )
    place = jnp.stack([zi, ci, yi, xi])
    smem = pl.BlockSpec(memory_space=pltpu.SMEM)
    qk, value, packed, gates, gain, out_part = pl.pallas_call(
        project_kernel,
        out_shape=(
            jax.ShapeDtypeStruct((nx, nx, nc, length, 2 * width), BF16),
            jax.ShapeDtypeStruct((nx, nc, length, 2 * width), BF16),
            jax.ShapeDtypeStruct((nc, length, nx * chan), BF16),
            jax.ShapeDtypeStruct((2, nx * nc, length), F32),
            jax.ShapeDtypeStruct((ny, nc * nx, 2 * width), F32),
            jax.ShapeDtypeStruct((nzh, nzl, rows, deep), BF16),
        ),
        in_specs=[smem] + vmem(8),
        out_specs=vmem(6),
        interpret=INTERPRET,
        name="project",
    )(place, own, other, *sets, gate_weight)
    value = value.reshape(slab, 2 * width)
    all_qk = exchange(qk.reshape(nx, slab, 2 * width), "x")
    out_part, all_qk = lax.optimization_barrier((out_part, all_qk))
    out_parts = [out_part] + [
        lax.ppermute(out_part, "x", [(j, (j - ahead) % nx) for j in range(nx)])
        for ahead in range(1, nx)
    ]
    own_out = jnp.stack(out_parts, axis=0)
    other_out = swapped(own_out, "c")

    state_rows = width + 8
    states, query, key = pl.pallas_call(
        slab_kernel,
        out_shape=(
            jax.ShapeDtypeStruct((members, state_rows, head), BF16),
            jax.ShapeDtypeStruct((slab, head), BF16),
            jax.ShapeDtypeStruct((slab, head), BF16),
        ),
        in_specs=vmem(4),
        out_specs=vmem(3),
        interpret=INTERPRET,
        name="slab_state",
    )(all_qk, value, gates, packed)
    states = exchange(states, Z)
    last = pl.pallas_call(
        cell_kernel,
        out_shape=jax.ShapeDtypeStruct((nx, nc, ny, length, 2 * width), BF16),
        in_specs=[smem] + vmem(7),
        out_specs=pl.BlockSpec(memory_space=pltpu.VMEM),
        interpret=INTERPRET,
        name="cell",
    )(place, states, query, key, value, gates, packed, conv_kernel)
    arrived = exchange(last.reshape(nx * nc * ny, length, -1), ("x", "c", "tp"))
    arrived = arrived.reshape(nx, nc, ny, length, -1)
    return pl.pallas_call(
        finish_kernel,
        out_shape=jax.ShapeDtypeStruct((length, part), BF16),
        in_specs=[smem] + vmem(4),
        out_specs=pl.BlockSpec(memory_space=pltpu.VMEM),
        scratch_shapes=[pltpu.VMEM((ny, nzl, nx, nc, rows, deep), BF16)],
        interpret=INTERPRET,
        name="finish",
    )(place, arrived, own_out, other_out, gain)


def solution(mesh):
    shape = mesh.shape
    depth = shape["sp"] // 32
    split = Mesh(mesh.devices.reshape(4, depth, 4, 2, shape["tp"]), AXES)
    in_specs = (
        P(SP, "tp"),
        P(SP, "tp"),
        P(SP, "tp"),
        P(None, "tp"),
        P("tp"),
        P(SP, "tp"),
        P(SP, "tp"),
        P(SP, "tp"),
        P(None, "tp"),
        P(None, "tp"),
        P(SP, "tp"),
        P(SP, "tp"),
        P("tp"),
        P("tp", SP),
        P("tp", SP),
    )
    return jax.shard_map(
        layer, mesh=split, in_specs=in_specs, out_specs=P(SP, "tp"), check_vma=False
    )
```

```python
import jax
import jax.numpy as jnp
from jax import lax
from jax.experimental import pallas as pl
from jax.experimental.pallas import tpu as pltpu
from jax.sharding import Mesh
from jax.sharding import PartitionSpec as P

AXES = ("zh", "zl", "x", "c", "tp")
Z = ("zh", "zl")
SP = ("zh", "zl", "x", "c")
EPS = 1e-06
LOW = -1e30
F32 = jnp.float32
BF16 = jnp.bfloat16
INTERPRET = False


def size(axis):
    return lax.axis_size(axis)


def exchange(pieces, axes):
    return lax.all_to_all(pieces, axes, split_axis=0, concat_axis=0, tiled=True)


def swapped(value, axis):
    return lax.ppermute(value, axis, [(0, 1), (1, 0)])


def lane_cumsum(rows):
    lane = lax.broadcasted_iota(jnp.int32, rows.shape, 1)
    step = 1
    while step < rows.shape[1]:
        moved = pltpu.roll(rows, step, 1)
        rows = rows + jnp.where(lane >= step, moved, 0.0)
        step *= 2
    return rows


def columns_of(rows):
    count, length = rows.shape
    square = jnp.concatenate([rows, jnp.zeros((length - count, length), F32)], axis=0)
    return square.T


def dot(a, b, dims):
    return lax.dot_general(a, b, (dims, ((), ())), preferred_element_type=F32)


NN = ((1,), (0,))
NT = ((1,), (1,))
TN = ((0,), (0,))


def joined(parts_ref, start, width, chunk, length):
    picked = [
        parts_ref[j, chunk * length : (chunk + 1) * length, start : start + width]
        for j in range(parts_ref.shape[0])
    ]
    return jnp.concatenate(picked, axis=1)


def three_parts(value):
    high = value.astype(BF16).astype(F32)
    mid = (value - high).astype(BF16).astype(F32)
    return high, mid, value - high - mid


def pack_kernel(tokens_ref, offsets_ref, conv_gain_ref, memory_gain_ref, out_ref):
    length = tokens_ref.shape[0]
    offsets = three_parts(offsets_ref[...])
    conv_gain = three_parts(conv_gain_ref[...])
    memory_gain = three_parts(memory_gain_ref[...])
    rows = [jnp.concatenate([p[k : k + 1] for k in range(p.shape[0])], axis=1) for p in offsets]
    rows += memory_gain
    rows.append(jnp.concatenate(conv_gain[:2], axis=1))
    rows.append(jnp.concatenate([conv_gain[2], jnp.zeros_like(conv_gain[2])], axis=1))
    extra = jnp.concatenate(rows, axis=0).astype(BF16)
    tokens = tokens_ref[...]
    for j in range(out_ref.shape[0]):
        out_ref[j, :length] = tokens
        out_ref[j, length:] = extra


def piece_kernel(
    query_ref, key_ref, value_ref, left_ref, right_ref, memory_ref, conv_ref, out_ref, turn_ref
):
    nx, nc = out_ref.shape[0], out_ref.shape[1]
    rows = memory_ref.shape[0]
    width, chan = memory_ref.shape[1] // (nx * nc), conv_ref.shape[1] // (nx * nc)
    parts = []
    for at in range(nx * nc):
        parts.append(memory_ref[:, at * width : (at + 1) * width])
        parts.append(conv_ref[:, at * chan : (at + 1) * chan])
    whole = jnp.concatenate(parts, axis=1)
    wide = out_ref.shape[3]
    for j in range(whole.shape[1] // wide):
        turn_ref[j * rows : (j + 1) * rows] = whole[:, j * wide : (j + 1) * wide]
    for x in range(nx):
        for c in range(nc):
            at = c * nx + x
            parts = []
            for ref in (query_ref, key_ref, value_ref, left_ref, right_ref):
                width = ref.shape[1] // (nx * nc)
                parts.append(ref[:, at * width : (at + 1) * width])
            out_ref[x, c] = jnp.concatenate(parts, axis=1)


def arrange_kernel(in_ref, near_ref, low_ref, high_ref):
    half = low_ref.shape[0]
    near_ref[...] = in_ref[...]
    low_ref[...] = in_ref[:half]
    high_ref[...] = in_ref[half:]


def project_kernel(
    place_ref, own_ref, other_ref,
    w0_ref, w1_ref, w3_ref, low_ref, high_ref, gate_ref,
    qk_ref, v_ref, glu_ref, gates_ref, gain_ref, out_weight_ref,
):
    nx, ny, _, part = own_ref.shape
    far, tall, wide = w0_ref.shape
    depth, chunks = out_weight_ref.shape[2], out_weight_ref.shape[3] // wide
    rows = tall - depth * chunks
    close = part // rows
    length = glu_ref.shape[1]
    place, core, column = place_ref[0], place_ref[1], place_ref[2]
    tokens_rows = nx * length
    width = qk_ref.shape[4] // 2
    chan = glu_ref.shape[2] // nx
    lane = lax.broadcasted_iota(jnp.int32, (length, width), 1)
    ones = jnp.where(lane == 0, 1.0, 0.0).astype(BF16)
    row = lax.broadcasted_iota(jnp.int32, (2 * nx, length), 0)
    gate_in = jnp.zeros((2 * nx, length), F32)
    forget = jnp.zeros((2 * nx, length), F32)

    blocks = [
        (ref, i, ahead, i)
        for ref, ahead in ((w0_ref, 0), (w1_ref, 1), (w3_ref, close - 1))
        for i in range(far)
    ]
    blocks += [(low_ref, i, 2, i) for i in range(far // 2)]
    blocks += [(high_ref, i, 2, i + far // 2) for i in range(far // 2)]
    homes = []
    for ref, i, ahead, y in blocks:
        homes.append((y, lax.rem(place + ahead, close)))
        behind = lax.rem(y + ny - column, ny)
        out_weight_ref[pl.ds(behind, 1), pl.ds(homes[-1][1], 1)] = jnp.concatenate(
            [ref[i, rows + j * depth : rows + (j + 1) * depth] for j in range(chunks)], axis=1
        )[None, None]
    for half, ref in enumerate((own_ref, other_ref)):
        home = core if half == 0 else 1 - core
        acc = jnp.zeros((tokens_rows, wide), F32)
        pre = jnp.zeros((tokens_rows, gate_ref.shape[1]), F32)
        for pair in range(0, len(blocks), 2):
            left, right, gate_rows = [], [], []
            for at in (pair, pair + 1):
                w_ref, i, _, _ = blocks[at]
                y, z = homes[at]
                start = pl.multiple_of(z * rows, rows)
                left.append(ref[:, y, :length, pl.ds(start, rows)].reshape(tokens_rows, rows))
                right.append(w_ref[i, :rows])
                gate_rows.append(gate_ref[pl.ds(y * part + start, rows)])
            lhs = jnp.concatenate(left, axis=1)
            acc = acc + dot(lhs, jnp.concatenate(right, axis=0), NN)
            pre = pre + dot(lhs, jnp.concatenate(gate_rows, axis=0), NN)
        glu = []
        for x in range(nx):
            mine = acc[x * length : (x + 1) * length]
            qk = mine[:, : 2 * width].astype(BF16)[None]
            for j in range(qk_ref.shape[0]):
                qk_ref[j, x, pl.ds(home, 1)] = qk
            v_ref[x, pl.ds(home, 1)] = jnp.concatenate(
                [mine[:, 2 * width : 3 * width].astype(BF16), ones], axis=1
            )[None]
            left = mine[:, 3 * width : 3 * width + chan]
            right = mine[:, 3 * width + chan :]
            glu.append(left / (1.0 + jnp.exp(-right)))
        glu_ref[pl.ds(home, 1)] = jnp.concatenate(glu, axis=1).astype(BF16)[None]
        for x in range(nx):
            turned = pre[x * length : (x + 1) * length].T
            extra = ref[x, column, length : length + 8].astype(F32)
            values = extra[0:1] + extra[1:2] + extra[2:3]
            offsets = jnp.where(core == 0, values[:, :length], values[:, length : 2 * length])
            offsets_f = jnp.where(
                core == 0, values[:, 2 * length : 3 * length], values[:, 3 * length : 4 * length]
            )
            at = row == 2 * x + home
            gate_pre = jnp.where(core == 0, turned[0:1], turned[1:2])
            forget_pre = jnp.where(core == 0, turned[2:3], turned[3:4])
            gate_in = jnp.where(at, gate_pre + offsets, gate_in)
            forget = jnp.where(at, forget_pre + offsets_f, forget)
    for b in range(ny):
        extra = own_ref[0, b, length : length + 8].astype(F32)
        memory_gain = extra[3:4] + extra[4:5] + extra[5:6]
        half = part // 2
        conv_gain = extra[6:7, :half] + extra[6:7, half:] + extra[7:8, :half]
        for at in range(2 * nx):
            gain_ref[b, at : at + 1] = jnp.concatenate(
                [
                    memory_gain[:, at * width : (at + 1) * width],
                    conv_gain[:, at * chan : (at + 1) * chan],
                    jnp.zeros((1, width - chan), F32),
                ],
                axis=1,
            )
    y = jnp.exp(-jnp.abs(forget))
    small = y * (1.0 - y * (1 / 2 - y * (1 / 3 - y * (1 / 4 - y * (1 / 5)))))
    gates_ref[0] = gate_in
    gates_ref[1] = jnp.minimum(forget, 0.0) - jnp.where(y < 0.03, small, jnp.log(1.0 + y))


def finish_kernel(place_ref, arrived_ref, own_ref, other_ref, gain_ref, out_ref, weight_ref):
    nx, nc, ny, _, lanes = arrived_ref.shape
    core, x_at = place_ref[1], place_ref[3]
    width = lanes // 2
    chan = width // 2
    length, part = out_ref.shape
    lane = lax.broadcasted_iota(jnp.int32, (length, width + chan), 1)
    is_memory = lane < width
    half = length // 2

    def block(x, c, b):
        got = arrived_ref[x, c, b].astype(F32)
        memory = jnp.concatenate([got[:half, :width], got[:half, width:]], axis=0)
        conv = [got[half:, k * chan : (k + 1) * chan] for k in range(4)]
        return jnp.concatenate([memory, jnp.concatenate(conv, axis=0)], axis=1)

    blocks = {
        (x, c, b): block(x, c, b) for x in range(nx) for c in range(nc) for b in range(ny)
    }
    first = sum(blocks.values())
    second = sum(got * got for got in blocks.values())
    senders = nx * nc * ny
    memory_mean = jnp.sum(jnp.where(is_memory, second, 0.0), axis=1, keepdims=True)
    scale = lax.rsqrt(memory_mean / (senders * width) + EPS)
    mean = jnp.sum(jnp.where(is_memory, 0.0, first), axis=1, keepdims=True) / (senders * chan)
    power = jnp.sum(jnp.where(is_memory, 0.0, second), axis=1, keepdims=True) / (senders * chan)
    spread = lax.rsqrt(power - mean * mean + EPS)
    shift = jnp.where(is_memory, 0.0, mean)
    factor = jnp.where(is_memory, scale, spread)
    deep = weight_ref.shape[5]
    for ahead in range(nx):
        x = lax.rem(x_at + ahead, nx)
        for c, ref in ((core, own_ref), (1 - core, other_ref)):
            for b in range(ny):
                for near in range(ref.shape[2]):
                    at = lax.rem(place_ref[2] + ny - b, ny)
                    weight_ref[pl.ds(at, 1), near, pl.ds(x, 1), pl.ds(c, 1)] = ref[ahead, b, near][
                        None, None, None
                    ]
    total = jnp.zeros((length, part), F32)
    for b in range(ny):
        left = []
        for c in range(nc):
            for x in range(nx):
                gain = gain_ref[b, c * nx + x : c * nx + x + 1, : width + chan]
                normed = (blocks[x, c, b] - shift) * factor * gain
                branch = normed / (1.0 + jnp.exp(-normed))
                left.append(jnp.where(is_memory, normed, branch).astype(BF16))
        total = total + dot(
            jnp.concatenate(left, axis=1), weight_ref[b].reshape(part, deep), NT
        )
    out_ref[...] = total.astype(BF16)


def convolve(glu_ref, prior, taps_ref, nx, core, x_at):
    nc, length, lanes = glu_ref.shape
    chan = lanes // nx
    group = nc * length
    glu = glu_ref[...].reshape(group, lanes).astype(F32)
    taps = taps_ref.shape[0]
    hold = 32
    lane = lax.broadcasted_iota(jnp.int32, (hold, lanes), 1)
    before = pltpu.roll(glu[group - hold :], chan, 1)
    prior = jnp.concatenate([prior, jnp.zeros((hold, lanes - chan), F32)], axis=1)
    extended = jnp.concatenate([jnp.where(lane < chan, prior, before), glu], axis=0)
    weights = taps_ref[...].astype(F32)
    weights = jnp.where(core == 0, weights[:, :lanes], weights[:, lanes:])
    weights = pltpu.roll(weights, lax.rem(lanes - chan * x_at, lanes), 1)
    weights = jnp.where(lax.broadcasted_iota(jnp.int32, weights.shape, 1) < chan, weights, 0.0)
    weights = sum(pltpu.roll(weights, chan * k, 1) for k in range(1, nx)) + weights
    total = jnp.zeros((group, lanes), F32)
    first = hold - (taps - 1)
    for shift in range(8):
        moved = extended[shift : shift + group + hold - 8] if shift else extended
        for j in range(taps):
            at = first + j
            if at % 8 == shift:
                total = total + moved[at - shift : at - shift + group] * weights[j : j + 1]
    return [total[:, x * chan : (x + 1) * chan].astype(BF16) for x in range(nx)]


def slab_kernel(
    qk_ref, v_ref, gate_ref, glu_ref, out_ref, q_ref, k_ref,
):
    chunks, length = gate_ref.shape[1], gate_ref.shape[2]
    width = qk_ref.shape[2] // 2
    gate, forget = gate_ref[0], gate_ref[1]
    within = lane_cumsum(forget)
    ends = [within[r : r + 1, length - 1 :] for r in range(chunks)]
    after = [jnp.zeros((1, 1), F32)]
    for r in range(chunks - 1, 0, -1):
        after.insert(0, after[0] + ends[r])
    total = after[0] + ends[0]
    to_end = jnp.concatenate([e + a for e, a in zip(ends, after)], axis=0)
    end_log = to_end - within + gate
    level = jnp.max(jnp.max(end_log, axis=1, keepdims=True), axis=0, keepdims=True)
    fresh = columns_of(jnp.exp(end_log - level))
    state = jnp.zeros((2 * width, width * qk_ref.shape[0]), F32)
    for r in range(chunks):
        q_ref[r * length : (r + 1) * length] = joined(qk_ref, 0, width, r, length)
        key = joined(qk_ref, width, width, r, length)
        k_ref[r * length : (r + 1) * length] = key
        scaled = (fresh[:, r : r + 1] * key.astype(F32)).astype(BF16)
        state = state + dot(v_ref[r * length : (r + 1) * length], scaled, TN)
    rows, head_lanes = out_ref.shape[1], out_ref.shape[2]
    kept = state[:rows]
    row = lax.broadcasted_iota(jnp.int32, kept.shape, 0)
    lane = lax.broadcasted_iota(jnp.int32, kept.shape, 1)
    for at, value in ((0, level), (3, total)):
        high = value.astype(BF16).astype(F32)
        mid = (value - high).astype(BF16).astype(F32)
        low = value - high - mid
        for k, part in enumerate((high, mid, low)):
            kept = jnp.where((row == width + 1) & (lane == at + k), part, kept)
    chan = glu_ref.shape[2] // qk_ref.shape[0]
    hold = 32
    tail = glu_ref[glu_ref.shape[0] - 1, length - hold :].astype(F32)[:, glu_ref.shape[2] - chan :]
    group = head_lanes // chan
    each = hold // group
    tail = jnp.concatenate([tail[g * each : (g + 1) * each] for g in range(group)], axis=1)
    kept = jnp.concatenate([kept[: width + 2], tail, kept[width + 2 + each :]], axis=0)
    kept = kept.astype(BF16)
    for j in range(out_ref.shape[0]):
        out_ref[j] = kept


def cell_kernel(place_ref, in_ref, q_ref, k_ref, v_ref, gate_ref, glu_ref, taps_ref, out_ref):
    chunks, length = gate_ref.shape[1], gate_ref.shape[2]
    members, rows, head = in_ref.shape
    width = v_ref.shape[1] // 2
    nc, ny = out_ref.shape[1], out_ref.shape[2]
    scale = head ** (-0.5)
    place = place_ref[0]
    chan = glu_ref.shape[2] // out_ref.shape[0]
    hold, group = 32, head // chan
    each = hold // group
    last_rows = in_ref[jnp.maximum(place - 1, 0), width : width + 8].astype(F32)
    last_rows = jnp.where(place > 0, last_rows[2 : 2 + each], 0.0)
    prior = jnp.concatenate([last_rows[:, g * chan : (g + 1) * chan] for g in range(group)], axis=0)
    conv = convolve(glu_ref, prior, taps_ref, out_ref.shape[0], place_ref[1], place_ref[3])
    acc = jnp.zeros((1, 1), F32)
    logs = [None] * members
    for j in range(members - 1, -1, -1):
        line = in_ref[j, width + 1 : width + 2, :128].astype(F32)
        level_j = line[:, 0:1] + line[:, 1:2] + line[:, 2:3]
        total_j = line[:, 3:4] + line[:, 4:5] + line[:, 5:6]
        before = j < place
        logs[j] = jnp.where(before, level_j + acc, LOW)
        acc = acc + jnp.where(before, total_j, 0.0)
    level = logs[0]
    for j in range(1, members):
        level = jnp.maximum(level, logs[j])
    state = jnp.zeros((rows, head), F32)
    for j in range(members):
        weight = jnp.where(j < place, jnp.exp(logs[j] - level), 0.0)
        state = state + weight * in_ref[j].astype(F32)
    state = jnp.concatenate([state, jnp.zeros((2 * width - rows, head), F32)], axis=0)
    gate, forget = gate_ref[0], gate_ref[1]
    within = lane_cumsum(forget)
    turned = columns_of(jnp.concatenate([within, gate], axis=0))
    causal = lax.broadcasted_iota(jnp.int32, (length, length), 0) >= lax.broadcasted_iota(
        jnp.int32, (length, length), 1
    )
    for r in range(chunks):
        here = slice(r * length, (r + 1) * length)
        query, key, value = q_ref[here], k_ref[here], v_ref[here]
        within_row, gate_row = within[r : r + 1], gate[r : r + 1]
        within_col = turned[:, r : r + 1]
        gate_col = turned[:, chunks + r : chunks + r + 1]
        log_weight = jnp.where(causal, within_col - within_row + gate_row, -jnp.inf)
        carried = within_col + level
        top = jnp.maximum(carried, jnp.max(log_weight, axis=1, keepdims=True))
        weight = jnp.exp(log_weight - top)
        carried_weight = jnp.exp(carried - top) * scale
        scores = dot(query, key, NT) * (scale * weight)
        older = dot(query, state.astype(BF16), NT)
        numer = dot(scores.astype(BF16), value, NN) + carried_weight * older
        denom = jnp.sum(scores, axis=1, keepdims=True) + carried_weight * older[:, width : width + 1]
        result = numer[:, :width] / jnp.maximum(jnp.abs(denom), 1.0)
        x, c = r // nc, r % nc
        half, quarter = length // 2, length // 4
        memory = jnp.concatenate([result[:half], result[half:]], axis=1).astype(BF16)
        branch = [conv[x][c * length + g * quarter : c * length + (g + 1) * quarter] for g in range(4)]
        sent = jnp.concatenate([memory, jnp.concatenate(branch, axis=1)], axis=0)
        for y in range(ny):
            out_ref[x, c, y] = sent
        last = within_row[:, length - 1 :]
        end_row = last - within_row + gate_row
        new_level = jnp.maximum(last + level, jnp.max(end_row, axis=1, keepdims=True))
        keep = jnp.exp(last + level - new_level)
        fresh = jnp.exp(last - within_col + gate_col - new_level)
        scaled = (fresh * key.astype(F32)).astype(BF16)
        state = keep * state + dot(value, scaled, TN)
        level = new_level


def vmem(count):
    return [pl.BlockSpec(memory_space=pltpu.VMEM)] * count


def layer(
    tokens,
    conv_value_weight,
    conv_gate_weight,
    conv_kernel,
    conv_norm_gain,
    query_weight,
    key_weight,
    value_weight,
    input_gate_weight,
    forget_gate_weight,
    input_offset,
    forget_offset,
    memory_norm_gain,
    conv_out_weight,
    memory_out_weight,
):
    nzh, nzl, nx, nc, ny = (size(a) for a in AXES)
    xi, ci, yi = lax.axis_index("x"), lax.axis_index("c"), lax.axis_index("tp")
    members = nzh * nzl
    zi = lax.axis_index("zh") * nzl + lax.axis_index("zl")
    length, part = tokens.shape
    slab = length * nx * nc
    head = query_weight.shape[1] // nc
    width = head // nx
    chan = conv_value_weight.shape[1] // nc // nx
    rows = query_weight.shape[0]
    wide = 3 * width + 2 * chan

    def from_z(value, ahead):
        return lax.ppermute(value, Z, [(j, (j - ahead) % members) for j in range(members)])

    deep = memory_out_weight.shape[0] + conv_out_weight.shape[0]
    pieces, out_rows = pl.pallas_call(
        piece_kernel,
        out_shape=(
            jax.ShapeDtypeStruct((nx, nc, rows, wide), BF16),
            jax.ShapeDtypeStruct((deep // wide * rows, wide), BF16),
        ),
        in_specs=vmem(7),
        out_specs=vmem(2),
        interpret=INTERPRET,
        name="pieces",
    )(
        query_weight,
        key_weight,
        value_weight,
        conv_value_weight,
        conv_gate_weight,
        memory_out_weight.T,
        conv_out_weight.T,
    )
    offsets = jnp.concatenate([input_offset.T, forget_offset.T], axis=0)
    call_pack = pl.pallas_call(
        pack_kernel,
        out_shape=jax.ShapeDtypeStruct((nx * ny, length + 8, part), BF16),
        in_specs=vmem(4),
        out_specs=pl.BlockSpec(memory_space=pltpu.VMEM),
        interpret=INTERPRET,
        name="pack",
    )
    sent = call_pack(tokens, offsets, conv_norm_gain[None], memory_norm_gain[None])
    mine = exchange(pieces.reshape(nx * nc, rows, wide), ("x", "c"))
    mine = mine.reshape(nx * nc * rows, wide)
    mine = jnp.concatenate([mine, out_rows], axis=0)
    near = exchange(jnp.broadcast_to(mine, (nzh, *mine.shape)), "zh")
    own = exchange(sent, ("x", "tp")).reshape(nx, ny, length + 8, part)
    half_shape = (nzh // 2, *mine.shape)
    near, *halves = pl.pallas_call(
        arrange_kernel,
        out_shape=(
            jax.ShapeDtypeStruct(near.shape, BF16),
            jax.ShapeDtypeStruct(half_shape, BF16),
            jax.ShapeDtypeStruct(half_shape, BF16),
        ),
        in_specs=vmem(1),
        out_specs=vmem(3),
        interpret=INTERPRET,
        name="arrange",
    )(near)
    sets = [near, from_z(near, 1), from_z(near, -1)]
    sets += [from_z(halves[0], 2), from_z(halves[1], -2)]
    other = swapped(own, "c")

    gate_weight = jnp.pad(
        jnp.concatenate([input_gate_weight, forget_gate_weight], axis=1), ((0, 0), (0, 124))
    )
    place = jnp.stack([zi, ci, yi, xi])
    smem = pl.BlockSpec(memory_space=pltpu.SMEM)
    qk, value, packed, gates, gain, out_part = pl.pallas_call(
        project_kernel,
        out_shape=(
            jax.ShapeDtypeStruct((nx, nx, nc, length, 2 * width), BF16),
            jax.ShapeDtypeStruct((nx, nc, length, 2 * width), BF16),
            jax.ShapeDtypeStruct((nc, length, nx * chan), BF16),
            jax.ShapeDtypeStruct((2, nx * nc, length), F32),
            jax.ShapeDtypeStruct((ny, nc * nx, 2 * width), F32),
            jax.ShapeDtypeStruct((nzh, nzl, rows, deep), BF16),
        ),
        in_specs=[smem] + vmem(8),
        out_specs=vmem(6),
        interpret=INTERPRET,
        name="project",
    )(place, own, other, *sets, gate_weight)
    value = value.reshape(slab, 2 * width)
    all_qk = exchange(qk.reshape(nx, slab, 2 * width), "x")
    out_part = [out_part[0]] + [
        lax.ppermute(out_part[ahead], "tp", [(j, (j + ahead) % ny) for j in range(ny)])
        for ahead in range(1, ny)
    ]
    out_part = jnp.stack(out_part, axis=0)
    out_parts = [out_part] + [
        lax.ppermute(out_part, "x", [(j, (j - ahead) % nx) for j in range(nx)])
        for ahead in range(1, nx)
    ]
    own_out = jnp.stack(out_parts, axis=0)
    other_out = swapped(own_out, "c")

    state_rows = width + 8
    call_slab = pl.pallas_call(
        slab_kernel,
        out_shape=(
            jax.ShapeDtypeStruct((members, state_rows, head), BF16),
            jax.ShapeDtypeStruct((slab, head), BF16),
            jax.ShapeDtypeStruct((slab, head), BF16),
        ),
        in_specs=vmem(4),
        out_specs=vmem(3),
        interpret=INTERPRET,
        name="slab_state",
    )
    states, query, key = call_slab(all_qk, value, gates, packed)
    states = exchange(states, Z)
    call_cell = pl.pallas_call(
        cell_kernel,
        out_shape=jax.ShapeDtypeStruct((nx, nc, ny, length // 4 * 3, 2 * width), BF16),
        in_specs=[smem] + vmem(7),
        out_specs=pl.BlockSpec(memory_space=pltpu.VMEM),
        interpret=INTERPRET,
        name="cell",
    )
    last = call_cell(place, states, query, key, value, gates, packed, conv_kernel)
    arrived = exchange(last.reshape(nx * nc * ny, length // 4 * 3, -1), ("x", "c", "tp"))
    arrived = arrived.reshape(nx, nc, ny, length // 4 * 3, -1)
    return pl.pallas_call(
        finish_kernel,
        out_shape=jax.ShapeDtypeStruct((length, part), BF16),
        in_specs=[smem] + vmem(4),
        out_specs=pl.BlockSpec(memory_space=pltpu.VMEM),
        scratch_shapes=[pltpu.VMEM((ny, nzl, nx, nc, rows, deep), BF16)],
        interpret=INTERPRET,
        name="finish",
    )(place, arrived, own_out, other_out, gain)


def solution(mesh):
    shape = mesh.shape
    depth = shape["sp"] // 32
    split = Mesh(mesh.devices.reshape(4, depth, 4, 2, shape["tp"]), AXES)
    in_specs = (
        P(SP, "tp"),
        P(SP, "tp"),
        P(SP, "tp"),
        P(None, "tp"),
        P("tp"),
        P(SP, "tp"),
        P(SP, "tp"),
        P(SP, "tp"),
        P(None, "tp"),
        P(None, "tp"),
        P(SP, "tp"),
        P(SP, "tp"),
        P("tp"),
        P("tp", SP),
        P("tp", SP),
    )
    return jax.shard_map(
        layer, mesh=split, in_specs=in_specs, out_specs=P(SP, "tp"), check_vma=False
    )
```

```python
import jax
import jax.numpy as jnp
from jax import lax
from jax.experimental import pallas as pl
from jax.experimental.pallas import tpu as pltpu
from jax.sharding import Mesh
from jax.sharding import PartitionSpec as P

AXES = ("zh", "zl", "x", "c", "tp")
Z = ("zh", "zl")
SP = ("zh", "zl", "x", "c")
EPS = 1e-06
LOW = -1e30
F32 = jnp.float32
BF16 = jnp.bfloat16
INTERPRET = False


def size(axis):
    return lax.axis_size(axis)


def exchange(pieces, axes):
    return lax.all_to_all(pieces, axes, split_axis=0, concat_axis=0, tiled=True)


def swapped(value, axis):
    return lax.ppermute(value, axis, [(0, 1), (1, 0)])


def lane_cumsum(rows):
    lane = lax.broadcasted_iota(jnp.int32, rows.shape, 1)
    step = 1
    while step < rows.shape[1]:
        moved = pltpu.roll(rows, step, 1)
        rows = rows + jnp.where(lane >= step, moved, 0.0)
        step *= 2
    return rows


def columns_of(rows):
    count, length = rows.shape
    square = jnp.concatenate([rows, jnp.zeros((length - count, length), F32)], axis=0)
    return square.T


def dot(a, b, dims):
    return lax.dot_general(a, b, (dims, ((), ())), preferred_element_type=F32)


NN = ((1,), (0,))
NT = ((1,), (1,))
TN = ((0,), (0,))


def joined(parts_ref, start, width, chunk, length):
    picked = [
        parts_ref[j, chunk * length : (chunk + 1) * length, start : start + width]
        for j in range(parts_ref.shape[0])
    ]
    return jnp.concatenate(picked, axis=1)


def three_parts(value):
    high = value.astype(BF16).astype(F32)
    mid = (value - high).astype(BF16).astype(F32)
    return high, mid, value - high - mid


def pack_kernel(tokens_ref, offsets_ref, conv_gain_ref, memory_gain_ref, out_ref):
    length = tokens_ref.shape[0]
    offsets = three_parts(offsets_ref[...])
    conv_gain = three_parts(conv_gain_ref[...])
    memory_gain = three_parts(memory_gain_ref[...])
    rows = [jnp.concatenate([p[k : k + 1] for k in range(p.shape[0])], axis=1) for p in offsets]
    rows += memory_gain
    rows.append(jnp.concatenate(conv_gain[:2], axis=1))
    rows.append(jnp.concatenate([conv_gain[2], jnp.zeros_like(conv_gain[2])], axis=1))
    extra = jnp.concatenate(rows, axis=0).astype(BF16)
    tokens = tokens_ref[...]
    for j in range(out_ref.shape[0]):
        out_ref[j, :length] = tokens
        out_ref[j, length:] = extra


def piece_kernel(
    query_ref, key_ref, value_ref, left_ref, right_ref, memory_ref, conv_ref, out_ref, turn_ref
):
    nx, nc = out_ref.shape[0], out_ref.shape[1]
    rows = memory_ref.shape[0]
    width, chan = memory_ref.shape[1] // (nx * nc), conv_ref.shape[1] // (nx * nc)
    parts = []
    for at in range(nx * nc):
        parts.append(memory_ref[:, at * width : (at + 1) * width])
        parts.append(conv_ref[:, at * chan : (at + 1) * chan])
    whole = jnp.concatenate(parts, axis=1)
    wide = out_ref.shape[3]
    for j in range(whole.shape[1] // wide):
        turn_ref[j * rows : (j + 1) * rows] = whole[:, j * wide : (j + 1) * wide]
    for x in range(nx):
        for c in range(nc):
            at = c * nx + x
            parts = []
            for ref in (query_ref, key_ref, value_ref, left_ref, right_ref):
                width = ref.shape[1] // (nx * nc)
                parts.append(ref[:, at * width : (at + 1) * width])
            out_ref[x, c] = jnp.concatenate(parts, axis=1)


def arrange_kernel(
    before_ref, mine_ref, after_ref, main_ref, rest_ref, near_ref, low_ref, high_ref
):
    rows = main_ref.shape[0]
    for refs in ((near_ref, 0), (high_ref, 0)):
        refs[0][refs[1]] = before_ref[...]
    for refs in ((near_ref, 1), (high_ref, 1), (low_ref, 0)):
        refs[0][refs[1]] = mine_ref[...]
    for refs in ((near_ref, 2), (low_ref, 1)):
        refs[0][refs[1]] = after_ref[...]
    near_ref[3, :rows] = main_ref[...]
    near_ref[3, rows:] = rest_ref[...]


def assemble_kernel(place_ref, *refs):
    out_ref = refs[-1]
    nx, ny = out_ref.shape[2], out_ref.shape[0]
    core, column, x_at = place_ref[1], place_ref[2], place_ref[3]
    for ahead in range(nx):
        x = lax.rem(x_at + ahead, nx)
        for c, ref in ((core, refs[ahead]), (1 - core, refs[nx + ahead])):
            for b in range(ny):
                at = lax.rem(column + ny - b, ny)
                for near in range(ref.shape[1]):
                    out_ref[pl.ds(at, 1), near, pl.ds(x, 1), pl.ds(c, 1)] = ref[b, near][
                        None, None, None
                    ]


def project_kernel(
    place_ref, own_ref, other_ref,
    w0_ref, w1_ref, w3_ref, low_ref, high_ref, gate_ref,
    qk_ref, v_ref, glu_ref, gates_ref, gain_ref, out_weight_ref,
):
    nx, ny, _, part = own_ref.shape
    far, tall, wide = w0_ref.shape
    depth, chunks = out_weight_ref.shape[2], out_weight_ref.shape[3] // wide
    rows = tall - depth * chunks
    close = part // rows
    length = glu_ref.shape[1]
    place, core, column = place_ref[0], place_ref[1], place_ref[2]
    tokens_rows = nx * length
    width = qk_ref.shape[4] // 2
    chan = glu_ref.shape[2] // nx
    lane = lax.broadcasted_iota(jnp.int32, (length, width), 1)
    ones = jnp.where(lane == 0, 1.0, 0.0).astype(BF16)
    row = lax.broadcasted_iota(jnp.int32, (2 * nx, length), 0)
    gate_in = jnp.zeros((2 * nx, length), F32)
    forget = jnp.zeros((2 * nx, length), F32)

    members = far * close
    blocks = [
        (ref, i, ahead + close * (i - 1))
        for ref, ahead in ((w0_ref, 0), (w1_ref, 1), (w3_ref, -1))
        for i in range(far)
    ]
    blocks += [(low_ref, i, 2 + close * i) for i in range(far // 2)]
    blocks += [(high_ref, i, -2 + close * (i - 1)) for i in range(far // 2)]
    homes = []
    for ref, i, ahead in blocks:
        home = lax.rem(place + (ahead + members), members)
        y = lax.div(home, close)
        homes.append((y, lax.rem(home, close)))
        behind = lax.rem(y + ny - column, ny)
        out_weight_ref[pl.ds(behind, 1), pl.ds(homes[-1][1], 1)] = jnp.concatenate(
            [ref[i, rows + j * depth : rows + (j + 1) * depth] for j in range(chunks)], axis=1
        )[None, None]
    for half, ref in enumerate((own_ref, other_ref)):
        home = core if half == 0 else 1 - core
        acc = jnp.zeros((tokens_rows, wide), F32)
        pre = jnp.zeros((tokens_rows, gate_ref.shape[1]), F32)
        for pair in range(0, len(blocks), 2):
            left, right, gate_rows = [], [], []
            for at in (pair, pair + 1):
                w_ref, i, _ = blocks[at]
                y, z = homes[at]
                start = pl.multiple_of(z * rows, rows)
                left.append(
                    ref[:, pl.ds(y, 1), :length, pl.ds(start, rows)].reshape(tokens_rows, rows)
                )
                right.append(w_ref[i, :rows])
                gate_rows.append(gate_ref[pl.ds(y * part + start, rows)])
            lhs = jnp.concatenate(left, axis=1)
            acc = acc + dot(lhs, jnp.concatenate(right, axis=0), NN)
            pre = pre + dot(lhs, jnp.concatenate(gate_rows, axis=0), NN)
        glu = []
        for x in range(nx):
            mine = acc[x * length : (x + 1) * length]
            qk = mine[:, : 2 * width].astype(BF16)[None]
            for j in range(qk_ref.shape[0]):
                qk_ref[j, x, pl.ds(home, 1)] = qk
            v_ref[x, pl.ds(home, 1)] = jnp.concatenate(
                [mine[:, 2 * width : 3 * width].astype(BF16), ones], axis=1
            )[None]
            left = mine[:, 3 * width : 3 * width + chan]
            right = mine[:, 3 * width + chan :]
            glu.append(left / (1.0 + jnp.exp(-right)))
        glu_ref[pl.ds(home, 1)] = jnp.concatenate(glu, axis=1).astype(BF16)[None]
        for x in range(nx):
            turned = pre[x * length : (x + 1) * length].T
            extra = ref[x, column, length : length + 8].astype(F32)
            values = extra[0:1] + extra[1:2] + extra[2:3]
            offsets = jnp.where(core == 0, values[:, :length], values[:, length : 2 * length])
            offsets_f = jnp.where(
                core == 0, values[:, 2 * length : 3 * length], values[:, 3 * length : 4 * length]
            )
            at = row == 2 * x + home
            gate_pre = jnp.where(core == 0, turned[0:1], turned[1:2])
            forget_pre = jnp.where(core == 0, turned[2:3], turned[3:4])
            gate_in = jnp.where(at, gate_pre + offsets, gate_in)
            forget = jnp.where(at, forget_pre + offsets_f, forget)
    for b in range(ny):
        extra = own_ref[0, b, length : length + 8].astype(F32)
        memory_gain = extra[3:4] + extra[4:5] + extra[5:6]
        half = part // 2
        conv_gain = extra[6:7, :half] + extra[6:7, half:] + extra[7:8, :half]
        for at in range(2 * nx):
            gain_ref[b, at : at + 1] = jnp.concatenate(
                [
                    memory_gain[:, at * width : (at + 1) * width],
                    conv_gain[:, at * chan : (at + 1) * chan],
                    jnp.zeros((1, width - chan), F32),
                ],
                axis=1,
            )
    y = jnp.exp(-jnp.abs(forget))
    small = y * (1.0 - y * (1 / 2 - y * (1 / 3 - y * (1 / 4 - y * (1 / 5)))))
    gates_ref[0] = gate_in
    gates_ref[1] = jnp.minimum(forget, 0.0) - jnp.where(y < 0.03, small, jnp.log(1.0 + y))


def finish_kernel(arrived_ref, weight_ref, gain_ref, out_ref):
    nx, nc, ny, _, lanes = arrived_ref.shape
    width = lanes // 2
    chan = width // 2
    length, part = out_ref.shape
    lane = lax.broadcasted_iota(jnp.int32, (length, width + chan), 1)
    is_memory = lane < width
    half = length // 2

    def block(x, c, b):
        got = arrived_ref[x, c, b].astype(F32)
        memory = jnp.concatenate([got[:half, :width], got[:half, width:]], axis=0)
        conv = [got[half:, k * chan : (k + 1) * chan] for k in range(4)]
        return jnp.concatenate([memory, jnp.concatenate(conv, axis=0)], axis=1)

    blocks = {
        (x, c, b): block(x, c, b) for x in range(nx) for c in range(nc) for b in range(ny)
    }
    first = sum(blocks.values())
    second = sum(got * got for got in blocks.values())
    senders = nx * nc * ny
    memory_mean = jnp.sum(jnp.where(is_memory, second, 0.0), axis=1, keepdims=True)
    scale = lax.rsqrt(memory_mean / (senders * width) + EPS)
    mean = jnp.sum(jnp.where(is_memory, 0.0, first), axis=1, keepdims=True) / (senders * chan)
    power = jnp.sum(jnp.where(is_memory, 0.0, second), axis=1, keepdims=True) / (senders * chan)
    spread = lax.rsqrt(power - mean * mean + EPS)
    shift = jnp.where(is_memory, 0.0, mean)
    factor = jnp.where(is_memory, scale, spread)
    deep = weight_ref.shape[5]
    total = jnp.zeros((length, part), F32)
    for b in range(ny):
        left = []
        for c in range(nc):
            for x in range(nx):
                gain = gain_ref[b, c * nx + x : c * nx + x + 1, : width + chan]
                normed = (blocks[x, c, b] - shift) * factor * gain
                branch = normed / (1.0 + jnp.exp(-normed))
                left.append(jnp.where(is_memory, normed, branch).astype(BF16))
        total = total + dot(
            jnp.concatenate(left, axis=1), weight_ref[b].reshape(part, deep), NT
        )
    out_ref[...] = total.astype(BF16)


HOLD = 32


def tap_rows(taps_ref, core, x_at, nx, lanes):
    chan = lanes // nx
    weights = taps_ref[...].astype(F32)
    weights = jnp.where(core == 0, weights[:, :lanes], weights[:, lanes:])
    weights = pltpu.roll(weights, lax.rem(lanes - chan * x_at, lanes), 1)
    weights = jnp.where(lax.broadcasted_iota(jnp.int32, weights.shape, 1) < chan, weights, 0.0)
    return sum(pltpu.roll(weights, chan * k, 1) for k in range(1, nx)) + weights


def convolve(extended, weights):
    taps = weights.shape[0]
    length = extended.shape[0] - HOLD
    total = jnp.zeros((length, extended.shape[1]), F32)
    first = HOLD - (taps - 1)
    for shift in range(8):
        moved = extended[shift : shift + length + HOLD - 8] if shift else extended
        for j in range(taps):
            at = first + j
            if at % 8 == shift:
                total = total + moved[at - shift : at - shift + length] * weights[j : j + 1]
    return total


def slab_kernel(
    qk_ref, v_ref, gate_ref, glu_ref, out_ref, q_ref, k_ref,
):
    chunks, length = gate_ref.shape[1], gate_ref.shape[2]
    width = qk_ref.shape[2] // 2
    gate, forget = gate_ref[0], gate_ref[1]
    within = lane_cumsum(forget)
    ends = [within[r : r + 1, length - 1 :] for r in range(chunks)]
    after = [jnp.zeros((1, 1), F32)]
    for r in range(chunks - 1, 0, -1):
        after.insert(0, after[0] + ends[r])
    total = after[0] + ends[0]
    to_end = jnp.concatenate([e + a for e, a in zip(ends, after)], axis=0)
    end_log = to_end - within + gate
    level = jnp.max(jnp.max(end_log, axis=1, keepdims=True), axis=0, keepdims=True)
    fresh = columns_of(jnp.exp(end_log - level))
    state = jnp.zeros((2 * width, width * qk_ref.shape[0]), F32)
    for r in range(chunks):
        q_ref[r * length : (r + 1) * length] = joined(qk_ref, 0, width, r, length)
        key = joined(qk_ref, width, width, r, length)
        k_ref[r * length : (r + 1) * length] = key
        scaled = (fresh[:, r : r + 1] * key.astype(F32)).astype(BF16)
        state = state + dot(v_ref[r * length : (r + 1) * length], scaled, TN)
    rows, head_lanes = out_ref.shape[1], out_ref.shape[2]
    kept = state[:rows]
    row = lax.broadcasted_iota(jnp.int32, kept.shape, 0)
    lane = lax.broadcasted_iota(jnp.int32, kept.shape, 1)
    for at, value in ((0, level), (3, total)):
        high = value.astype(BF16).astype(F32)
        mid = (value - high).astype(BF16).astype(F32)
        low = value - high - mid
        for k, part in enumerate((high, mid, low)):
            kept = jnp.where((row == width + 1) & (lane == at + k), part, kept)
    chan = glu_ref.shape[2] // qk_ref.shape[0]
    hold = HOLD
    tail = glu_ref[glu_ref.shape[0] - 1, length - hold :].astype(F32)[:, glu_ref.shape[2] - chan :]
    group = head_lanes // chan
    each = hold // group
    tail = jnp.concatenate([tail[g * each : (g + 1) * each] for g in range(group)], axis=1)
    kept = jnp.concatenate([kept[: width + 2], tail, kept[width + 2 + each :]], axis=0)
    kept = kept.astype(BF16)
    for j in range(out_ref.shape[0]):
        out_ref[j] = kept


def local_kernel(place_ref, q_ref, k_ref, v_ref, gate_ref, glu_ref, taps_ref, out_ref, conv_ref):
    chunks, length = gate_ref.shape[1], gate_ref.shape[2]
    head = q_ref.shape[1]
    lanes = v_ref.shape[1]
    width = lanes // 2
    nx = chunks // glu_ref.shape[0]
    group = glu_ref.shape[0] * glu_ref.shape[1]
    glu = glu_ref[...].reshape(group, lanes).astype(F32)
    lane = lax.broadcasted_iota(jnp.int32, (HOLD, lanes), 1)
    before = pltpu.roll(glu[group - HOLD :], lanes // nx, 1)
    before = jnp.where(lane < lanes // nx, 0.0, before)
    weights = tap_rows(taps_ref, place_ref[1], place_ref[3], nx, lanes)
    conv_ref[...] = convolve(jnp.concatenate([before, glu], axis=0), weights)

    scale = head ** (-0.5)
    gate, forget = gate_ref[0], gate_ref[1]
    within = lane_cumsum(forget)
    turned = columns_of(jnp.concatenate([within, gate], axis=0))
    causal = lax.broadcasted_iota(jnp.int32, (length, length), 0) >= lax.broadcasted_iota(
        jnp.int32, (length, length), 1
    )
    lane = lax.broadcasted_iota(jnp.int32, (length, lanes), 1)
    state = jnp.zeros((lanes, head), F32)
    level = jnp.full((1, 1), LOW, F32)
    passed = jnp.zeros((1, 1), F32)
    for r in range(chunks):
        here = slice(r * length, (r + 1) * length)
        query, key, value = q_ref[here], k_ref[here], v_ref[here]
        within_row, gate_row = within[r : r + 1], gate[r : r + 1]
        within_col = turned[:, r : r + 1]
        gate_col = turned[:, chunks + r : chunks + r + 1]
        log_weight = jnp.where(causal, within_col - within_row + gate_row, -jnp.inf)
        carried = within_col + level
        top = jnp.maximum(carried, jnp.max(log_weight, axis=1, keepdims=True))
        weight = jnp.exp(log_weight - top)
        carried_weight = jnp.exp(carried - top) * scale
        scores = dot(query, key, NT) * (scale * weight)
        numer = dot(scores.astype(BF16), value, NN)
        denom = jnp.sum(scores, axis=1, keepdims=True)
        if r:
            older = dot(query, state.astype(BF16), NT)
            numer = numer + carried_weight * older
            denom = denom + carried_weight * older[:, width : width + 1]
        sent = jnp.where(lane == width, denom, numer)
        sent = jnp.where(lane == width + 1, top, sent)
        out_ref[here] = jnp.where(lane == width + 2, within_col + passed, sent)
        last = within_row[:, length - 1 :]
        passed = passed + last
        end_row = last - within_row + gate_row
        new_level = jnp.maximum(last + level, jnp.max(end_row, axis=1, keepdims=True))
        keep = jnp.exp(last + level - new_level)
        fresh = jnp.exp(last - within_col + gate_col - new_level)
        scaled = (fresh * key.astype(F32)).astype(BF16)
        state = keep * state + dot(value, scaled, TN)
        level = new_level


def cell_kernel(place_ref, in_ref, q_ref, local_ref, conv_ref, taps_ref, out_ref):
    members, rows, head = in_ref.shape
    nx, nc, ny, _, lanes = out_ref.shape
    width, chan = lanes // 2, lanes // nx
    length = q_ref.shape[0] // (nx * nc)
    scale = head ** (-0.5)
    place = place_ref[0]
    acc = jnp.zeros((1, 1), F32)
    logs = [None] * members
    for j in range(members - 1, -1, -1):
        line = in_ref[j, width + 1 : width + 2, :128].astype(F32)
        level_j = line[:, 0:1] + line[:, 1:2] + line[:, 2:3]
        total_j = line[:, 3:4] + line[:, 4:5] + line[:, 5:6]
        before = j < place
        logs[j] = jnp.where(before, level_j + acc, LOW)
        acc = acc + jnp.where(before, total_j, 0.0)
    level = logs[0]
    for j in range(1, members):
        level = jnp.maximum(level, logs[j])
    state = jnp.zeros((rows, head), F32)
    for j in range(members):
        weight = jnp.where(j < place, jnp.exp(logs[j] - level), 0.0)
        state = state + weight * in_ref[j].astype(F32)
    state = jnp.concatenate([state, jnp.zeros((lanes - rows, head), F32)], axis=0).astype(BF16)

    group = head // chan
    each = HOLD // group
    last_rows = in_ref[jnp.maximum(place - 1, 0), width : width + 8].astype(F32)
    last_rows = jnp.where(place > 0, last_rows[2 : 2 + each], 0.0)
    prior = jnp.concatenate([last_rows[:, g * chan : (g + 1) * chan] for g in range(group)], axis=0)
    prior = jnp.concatenate([prior, jnp.zeros((HOLD, lanes - chan), F32)], axis=1)
    weights = tap_rows(taps_ref, place_ref[1], place_ref[3], nx, lanes)
    edge = convolve(jnp.concatenate([prior, jnp.zeros((HOLD, lanes), F32)], axis=0), weights)
    half, quarter = length // 2, length // 4
    for r in range(nx * nc):
        here = slice(r * length, (r + 1) * length)
        local = local_ref[here]
        top_here, passed = local[:, width + 1 : width + 2], local[:, width + 2 : width + 3]
        carried = passed + level
        top = jnp.maximum(carried, top_here)
        local_weight = jnp.exp(top_here - top)
        carried_weight = jnp.exp(carried - top) * scale
        mixed = local_weight * local + carried_weight * dot(q_ref[here], state, NT)
        denom = mixed[:, width : width + 1]
        result = mixed[:, :width] / jnp.maximum(jnp.abs(denom), 1.0)
        x, c = r // nc, r % nc
        memory = jnp.concatenate([result[:half], result[half:]], axis=1)
        branch = []
        for g in range(4):
            at = c * length + g * quarter
            part = conv_ref[at : at + quarter]
            if at == 0:
                part = part + edge
            branch.append(part[:, x * chan : (x + 1) * chan])
        sent = jnp.concatenate([memory, jnp.concatenate(branch, axis=1)], axis=0).astype(BF16)
        for y in range(ny):
            out_ref[x, c, y] = sent


def vmem(count):
    return [pl.BlockSpec(memory_space=pltpu.VMEM)] * count


def layer(
    tokens,
    conv_value_weight,
    conv_gate_weight,
    conv_kernel,
    conv_norm_gain,
    query_weight,
    key_weight,
    value_weight,
    input_gate_weight,
    forget_gate_weight,
    input_offset,
    forget_offset,
    memory_norm_gain,
    conv_out_weight,
    memory_out_weight,
):
    nzh, nzl, nx, nc, ny = (size(a) for a in AXES)
    xi, ci, yi = lax.axis_index("x"), lax.axis_index("c"), lax.axis_index("tp")
    members = nzh * nzl
    zi = lax.axis_index("zh") * nzl + lax.axis_index("zl")
    length, part = tokens.shape
    slab = length * nx * nc
    head = query_weight.shape[1] // nc
    width = head // nx
    chan = conv_value_weight.shape[1] // nc // nx
    rows = query_weight.shape[0]
    wide = 3 * width + 2 * chan

    def from_z(value, ahead):
        return lax.ppermute(value, Z, [(j, (j - ahead) % members) for j in range(members)])

    deep = memory_out_weight.shape[0] + conv_out_weight.shape[0]
    pieces, out_rows = pl.pallas_call(
        piece_kernel,
        out_shape=(
            jax.ShapeDtypeStruct((nx, nc, rows, wide), BF16),
            jax.ShapeDtypeStruct((deep // wide * rows, wide), BF16),
        ),
        in_specs=vmem(7),
        out_specs=vmem(2),
        interpret=INTERPRET,
        name="pieces",
    )(
        query_weight,
        key_weight,
        value_weight,
        conv_value_weight,
        conv_gate_weight,
        memory_out_weight.T,
        conv_out_weight.T,
    )
    offsets = jnp.concatenate([input_offset.T, forget_offset.T], axis=0)
    call_pack = pl.pallas_call(
        pack_kernel,
        out_shape=jax.ShapeDtypeStruct((nx * ny, length + 8, part), BF16),
        in_specs=vmem(4),
        out_specs=pl.BlockSpec(memory_space=pltpu.VMEM),
        interpret=INTERPRET,
        name="pack",
    )
    sent = call_pack(tokens, offsets, conv_norm_gain[None], memory_norm_gain[None])
    mine = exchange(pieces.reshape(nx * nc, rows, wide), ("x", "c"))
    main = mine.reshape(nx * nc * rows, wide)
    mine = jnp.concatenate([main, out_rows], axis=0)
    step = members // 4
    far = [
        from_z(mine, -step),
        mine,
        from_z(mine, step),
        from_z(main, 2 * step),
        from_z(out_rows, -2 * step),
    ]
    own = exchange(sent, ("x", "tp")).reshape(nx, ny, length + 8, part)
    half_shape = (nzh // 2, *mine.shape)
    call_arrange = pl.pallas_call(
        arrange_kernel,
        out_shape=(
            jax.ShapeDtypeStruct((nzh, *mine.shape), BF16),
            jax.ShapeDtypeStruct(half_shape, BF16),
            jax.ShapeDtypeStruct(half_shape, BF16),
        ),
        in_specs=vmem(5),
        out_specs=vmem(3),
        interpret=INTERPRET,
        name="arrange",
    )
    near, *halves = call_arrange(*far)
    sets = [near, from_z(near, 1), from_z(near, -1)]
    sets += [from_z(halves[0], 2), from_z(halves[1], -2)]
    other = swapped(own, "c")

    gate_weight = jnp.pad(
        jnp.concatenate([input_gate_weight, forget_gate_weight], axis=1), ((0, 0), (0, 124))
    )
    place = jnp.stack([zi, ci, yi, xi])
    smem = pl.BlockSpec(memory_space=pltpu.SMEM)
    qk, value, packed, gates, gain, out_part = pl.pallas_call(
        project_kernel,
        out_shape=(
            jax.ShapeDtypeStruct((nx, nx, nc, length, 2 * width), BF16),
            jax.ShapeDtypeStruct((nx, nc, length, 2 * width), BF16),
            jax.ShapeDtypeStruct((nc, length, nx * chan), BF16),
            jax.ShapeDtypeStruct((2, nx * nc, length), F32),
            jax.ShapeDtypeStruct((ny, nc * nx, 2 * width), F32),
            jax.ShapeDtypeStruct((nzh, nzl, rows, deep), BF16),
        ),
        in_specs=[smem] + vmem(8),
        out_specs=vmem(6),
        interpret=INTERPRET,
        name="project",
    )(place, own, other, *sets, gate_weight)
    value = value.reshape(slab, 2 * width)
    all_qk = exchange(qk.reshape(nx, slab, 2 * width), "x")
    out_part = [out_part[0]] + [
        lax.ppermute(out_part[ahead], "tp", [(j, (j + ahead) % ny) for j in range(ny)])
        for ahead in range(1, ny)
    ]
    out_part = jnp.stack(out_part, axis=0)
    out_parts = [out_part] + [
        lax.ppermute(out_part, "x", [(j, (j - ahead) % nx) for j in range(nx)])
        for ahead in range(1, nx)
    ]
    other_parts = [swapped(out, "c") for out in out_parts]

    state_rows = width + 8
    call_slab = pl.pallas_call(
        slab_kernel,
        out_shape=(
            jax.ShapeDtypeStruct((members, state_rows, head), BF16),
            jax.ShapeDtypeStruct((slab, head), BF16),
            jax.ShapeDtypeStruct((slab, head), BF16),
        ),
        in_specs=vmem(4),
        out_specs=vmem(3),
        interpret=INTERPRET,
        name="slab_state",
    )
    states, query, key = call_slab(all_qk, value, gates, packed)
    states = exchange(states, Z)
    call_local = pl.pallas_call(
        local_kernel,
        out_shape=(
            jax.ShapeDtypeStruct((slab, 2 * width), F32),
            jax.ShapeDtypeStruct((nc * length, nx * chan), F32),
        ),
        in_specs=[smem] + vmem(6),
        out_specs=vmem(2),
        interpret=INTERPRET,
        name="local",
    )
    local, conv = call_local(place, query, key, value, gates, packed, conv_kernel)
    call_cell = pl.pallas_call(
        cell_kernel,
        out_shape=jax.ShapeDtypeStruct((nx, nc, ny, length // 4 * 3, 2 * width), BF16),
        in_specs=[smem] + vmem(5),
        out_specs=pl.BlockSpec(memory_space=pltpu.VMEM),
        interpret=INTERPRET,
        name="cell",
    )
    last = call_cell(place, states, query, local, conv, conv_kernel)
    arrived = exchange(last.reshape(nx * nc * ny, length // 4 * 3, -1), ("x", "c", "tp"))
    arrived = arrived.reshape(nx, nc, ny, length // 4 * 3, -1)
    call_assemble = pl.pallas_call(
        assemble_kernel,
        out_shape=jax.ShapeDtypeStruct((ny, nzl, nx, nc, rows, deep), BF16),
        in_specs=[smem] + vmem(2 * nx),
        out_specs=pl.BlockSpec(memory_space=pltpu.VMEM),
        interpret=INTERPRET,
        name="assemble",
    )
    out_weight = call_assemble(place, *out_parts, *other_parts)
    return pl.pallas_call(
        finish_kernel,
        out_shape=jax.ShapeDtypeStruct((length, part), BF16),
        in_specs=vmem(3),
        out_specs=pl.BlockSpec(memory_space=pltpu.VMEM),
        interpret=INTERPRET,
        name="finish",
    )(arrived, out_weight, gain)


def solution(mesh):
    shape = mesh.shape
    depth = shape["sp"] // 32
    split = Mesh(mesh.devices.reshape(4, depth, 4, 2, shape["tp"]), AXES)
    in_specs = (
        P(SP, "tp"),
        P(SP, "tp"),
        P(SP, "tp"),
        P(None, "tp"),
        P("tp"),
        P(SP, "tp"),
        P(SP, "tp"),
        P(SP, "tp"),
        P(None, "tp"),
        P(None, "tp"),
        P(SP, "tp"),
        P(SP, "tp"),
        P("tp"),
        P("tp", SP),
        P("tp", SP),
    )
    return jax.shard_map(
        layer, mesh=split, in_specs=in_specs, out_specs=P(SP, "tp"), check_vma=False
    )
```

```python
import jax
import jax.numpy as jnp
from jax import lax
from jax.experimental import pallas as pl
from jax.experimental.pallas import tpu as pltpu
from jax.sharding import Mesh
from jax.sharding import PartitionSpec as P

AXES = ("zh", "zl", "x", "c", "tp")
Z = ("zh", "zl")
SP = ("zh", "zl", "x", "c")
EPS = 1e-06
LOW = -1e30
F32 = jnp.float32
BF16 = jnp.bfloat16
INTERPRET = False


def size(axis):
    return lax.axis_size(axis)


def exchange(pieces, axes):
    return lax.all_to_all(pieces, axes, split_axis=0, concat_axis=0, tiled=True)


def swapped(value, axis):
    return lax.ppermute(value, axis, [(0, 1), (1, 0)])


def lane_cumsum(rows):
    lane = lax.broadcasted_iota(jnp.int32, rows.shape, 1)
    step = 1
    while step < rows.shape[1]:
        moved = pltpu.roll(rows, step, 1)
        rows = rows + jnp.where(lane >= step, moved, 0.0)
        step *= 2
    return rows


def columns_of(rows):
    count, length = rows.shape
    square = jnp.concatenate([rows, jnp.zeros((length - count, length), F32)], axis=0)
    return square.T


def dot(a, b, dims):
    return lax.dot_general(a, b, (dims, ((), ())), preferred_element_type=F32)


NN = ((1,), (0,))
NT = ((1,), (1,))
TN = ((0,), (0,))


def joined(parts_ref, start, width, chunk, length):
    picked = [
        parts_ref[j, chunk * length : (chunk + 1) * length, start : start + width]
        for j in range(parts_ref.shape[0])
    ]
    return jnp.concatenate(picked, axis=1)


def three_parts(value):
    high = value.astype(BF16).astype(F32)
    mid = (value - high).astype(BF16).astype(F32)
    return high, mid, value - high - mid


def pack_kernel(tokens_ref, offsets_ref, conv_gain_ref, memory_gain_ref, out_ref):
    length = tokens_ref.shape[0]
    offsets = three_parts(offsets_ref[...])
    conv_gain = three_parts(conv_gain_ref[...])
    memory_gain = three_parts(memory_gain_ref[...])
    rows = [jnp.concatenate([p[k : k + 1] for k in range(p.shape[0])], axis=1) for p in offsets]
    rows += memory_gain
    rows.append(jnp.concatenate(conv_gain[:2], axis=1))
    rows.append(jnp.concatenate([conv_gain[2], jnp.zeros_like(conv_gain[2])], axis=1))
    extra = jnp.concatenate(rows, axis=0).astype(BF16)
    tokens = tokens_ref[...]
    for j in range(out_ref.shape[0]):
        out_ref[j, :length] = tokens
        out_ref[j, length:] = extra


def piece_kernel(
    query_ref, key_ref, value_ref, left_ref, right_ref, memory_ref, conv_ref, out_ref, turn_ref
):
    nx, nc = out_ref.shape[0], out_ref.shape[1]
    rows = memory_ref.shape[0]
    width, chan = memory_ref.shape[1] // (nx * nc), conv_ref.shape[1] // (nx * nc)
    parts = []
    for at in range(nx * nc):
        parts.append(memory_ref[:, at * width : (at + 1) * width])
        parts.append(conv_ref[:, at * chan : (at + 1) * chan])
    whole = jnp.concatenate(parts, axis=1)
    wide = out_ref.shape[3]
    for j in range(whole.shape[1] // wide):
        turn_ref[j * rows : (j + 1) * rows] = whole[:, j * wide : (j + 1) * wide]
    for x in range(nx):
        for c in range(nc):
            at = c * nx + x
            parts = []
            for ref in (query_ref, key_ref, value_ref, left_ref, right_ref):
                width = ref.shape[1] // (nx * nc)
                parts.append(ref[:, at * width : (at + 1) * width])
            out_ref[x, c] = jnp.concatenate(parts, axis=1)


def arrange_kernel(
    before_ref, mine_ref, after_ref, main_ref, rest_ref, near_ref, low_ref, high_ref
):
    rows = main_ref.shape[0]
    for refs in ((near_ref, 0), (high_ref, 0)):
        refs[0][refs[1]] = before_ref[...]
    for refs in ((near_ref, 1), (high_ref, 1), (low_ref, 0)):
        refs[0][refs[1]] = mine_ref[...]
    for refs in ((near_ref, 2), (low_ref, 1)):
        refs[0][refs[1]] = after_ref[...]
    near_ref[3, :rows] = main_ref[...]
    near_ref[3, rows:] = rest_ref[...]


def assemble_kernel(place_ref, *refs):
    out_ref = refs[-1]
    nx, ny = out_ref.shape[2], out_ref.shape[0]
    core, column, x_at = place_ref[1], place_ref[2], place_ref[3]
    for ahead in range(nx):
        x = lax.rem(x_at + ahead, nx)
        for c, ref in ((core, refs[ahead]), (1 - core, refs[nx + ahead])):
            for b in range(ny):
                at = lax.rem(column + ny - b, ny)
                for near in range(ref.shape[1]):
                    out_ref[pl.ds(at, 1), near, pl.ds(x, 1), pl.ds(c, 1)] = ref[b, near][
                        None, None, None
                    ]


def project_kernel(
    place_ref, own_ref, other_ref,
    w0_ref, w1_ref, w3_ref, low_ref, high_ref, gate_ref,
    qk_ref, v_ref, glu_ref, gates_ref, gain_ref, out_weight_ref,
):
    nx, ny, _, part = own_ref.shape
    far, tall, wide = w0_ref.shape
    depth, chunks = out_weight_ref.shape[2], out_weight_ref.shape[3] // wide
    rows = tall - depth * chunks
    close = part // rows
    length = glu_ref.shape[1]
    place, core, column = place_ref[0], place_ref[1], place_ref[2]
    tokens_rows = nx * length
    width = qk_ref.shape[4] // 2
    chan = glu_ref.shape[2] // nx
    lane = lax.broadcasted_iota(jnp.int32, (length, width), 1)
    ones = jnp.where(lane == 0, 1.0, 0.0).astype(BF16)
    row = lax.broadcasted_iota(jnp.int32, (2 * nx, length), 0)
    gate_in = jnp.zeros((2 * nx, length), F32)
    forget = jnp.zeros((2 * nx, length), F32)

    members = far * close
    blocks = [
        (ref, i, ahead + close * (i - 1))
        for ref, ahead in ((w0_ref, 0), (w1_ref, 1), (w3_ref, -1))
        for i in range(far)
    ]
    blocks += [(low_ref, i, 2 + close * i) for i in range(far // 2)]
    blocks += [(high_ref, i, -2 + close * (i - 1)) for i in range(far // 2)]
    homes = []
    for ref, i, ahead in blocks:
        home = lax.rem(place + (ahead + members), members)
        y = lax.div(home, close)
        homes.append((y, lax.rem(home, close)))
        behind = lax.rem(y + ny - column, ny)
        out_weight_ref[pl.ds(behind, 1), pl.ds(homes[-1][1], 1)] = jnp.concatenate(
            [ref[i, rows + j * depth : rows + (j + 1) * depth] for j in range(chunks)], axis=1
        )[None, None]
    for half, ref in enumerate((own_ref, other_ref)):
        home = core if half == 0 else 1 - core
        acc = jnp.zeros((tokens_rows, wide), F32)
        pre = jnp.zeros((tokens_rows, gate_ref.shape[1]), F32)
        for pair in range(0, len(blocks), 2):
            left, right, gate_rows = [], [], []
            for at in (pair, pair + 1):
                w_ref, i, _ = blocks[at]
                y, z = homes[at]
                start = pl.multiple_of(z * rows, rows)
                left.append(
                    ref[:, pl.ds(y, 1), :length, pl.ds(start, rows)].reshape(tokens_rows, rows)
                )
                right.append(w_ref[i, :rows])
                gate_rows.append(gate_ref[pl.ds(y * part + start, rows)])
            lhs = jnp.concatenate(left, axis=1)
            acc = acc + dot(lhs, jnp.concatenate(right, axis=0), NN)
            pre = pre + dot(lhs, jnp.concatenate(gate_rows, axis=0), NN)
        glu = []
        for x in range(nx):
            mine = acc[x * length : (x + 1) * length]
            qk = mine[:, : 2 * width].astype(BF16)[None]
            for j in range(qk_ref.shape[0]):
                qk_ref[j, x, pl.ds(home, 1)] = qk
            v_ref[x, pl.ds(home, 1)] = jnp.concatenate(
                [mine[:, 2 * width : 3 * width].astype(BF16), ones], axis=1
            )[None]
            left = mine[:, 3 * width : 3 * width + chan]
            right = mine[:, 3 * width + chan :]
            glu.append(left / (1.0 + jnp.exp(-right)))
        glu_ref[pl.ds(home, 1)] = jnp.concatenate(glu, axis=1).astype(BF16)[None]
        for x in range(nx):
            turned = pre[x * length : (x + 1) * length].T
            extra = ref[x, column, length : length + 8].astype(F32)
            values = extra[0:1] + extra[1:2] + extra[2:3]
            offsets = jnp.where(core == 0, values[:, :length], values[:, length : 2 * length])
            offsets_f = jnp.where(
                core == 0, values[:, 2 * length : 3 * length], values[:, 3 * length : 4 * length]
            )
            at = row == 2 * x + home
            gate_pre = jnp.where(core == 0, turned[0:1], turned[1:2])
            forget_pre = jnp.where(core == 0, turned[2:3], turned[3:4])
            gate_in = jnp.where(at, gate_pre + offsets, gate_in)
            forget = jnp.where(at, forget_pre + offsets_f, forget)
    for b in range(ny):
        extra = own_ref[0, b, length : length + 8].astype(F32)
        memory_gain = extra[3:4] + extra[4:5] + extra[5:6]
        half = part // 2
        conv_gain = extra[6:7, :half] + extra[6:7, half:] + extra[7:8, :half]
        for at in range(2 * nx):
            gain_ref[b, at : at + 1] = jnp.concatenate(
                [
                    memory_gain[:, at * width : (at + 1) * width],
                    conv_gain[:, at * chan : (at + 1) * chan],
                    jnp.zeros((1, width - chan), F32),
                ],
                axis=1,
            )
    y = jnp.exp(-jnp.abs(forget))
    small = y * (1.0 - y * (1 / 2 - y * (1 / 3 - y * (1 / 4 - y * (1 / 5)))))
    gates_ref[0] = gate_in
    gates_ref[1] = jnp.minimum(forget, 0.0) - jnp.where(y < 0.03, small, jnp.log(1.0 + y))


def finish_kernel(arrived_ref, weight_ref, gain_ref, out_ref):
    nx, nc, ny, _, lanes = arrived_ref.shape
    width = lanes // 2
    chan = width // 2
    length, part = out_ref.shape
    lane = lax.broadcasted_iota(jnp.int32, (length, width + chan), 1)
    is_memory = lane < width
    half = length // 2

    def block(x, c, b):
        got = arrived_ref[x, c, b].astype(F32)
        memory = jnp.concatenate([got[:half, :width], got[:half, width:]], axis=0)
        conv = [got[half:, k * chan : (k + 1) * chan] for k in range(4)]
        return jnp.concatenate([memory, jnp.concatenate(conv, axis=0)], axis=1)

    blocks = {
        (x, c, b): block(x, c, b) for x in range(nx) for c in range(nc) for b in range(ny)
    }
    first = sum(blocks.values())
    second = sum(got * got for got in blocks.values())
    senders = nx * nc * ny
    memory_mean = jnp.sum(jnp.where(is_memory, second, 0.0), axis=1, keepdims=True)
    scale = lax.rsqrt(memory_mean / (senders * width) + EPS)
    mean = jnp.sum(jnp.where(is_memory, 0.0, first), axis=1, keepdims=True) / (senders * chan)
    power = jnp.sum(jnp.where(is_memory, 0.0, second), axis=1, keepdims=True) / (senders * chan)
    spread = lax.rsqrt(power - mean * mean + EPS)
    shift = jnp.where(is_memory, 0.0, mean)
    factor = jnp.where(is_memory, scale, spread)
    deep = weight_ref.shape[5]
    total = jnp.zeros((length, part), F32)
    for b in range(ny):
        left = []
        for c in range(nc):
            for x in range(nx):
                gain = gain_ref[b, c * nx + x : c * nx + x + 1, : width + chan]
                normed = (blocks[x, c, b] - shift) * factor * gain
                branch = normed / (1.0 + jnp.exp(-normed))
                left.append(jnp.where(is_memory, normed, branch).astype(BF16))
        total = total + dot(
            jnp.concatenate(left, axis=1), weight_ref[b].reshape(part, deep), NT
        )
    out_ref[...] = total.astype(BF16)


HOLD = 32


def tap_rows(taps_ref, core, x_at, nx, lanes):
    chan = lanes // nx
    weights = taps_ref[...].astype(F32)
    weights = jnp.where(core == 0, weights[:, :lanes], weights[:, lanes:])
    weights = pltpu.roll(weights, lax.rem(lanes - chan * x_at, lanes), 1)
    weights = jnp.where(lax.broadcasted_iota(jnp.int32, weights.shape, 1) < chan, weights, 0.0)
    return sum(pltpu.roll(weights, chan * k, 1) for k in range(1, nx)) + weights


def convolve(extended, weights):
    taps = weights.shape[0]
    length = extended.shape[0] - HOLD
    total = jnp.zeros((length, extended.shape[1]), F32)
    first = HOLD - (taps - 1)
    for shift in range(8):
        moved = extended[shift : shift + length + HOLD - 8] if shift else extended
        for j in range(taps):
            at = first + j
            if at % 8 == shift:
                total = total + moved[at - shift : at - shift + length] * weights[j : j + 1]
    return total


def with_logs(kept, width, level, total):
    row = lax.broadcasted_iota(jnp.int32, kept.shape, 0)
    lane = lax.broadcasted_iota(jnp.int32, kept.shape, 1)
    for at, value in ((0, level), (3, total)):
        for k, part in enumerate(three_parts(value)):
            kept = jnp.where((row == width + 1) & (lane == at + k), part, kept)
    return kept


def read_logs(block, width):
    line = block[width + 1 : width + 2, :128].astype(F32)
    level = line[:, 0:1] + line[:, 1:2] + line[:, 2:3]
    return level, line[:, 3:4] + line[:, 4:5] + line[:, 5:6]


def merged(blocks, passed, width):
    acc = jnp.zeros((1, 1), F32)
    logs = []
    for block, use in zip(blocks[::-1], passed[::-1]):
        level, total = read_logs(block, width)
        logs.insert(0, jnp.where(use, level + acc, LOW))
        acc = acc + jnp.where(use, total, 0.0)
    level = logs[0]
    for log in logs[1:]:
        level = jnp.maximum(level, log)
    state = jnp.zeros(blocks[0].shape, F32)
    for block, use, log in zip(blocks, passed, logs):
        state = state + jnp.where(use, jnp.exp(log - level), 0.0) * block.astype(F32)
    return state, level, acc


def group_kernel(in_ref, out_ref):
    members, rows, _ = in_ref.shape
    width = rows - 8
    blocks = [in_ref[j] for j in range(members)]
    state, level, total = merged(blocks, [True] * members, width)
    last = blocks[-1].astype(F32)
    kept = jnp.concatenate([state[: width + 2], last[width + 2 :]], axis=0)
    kept = with_logs(kept, width, level, total).astype(BF16)
    for j in range(out_ref.shape[0]):
        out_ref[j] = kept


def slab_kernel(
    qk_ref, v_ref, gate_ref, glu_ref, out_ref, q_ref, k_ref,
):
    chunks, length = gate_ref.shape[1], gate_ref.shape[2]
    width = qk_ref.shape[2] // 2
    gate, forget = gate_ref[0], gate_ref[1]
    within = lane_cumsum(forget)
    ends = [within[r : r + 1, length - 1 :] for r in range(chunks)]
    after = [jnp.zeros((1, 1), F32)]
    for r in range(chunks - 1, 0, -1):
        after.insert(0, after[0] + ends[r])
    total = after[0] + ends[0]
    to_end = jnp.concatenate([e + a for e, a in zip(ends, after)], axis=0)
    end_log = to_end - within + gate
    level = jnp.max(jnp.max(end_log, axis=1, keepdims=True), axis=0, keepdims=True)
    fresh = columns_of(jnp.exp(end_log - level))
    state = jnp.zeros((2 * width, width * qk_ref.shape[0]), F32)
    for r in range(chunks):
        q_ref[r * length : (r + 1) * length] = joined(qk_ref, 0, width, r, length)
        key = joined(qk_ref, width, width, r, length)
        k_ref[r * length : (r + 1) * length] = key
        scaled = (fresh[:, r : r + 1] * key.astype(F32)).astype(BF16)
        state = state + dot(v_ref[r * length : (r + 1) * length], scaled, TN)
    rows, head_lanes = out_ref.shape[1], out_ref.shape[2]
    kept = state[:rows]
    kept = with_logs(kept, width, level, total)
    chan = glu_ref.shape[2] // qk_ref.shape[0]
    hold = HOLD
    tail = glu_ref[glu_ref.shape[0] - 1, length - hold :].astype(F32)[:, glu_ref.shape[2] - chan :]
    group = head_lanes // chan
    each = hold // group
    tail = jnp.concatenate([tail[g * each : (g + 1) * each] for g in range(group)], axis=1)
    kept = jnp.concatenate([kept[: width + 2], tail, kept[width + 2 + each :]], axis=0)
    kept = kept.astype(BF16)
    for j in range(out_ref.shape[0]):
        out_ref[j] = kept


def local_kernel(place_ref, q_ref, k_ref, v_ref, gate_ref, glu_ref, taps_ref, out_ref, conv_ref):
    chunks, length = gate_ref.shape[1], gate_ref.shape[2]
    head = q_ref.shape[1]
    lanes = v_ref.shape[1]
    width = lanes // 2
    nx = chunks // glu_ref.shape[0]
    group = glu_ref.shape[0] * glu_ref.shape[1]
    glu = glu_ref[...].reshape(group, lanes).astype(F32)
    lane = lax.broadcasted_iota(jnp.int32, (HOLD, lanes), 1)
    before = pltpu.roll(glu[group - HOLD :], lanes // nx, 1)
    before = jnp.where(lane < lanes // nx, 0.0, before)
    weights = tap_rows(taps_ref, place_ref[1], place_ref[3], nx, lanes)
    conv_ref[...] = convolve(jnp.concatenate([before, glu], axis=0), weights)

    scale = head ** (-0.5)
    gate, forget = gate_ref[0], gate_ref[1]
    within = lane_cumsum(forget)
    turned = columns_of(jnp.concatenate([within, gate], axis=0))
    causal = lax.broadcasted_iota(jnp.int32, (length, length), 0) >= lax.broadcasted_iota(
        jnp.int32, (length, length), 1
    )
    lane = lax.broadcasted_iota(jnp.int32, (length, lanes), 1)
    state = jnp.zeros((lanes, head), F32)
    level = jnp.full((1, 1), LOW, F32)
    passed = jnp.zeros((1, 1), F32)
    for r in range(chunks):
        here = slice(r * length, (r + 1) * length)
        query, key, value = q_ref[here], k_ref[here], v_ref[here]
        within_row, gate_row = within[r : r + 1], gate[r : r + 1]
        within_col = turned[:, r : r + 1]
        gate_col = turned[:, chunks + r : chunks + r + 1]
        log_weight = jnp.where(causal, within_col - within_row + gate_row, -jnp.inf)
        carried = within_col + level
        top = jnp.maximum(carried, jnp.max(log_weight, axis=1, keepdims=True))
        weight = jnp.exp(log_weight - top)
        carried_weight = jnp.exp(carried - top) * scale
        scores = dot(query, key, NT) * (scale * weight)
        numer = dot(scores.astype(BF16), value, NN)
        denom = jnp.sum(scores, axis=1, keepdims=True)
        if r:
            older = dot(query, state.astype(BF16), NT)
            numer = numer + carried_weight * older
            denom = denom + carried_weight * older[:, width : width + 1]
        sent = jnp.where(lane == width, denom, numer)
        sent = jnp.where(lane == width + 1, top, sent)
        out_ref[here] = jnp.where(lane == width + 2, within_col + passed, sent)
        last = within_row[:, length - 1 :]
        passed = passed + last
        end_row = last - within_row + gate_row
        new_level = jnp.maximum(last + level, jnp.max(end_row, axis=1, keepdims=True))
        keep = jnp.exp(last + level - new_level)
        fresh = jnp.exp(last - within_col + gate_col - new_level)
        scaled = (fresh * key.astype(F32)).astype(BF16)
        state = keep * state + dot(value, scaled, TN)
        level = new_level


def cell_kernel(place_ref, far_ref, in_ref, q_ref, local_ref, conv_ref, taps_ref, out_ref):
    members, rows, head = in_ref.shape
    groups = far_ref.shape[0]
    nx, nc, ny, _, lanes = out_ref.shape
    width, chan = lanes // 2, lanes // nx
    length = q_ref.shape[0] // (nx * nc)
    scale = head ** (-0.5)
    place = place_ref[0]
    at_far, at_close = lax.div(place, members), lax.rem(place, members)
    blocks = [far_ref[j] for j in range(groups)] + [in_ref[j] for j in range(members)]
    passed = [j < at_far for j in range(groups)] + [j < at_close for j in range(members)]
    state, level, _ = merged(blocks, passed, width)
    state = jnp.concatenate([state, jnp.zeros((lanes - rows, head), F32)], axis=0).astype(BF16)

    group = head // chan
    each = HOLD // group
    near_rows = in_ref[jnp.maximum(at_close - 1, 0), width : width + 8].astype(F32)
    far_rows = far_ref[jnp.maximum(at_far - 1, 0), width : width + 8].astype(F32)
    last_rows = jnp.where(at_close > 0, near_rows, jnp.where(at_far > 0, far_rows, 0.0))
    last_rows = last_rows[2 : 2 + each]
    prior = jnp.concatenate([last_rows[:, g * chan : (g + 1) * chan] for g in range(group)], axis=0)
    prior = jnp.concatenate([prior, jnp.zeros((HOLD, lanes - chan), F32)], axis=1)
    weights = tap_rows(taps_ref, place_ref[1], place_ref[3], nx, lanes)
    edge = convolve(jnp.concatenate([prior, jnp.zeros((HOLD, lanes), F32)], axis=0), weights)
    half, quarter = length // 2, length // 4
    for r in range(nx * nc):
        here = slice(r * length, (r + 1) * length)
        local = local_ref[here]
        top_here, since = local[:, width + 1 : width + 2], local[:, width + 2 : width + 3]
        carried = since + level
        top = jnp.maximum(carried, top_here)
        local_weight = jnp.exp(top_here - top)
        carried_weight = jnp.exp(carried - top) * scale
        mixed = local_weight * local + carried_weight * dot(q_ref[here], state, NT)
        denom = mixed[:, width : width + 1]
        result = mixed[:, :width] / jnp.maximum(jnp.abs(denom), 1.0)
        x, c = r // nc, r % nc
        memory = jnp.concatenate([result[:half], result[half:]], axis=1)
        branch = []
        for g in range(4):
            at = c * length + g * quarter
            part = conv_ref[at : at + quarter]
            if at == 0:
                part = part + edge
            branch.append(part[:, x * chan : (x + 1) * chan])
        sent = jnp.concatenate([memory, jnp.concatenate(branch, axis=1)], axis=0).astype(BF16)
        for y in range(ny):
            out_ref[x, c, y] = sent


def vmem(count):
    return [pl.BlockSpec(memory_space=pltpu.VMEM)] * count


def layer(
    tokens,
    conv_value_weight,
    conv_gate_weight,
    conv_kernel,
    conv_norm_gain,
    query_weight,
    key_weight,
    value_weight,
    input_gate_weight,
    forget_gate_weight,
    input_offset,
    forget_offset,
    memory_norm_gain,
    conv_out_weight,
    memory_out_weight,
):
    nzh, nzl, nx, nc, ny = (size(a) for a in AXES)
    xi, ci, yi = lax.axis_index("x"), lax.axis_index("c"), lax.axis_index("tp")
    members = nzh * nzl
    zi = lax.axis_index("zh") * nzl + lax.axis_index("zl")
    length, part = tokens.shape
    slab = length * nx * nc
    head = query_weight.shape[1] // nc
    width = head // nx
    chan = conv_value_weight.shape[1] // nc // nx
    rows = query_weight.shape[0]
    wide = 3 * width + 2 * chan

    def from_z(value, ahead):
        return lax.ppermute(value, Z, [(j, (j - ahead) % members) for j in range(members)])

    deep = memory_out_weight.shape[0] + conv_out_weight.shape[0]
    pieces, out_rows = pl.pallas_call(
        piece_kernel,
        out_shape=(
            jax.ShapeDtypeStruct((nx, nc, rows, wide), BF16),
            jax.ShapeDtypeStruct((deep // wide * rows, wide), BF16),
        ),
        in_specs=vmem(7),
        out_specs=vmem(2),
        interpret=INTERPRET,
        name="pieces",
    )(
        query_weight,
        key_weight,
        value_weight,
        conv_value_weight,
        conv_gate_weight,
        memory_out_weight.T,
        conv_out_weight.T,
    )
    offsets = jnp.concatenate([input_offset.T, forget_offset.T], axis=0)
    call_pack = pl.pallas_call(
        pack_kernel,
        out_shape=jax.ShapeDtypeStruct((nx * ny, length + 8, part), BF16),
        in_specs=vmem(4),
        out_specs=pl.BlockSpec(memory_space=pltpu.VMEM),
        interpret=INTERPRET,
        name="pack",
    )
    sent = call_pack(tokens, offsets, conv_norm_gain[None], memory_norm_gain[None])
    mine = exchange(pieces.reshape(nx * nc, rows, wide), ("x", "c"))
    main = mine.reshape(nx * nc * rows, wide)
    mine = jnp.concatenate([main, out_rows], axis=0)
    step = members // 4
    far = [
        from_z(mine, -step),
        mine,
        from_z(mine, step),
        from_z(main, 2 * step),
        from_z(out_rows, -2 * step),
    ]
    own = exchange(sent, ("x", "tp")).reshape(nx, ny, length + 8, part)
    half_shape = (nzh // 2, *mine.shape)
    call_arrange = pl.pallas_call(
        arrange_kernel,
        out_shape=(
            jax.ShapeDtypeStruct((nzh, *mine.shape), BF16),
            jax.ShapeDtypeStruct(half_shape, BF16),
            jax.ShapeDtypeStruct(half_shape, BF16),
        ),
        in_specs=vmem(5),
        out_specs=vmem(3),
        interpret=INTERPRET,
        name="arrange",
    )
    near, *halves = call_arrange(*far)
    sets = [near, from_z(near, 1), from_z(near, -1)]
    sets += [from_z(halves[0], 2), from_z(halves[1], -2)]
    other = swapped(own, "c")

    gate_weight = jnp.pad(
        jnp.concatenate([input_gate_weight, forget_gate_weight], axis=1), ((0, 0), (0, 124))
    )
    place = jnp.stack([zi, ci, yi, xi])
    smem = pl.BlockSpec(memory_space=pltpu.SMEM)
    qk, value, packed, gates, gain, out_part = pl.pallas_call(
        project_kernel,
        out_shape=(
            jax.ShapeDtypeStruct((nx, nx, nc, length, 2 * width), BF16),
            jax.ShapeDtypeStruct((nx, nc, length, 2 * width), BF16),
            jax.ShapeDtypeStruct((nc, length, nx * chan), BF16),
            jax.ShapeDtypeStruct((2, nx * nc, length), F32),
            jax.ShapeDtypeStruct((ny, nc * nx, 2 * width), F32),
            jax.ShapeDtypeStruct((nzh, nzl, rows, deep), BF16),
        ),
        in_specs=[smem] + vmem(8),
        out_specs=vmem(6),
        interpret=INTERPRET,
        name="project",
    )(place, own, other, *sets, gate_weight)
    value = value.reshape(slab, 2 * width)
    all_qk = exchange(qk.reshape(nx, slab, 2 * width), "x")
    out_part = [out_part[0]] + [
        lax.ppermute(out_part[ahead], "tp", [(j, (j + ahead) % ny) for j in range(ny)])
        for ahead in range(1, ny)
    ]
    out_part = jnp.stack(out_part, axis=0)
    out_parts = [out_part] + [
        lax.ppermute(out_part, "x", [(j, (j - ahead) % nx) for j in range(nx)])
        for ahead in range(1, nx)
    ]
    other_parts = [swapped(out, "c") for out in out_parts]

    state_rows = width + 8
    call_slab = pl.pallas_call(
        slab_kernel,
        out_shape=(
            jax.ShapeDtypeStruct((nzl, state_rows, head), BF16),
            jax.ShapeDtypeStruct((slab, head), BF16),
            jax.ShapeDtypeStruct((slab, head), BF16),
        ),
        in_specs=vmem(4),
        out_specs=vmem(3),
        interpret=INTERPRET,
        name="slab_state",
    )
    states, query, key = call_slab(all_qk, value, gates, packed)
    states = exchange(states, "zl")
    call_group = pl.pallas_call(
        group_kernel,
        out_shape=jax.ShapeDtypeStruct((nzh, state_rows, head), BF16),
        in_specs=vmem(1),
        out_specs=pl.BlockSpec(memory_space=pltpu.VMEM),
        interpret=INTERPRET,
        name="group",
    )
    groups = call_group(states)
    groups = exchange(groups, "zh")
    call_local = pl.pallas_call(
        local_kernel,
        out_shape=(
            jax.ShapeDtypeStruct((slab, 2 * width), F32),
            jax.ShapeDtypeStruct((nc * length, nx * chan), F32),
        ),
        in_specs=[smem] + vmem(6),
        out_specs=vmem(2),
        interpret=INTERPRET,
        name="local",
    )
    local, conv = call_local(place, query, key, value, gates, packed, conv_kernel)
    call_cell = pl.pallas_call(
        cell_kernel,
        out_shape=jax.ShapeDtypeStruct((nx, nc, ny, length // 4 * 3, 2 * width), BF16),
        in_specs=[smem] + vmem(6),
        out_specs=pl.BlockSpec(memory_space=pltpu.VMEM),
        interpret=INTERPRET,
        name="cell",
    )
    last = call_cell(place, groups, states, query, local, conv, conv_kernel)
    arrived = exchange(last.reshape(nx * nc * ny, length // 4 * 3, -1), ("x", "c", "tp"))
    arrived = arrived.reshape(nx, nc, ny, length // 4 * 3, -1)
    call_assemble = pl.pallas_call(
        assemble_kernel,
        out_shape=jax.ShapeDtypeStruct((ny, nzl, nx, nc, rows, deep), BF16),
        in_specs=[smem] + vmem(2 * nx),
        out_specs=pl.BlockSpec(memory_space=pltpu.VMEM),
        interpret=INTERPRET,
        name="assemble",
    )
    out_weight = call_assemble(place, *out_parts, *other_parts)
    return pl.pallas_call(
        finish_kernel,
        out_shape=jax.ShapeDtypeStruct((length, part), BF16),
        in_specs=vmem(3),
        out_specs=pl.BlockSpec(memory_space=pltpu.VMEM),
        interpret=INTERPRET,
        name="finish",
    )(arrived, out_weight, gain)


def solution(mesh):
    shape = mesh.shape
    depth = shape["sp"] // 32
    split = Mesh(mesh.devices.reshape(4, depth, 4, 2, shape["tp"]), AXES)
    in_specs = (
        P(SP, "tp"),
        P(SP, "tp"),
        P(SP, "tp"),
        P(None, "tp"),
        P("tp"),
        P(SP, "tp"),
        P(SP, "tp"),
        P(SP, "tp"),
        P(None, "tp"),
        P(None, "tp"),
        P(SP, "tp"),
        P(SP, "tp"),
        P("tp"),
        P("tp", SP),
        P("tp", SP),
    )
    return jax.shard_map(
        layer, mesh=split, in_specs=in_specs, out_specs=P(SP, "tp"), check_vma=False
    )
```

```python
import jax
import jax.numpy as jnp
from jax import lax
from jax.experimental import pallas as pl
from jax.experimental.pallas import tpu as pltpu
from jax.sharding import Mesh
from jax.sharding import PartitionSpec as P

AXES = ("zh", "zl", "x", "c", "tp")
Z = ("zh", "zl")
SP = ("zh", "zl", "x", "c")
EPS = 1e-06
LOW = -1e30
F32 = jnp.float32
BF16 = jnp.bfloat16
INTERPRET = False


def size(axis):
    return lax.axis_size(axis)


def exchange(pieces, axes):
    return lax.all_to_all(pieces, axes, split_axis=0, concat_axis=0, tiled=True)


def swapped(value, axis):
    return lax.ppermute(value, axis, [(0, 1), (1, 0)])


def lane_cumsum(rows):
    lane = lax.broadcasted_iota(jnp.int32, rows.shape, 1)
    step = 1
    while step < rows.shape[1]:
        moved = pltpu.roll(rows, step, 1)
        rows = rows + jnp.where(lane >= step, moved, 0.0)
        step *= 2
    return rows


def columns_of(rows):
    count, length = rows.shape
    square = jnp.concatenate([rows, jnp.zeros((length - count, length), F32)], axis=0)
    return square.T


def dot(a, b, dims):
    return lax.dot_general(a, b, (dims, ((), ())), preferred_element_type=F32)


NN = ((1,), (0,))
NT = ((1,), (1,))
TN = ((0,), (0,))


def joined(parts_ref, start, width, chunk, length):
    picked = [
        parts_ref[j, chunk * length : (chunk + 1) * length, start : start + width]
        for j in range(parts_ref.shape[0])
    ]
    return jnp.concatenate(picked, axis=1)


def three_parts(value):
    high = value.astype(BF16).astype(F32)
    mid = (value - high).astype(BF16).astype(F32)
    return high, mid, value - high - mid


def pack_kernel(tokens_ref, offsets_ref, conv_gain_ref, memory_gain_ref, out_ref):
    length = tokens_ref.shape[0]
    offsets = three_parts(offsets_ref[...])
    conv_gain = three_parts(conv_gain_ref[...])
    memory_gain = three_parts(memory_gain_ref[...])
    rows = [jnp.concatenate([p[k : k + 1] for k in range(p.shape[0])], axis=1) for p in offsets]
    rows += memory_gain
    rows.append(jnp.concatenate(conv_gain[:2], axis=1))
    rows.append(jnp.concatenate([conv_gain[2], jnp.zeros_like(conv_gain[2])], axis=1))
    extra = jnp.concatenate(rows, axis=0).astype(BF16)
    tokens = tokens_ref[...]
    for j in range(out_ref.shape[0]):
        out_ref[j, :length] = tokens
        out_ref[j, length:] = extra


def piece_kernel(
    query_ref, key_ref, value_ref, left_ref, right_ref, memory_ref, conv_ref, out_ref, turn_ref
):
    nx, nc = out_ref.shape[0], out_ref.shape[1]
    rows = memory_ref.shape[0]
    width, chan = memory_ref.shape[1] // (nx * nc), conv_ref.shape[1] // (nx * nc)
    parts = []
    for at in range(nx * nc):
        parts.append(memory_ref[:, at * width : (at + 1) * width])
        parts.append(conv_ref[:, at * chan : (at + 1) * chan])
    whole = jnp.concatenate(parts, axis=1)
    wide = out_ref.shape[3]
    for j in range(whole.shape[1] // wide):
        turn_ref[j * rows : (j + 1) * rows] = whole[:, j * wide : (j + 1) * wide]
    for x in range(nx):
        for c in range(nc):
            at = c * nx + x
            parts = []
            for ref in (query_ref, key_ref, value_ref, left_ref, right_ref):
                width = ref.shape[1] // (nx * nc)
                parts.append(ref[:, at * width : (at + 1) * width])
            out_ref[x, c] = jnp.concatenate(parts, axis=1)


def arrange_kernel(before_ref, mine_ref, after_ref, opposite_ref, near_ref, low_ref, high_ref):
    for ref, at in ((near_ref, 0), (high_ref, 0)):
        ref[at] = before_ref[...]
    for ref, at in ((near_ref, 1), (high_ref, 1), (low_ref, 0)):
        ref[at] = mine_ref[...]
    for ref, at in ((near_ref, 2), (low_ref, 1)):
        ref[at] = after_ref[...]
    near_ref[3] = opposite_ref[...]


def assemble_kernel(place_ref, *refs):
    out_ref = refs[-1]
    nx, ny = out_ref.shape[2], out_ref.shape[0]
    core, column, x_at = place_ref[1], place_ref[2], place_ref[3]
    for ahead in range(nx):
        x = lax.rem(x_at + ahead, nx)
        for c, ref in ((core, refs[ahead]), (1 - core, refs[nx + ahead])):
            for b in range(ny):
                at = lax.rem(column + ny - b, ny)
                for near in range(ref.shape[1]):
                    out_ref[pl.ds(at, 1), near, pl.ds(x, 1), pl.ds(c, 1)] = ref[b, near][
                        None, None, None
                    ]


def project_kernel(
    place_ref, own_ref, other_ref,
    w0_ref, w1_ref, w3_ref, low_ref, high_ref, gate_ref,
    qk_ref, v_ref, glu_ref, gates_ref, gain_ref, out_weight_ref,
):
    nx, ny, _, part = own_ref.shape
    far, tall, wide = w0_ref.shape
    depth, chunks = out_weight_ref.shape[2], out_weight_ref.shape[3] // wide
    rows = tall - depth * chunks
    close = part // rows
    length = glu_ref.shape[1]
    place, core, column = place_ref[0], place_ref[1], place_ref[2]
    tokens_rows = nx * length
    width = qk_ref.shape[4] // 2
    chan = glu_ref.shape[2] // nx
    lane = lax.broadcasted_iota(jnp.int32, (length, width), 1)
    ones = jnp.where(lane == 0, 1.0, 0.0).astype(BF16)
    row = lax.broadcasted_iota(jnp.int32, (2 * nx, length), 0)
    gate_in = jnp.zeros((2 * nx, length), F32)
    forget = jnp.zeros((2 * nx, length), F32)

    members = far * close
    blocks = [
        (ref, i, ahead + close * (i - 1))
        for ref, ahead in ((w0_ref, 0), (w1_ref, 1), (w3_ref, -1))
        for i in range(far)
    ]
    blocks += [(low_ref, i, 2 + close * i) for i in range(far // 2)]
    blocks += [(high_ref, i, -2 + close * (i - 1)) for i in range(far // 2)]
    homes = []
    for ref, i, ahead in blocks:
        home = lax.rem(place + (ahead + members), members)
        y = lax.div(home, close)
        homes.append((y, lax.rem(home, close)))
        behind = lax.rem(y + ny - column, ny)
        out_weight_ref[pl.ds(behind, 1), pl.ds(homes[-1][1], 1)] = jnp.concatenate(
            [ref[i, rows + j * depth : rows + (j + 1) * depth] for j in range(chunks)], axis=1
        )[None, None]
    for half, ref in enumerate((own_ref, other_ref)):
        home = core if half == 0 else 1 - core
        acc = jnp.zeros((tokens_rows, wide), F32)
        pre = jnp.zeros((tokens_rows, gate_ref.shape[1]), F32)
        for pair in range(0, len(blocks), 2):
            left, right, gate_rows = [], [], []
            for at in (pair, pair + 1):
                w_ref, i, _ = blocks[at]
                y, z = homes[at]
                start = pl.multiple_of(z * rows, rows)
                left.append(
                    ref[:, pl.ds(y, 1), :length, pl.ds(start, rows)].reshape(tokens_rows, rows)
                )
                right.append(w_ref[i, :rows])
                gate_rows.append(gate_ref[pl.ds(y * part + start, rows)])
            lhs = jnp.concatenate(left, axis=1)
            acc = acc + dot(lhs, jnp.concatenate(right, axis=0), NN)
            pre = pre + dot(lhs, jnp.concatenate(gate_rows, axis=0), NN)
        glu = []
        for x in range(nx):
            mine = acc[x * length : (x + 1) * length]
            qk = mine[:, : 2 * width].astype(BF16)[None]
            for j in range(qk_ref.shape[0]):
                qk_ref[j, x, pl.ds(home, 1)] = qk
            v_ref[x, pl.ds(home, 1)] = jnp.concatenate(
                [mine[:, 2 * width : 3 * width].astype(BF16), ones], axis=1
            )[None]
            left = mine[:, 3 * width : 3 * width + chan]
            right = mine[:, 3 * width + chan :]
            glu.append(left / (1.0 + jnp.exp(-right)))
        glu_ref[pl.ds(home, 1)] = jnp.concatenate(glu, axis=1).astype(BF16)[None]
        for x in range(nx):
            turned = pre[x * length : (x + 1) * length].T
            extra = ref[x, column, length : length + 8].astype(F32)
            values = extra[0:1] + extra[1:2] + extra[2:3]
            offsets = jnp.where(core == 0, values[:, :length], values[:, length : 2 * length])
            offsets_f = jnp.where(
                core == 0, values[:, 2 * length : 3 * length], values[:, 3 * length : 4 * length]
            )
            at = row == 2 * x + home
            gate_pre = jnp.where(core == 0, turned[0:1], turned[1:2])
            forget_pre = jnp.where(core == 0, turned[2:3], turned[3:4])
            gate_in = jnp.where(at, gate_pre + offsets, gate_in)
            forget = jnp.where(at, forget_pre + offsets_f, forget)
    for b in range(ny):
        extra = own_ref[0, b, length : length + 8].astype(F32)
        memory_gain = extra[3:4] + extra[4:5] + extra[5:6]
        half = part // 2
        conv_gain = extra[6:7, :half] + extra[6:7, half:] + extra[7:8, :half]
        for at in range(2 * nx):
            gain_ref[b, at : at + 1] = jnp.concatenate(
                [
                    memory_gain[:, at * width : (at + 1) * width],
                    conv_gain[:, at * chan : (at + 1) * chan],
                    jnp.zeros((1, width - chan), F32),
                ],
                axis=1,
            )
    y = jnp.exp(-jnp.abs(forget))
    small = y * (1.0 - y * (1 / 2 - y * (1 / 3 - y * (1 / 4 - y * (1 / 5)))))
    gates_ref[0] = gate_in
    gates_ref[1] = jnp.minimum(forget, 0.0) - jnp.where(y < 0.03, small, jnp.log(1.0 + y))


def finish_kernel(arrived_ref, weight_ref, gain_ref, out_ref):
    nx, nc, ny, _, lanes = arrived_ref.shape
    width = lanes // 2
    chan = width // 2
    length, part = out_ref.shape
    lane = lax.broadcasted_iota(jnp.int32, (length, width + chan), 1)
    is_memory = lane < width
    half = length // 2

    def block(x, c, b):
        got = arrived_ref[x, c, b].astype(F32)
        memory = jnp.concatenate([got[:half, :width], got[:half, width:]], axis=0)
        conv = [got[half:, k * chan : (k + 1) * chan] for k in range(4)]
        return jnp.concatenate([memory, jnp.concatenate(conv, axis=0)], axis=1)

    blocks = {
        (x, c, b): block(x, c, b) for x in range(nx) for c in range(nc) for b in range(ny)
    }
    first = sum(blocks.values())
    second = sum(got * got for got in blocks.values())
    senders = nx * nc * ny
    memory_mean = jnp.sum(jnp.where(is_memory, second, 0.0), axis=1, keepdims=True)
    scale = lax.rsqrt(memory_mean / (senders * width) + EPS)
    mean = jnp.sum(jnp.where(is_memory, 0.0, first), axis=1, keepdims=True) / (senders * chan)
    power = jnp.sum(jnp.where(is_memory, 0.0, second), axis=1, keepdims=True) / (senders * chan)
    spread = lax.rsqrt(power - mean * mean + EPS)
    shift = jnp.where(is_memory, 0.0, mean)
    factor = jnp.where(is_memory, scale, spread)
    deep = weight_ref.shape[5]
    total = jnp.zeros((length, part), F32)
    for b in range(ny):
        left = []
        for c in range(nc):
            for x in range(nx):
                gain = gain_ref[b, c * nx + x : c * nx + x + 1, : width + chan]
                normed = (blocks[x, c, b] - shift) * factor * gain
                branch = normed / (1.0 + jnp.exp(-normed))
                left.append(jnp.where(is_memory, normed, branch).astype(BF16))
        total = total + dot(
            jnp.concatenate(left, axis=1), weight_ref[b].reshape(part, deep), NT
        )
    out_ref[...] = total.astype(BF16)


HOLD = 32


def tap_rows(taps_ref, core, x_at, nx, lanes):
    chan = lanes // nx
    weights = taps_ref[...].astype(F32)
    weights = jnp.where(core == 0, weights[:, :lanes], weights[:, lanes:])
    weights = pltpu.roll(weights, lax.rem(lanes - chan * x_at, lanes), 1)
    weights = jnp.where(lax.broadcasted_iota(jnp.int32, weights.shape, 1) < chan, weights, 0.0)
    return sum(pltpu.roll(weights, chan * k, 1) for k in range(1, nx)) + weights


def convolve(extended, weights):
    taps = weights.shape[0]
    length = extended.shape[0] - HOLD
    total = jnp.zeros((length, extended.shape[1]), F32)
    first = HOLD - (taps - 1)
    for shift in range(8):
        moved = extended[shift : shift + length + HOLD - 8] if shift else extended
        for j in range(taps):
            at = first + j
            if at % 8 == shift:
                total = total + moved[at - shift : at - shift + length] * weights[j : j + 1]
    return total


def with_logs(kept, width, level, total):
    row = lax.broadcasted_iota(jnp.int32, kept.shape, 0)
    lane = lax.broadcasted_iota(jnp.int32, kept.shape, 1)
    for at, value in ((0, level), (3, total)):
        for k, part in enumerate(three_parts(value)):
            kept = jnp.where((row == width + 1) & (lane == at + k), part, kept)
    return kept


def read_logs(block, width):
    line = block[width + 1 : width + 2, :128].astype(F32)
    level = line[:, 0:1] + line[:, 1:2] + line[:, 2:3]
    return level, line[:, 3:4] + line[:, 4:5] + line[:, 5:6]


def merged(blocks, passed, width):
    acc = jnp.zeros((1, 1), F32)
    logs = []
    for block, use in zip(blocks[::-1], passed[::-1]):
        level, total = read_logs(block, width)
        logs.insert(0, jnp.where(use, level + acc, LOW))
        acc = acc + jnp.where(use, total, 0.0)
    level = logs[0]
    for log in logs[1:]:
        level = jnp.maximum(level, log)
    state = jnp.zeros(blocks[0].shape, F32)
    for block, use, log in zip(blocks, passed, logs):
        state = state + jnp.where(use, jnp.exp(log - level), 0.0) * block.astype(F32)
    return state, level, acc


def group_kernel(in_ref, out_ref):
    members, rows, _ = in_ref.shape
    width = rows - 8
    blocks = [in_ref[j] for j in range(members)]
    state, level, total = merged(blocks, [True] * members, width)
    last = blocks[-1].astype(F32)
    kept = jnp.concatenate([state[: width + 2], last[width + 2 :]], axis=0)
    kept = with_logs(kept, width, level, total).astype(BF16)
    for j in range(out_ref.shape[0]):
        out_ref[j] = kept


def slab_kernel(
    qk_ref, v_ref, gate_ref, glu_ref, out_ref, q_ref, k_ref,
):
    chunks, length = gate_ref.shape[1], gate_ref.shape[2]
    width = qk_ref.shape[2] // 2
    gate, forget = gate_ref[0], gate_ref[1]
    within = lane_cumsum(forget)
    ends = [within[r : r + 1, length - 1 :] for r in range(chunks)]
    after = [jnp.zeros((1, 1), F32)]
    for r in range(chunks - 1, 0, -1):
        after.insert(0, after[0] + ends[r])
    total = after[0] + ends[0]
    to_end = jnp.concatenate([e + a for e, a in zip(ends, after)], axis=0)
    end_log = to_end - within + gate
    level = jnp.max(jnp.max(end_log, axis=1, keepdims=True), axis=0, keepdims=True)
    fresh = columns_of(jnp.exp(end_log - level))
    state = jnp.zeros((2 * width, width * qk_ref.shape[0]), F32)
    for r in range(chunks):
        q_ref[r * length : (r + 1) * length] = joined(qk_ref, 0, width, r, length)
        key = joined(qk_ref, width, width, r, length)
        k_ref[r * length : (r + 1) * length] = key
        scaled = (fresh[:, r : r + 1] * key.astype(F32)).astype(BF16)
        state = state + dot(v_ref[r * length : (r + 1) * length], scaled, TN)
    rows, head_lanes = out_ref.shape[1], out_ref.shape[2]
    kept = state[:rows]
    kept = with_logs(kept, width, level, total)
    chan = glu_ref.shape[2] // qk_ref.shape[0]
    hold = HOLD
    tail = glu_ref[glu_ref.shape[0] - 1, length - hold :].astype(F32)[:, glu_ref.shape[2] - chan :]
    group = head_lanes // chan
    each = hold // group
    tail = jnp.concatenate([tail[g * each : (g + 1) * each] for g in range(group)], axis=1)
    kept = jnp.concatenate([kept[: width + 2], tail, kept[width + 2 + each :]], axis=0)
    kept = kept.astype(BF16)
    for j in range(out_ref.shape[0]):
        out_ref[j] = kept


def local_kernel(place_ref, q_ref, k_ref, v_ref, gate_ref, glu_ref, taps_ref, out_ref, conv_ref):
    chunks, length = gate_ref.shape[1], gate_ref.shape[2]
    head = q_ref.shape[1]
    lanes = v_ref.shape[1]
    width = lanes // 2
    nx = chunks // glu_ref.shape[0]
    group = glu_ref.shape[0] * glu_ref.shape[1]
    glu = glu_ref[...].reshape(group, lanes).astype(F32)
    lane = lax.broadcasted_iota(jnp.int32, (HOLD, lanes), 1)
    before = pltpu.roll(glu[group - HOLD :], lanes // nx, 1)
    before = jnp.where(lane < lanes // nx, 0.0, before)
    weights = tap_rows(taps_ref, place_ref[1], place_ref[3], nx, lanes)
    conv_ref[...] = convolve(jnp.concatenate([before, glu], axis=0), weights)

    scale = head ** (-0.5)
    gate, forget = gate_ref[0], gate_ref[1]
    within = lane_cumsum(forget)
    turned = columns_of(jnp.concatenate([within, gate], axis=0))
    causal = lax.broadcasted_iota(jnp.int32, (length, length), 0) >= lax.broadcasted_iota(
        jnp.int32, (length, length), 1
    )
    lane = lax.broadcasted_iota(jnp.int32, (length, lanes), 1)
    state = jnp.zeros((lanes, head), F32)
    level = jnp.full((1, 1), LOW, F32)
    passed = jnp.zeros((1, 1), F32)
    for r in range(chunks):
        here = slice(r * length, (r + 1) * length)
        query, key, value = q_ref[here], k_ref[here], v_ref[here]
        within_row, gate_row = within[r : r + 1], gate[r : r + 1]
        within_col = turned[:, r : r + 1]
        gate_col = turned[:, chunks + r : chunks + r + 1]
        log_weight = jnp.where(causal, within_col - within_row + gate_row, -jnp.inf)
        carried = within_col + level
        top = jnp.maximum(carried, jnp.max(log_weight, axis=1, keepdims=True))
        weight = jnp.exp(log_weight - top)
        carried_weight = jnp.exp(carried - top) * scale
        scores = dot(query, key, NT) * (scale * weight)
        numer = dot(scores.astype(BF16), value, NN)
        denom = jnp.sum(scores, axis=1, keepdims=True)
        if r:
            older = dot(query, state.astype(BF16), NT)
            numer = numer + carried_weight * older
            denom = denom + carried_weight * older[:, width : width + 1]
        sent = jnp.where(lane == width, denom, numer)
        sent = jnp.where(lane == width + 1, top, sent)
        out_ref[here] = jnp.where(lane == width + 2, within_col + passed, sent)
        last = within_row[:, length - 1 :]
        passed = passed + last
        end_row = last - within_row + gate_row
        new_level = jnp.maximum(last + level, jnp.max(end_row, axis=1, keepdims=True))
        keep = jnp.exp(last + level - new_level)
        fresh = jnp.exp(last - within_col + gate_col - new_level)
        scaled = (fresh * key.astype(F32)).astype(BF16)
        state = keep * state + dot(value, scaled, TN)
        level = new_level


def cell_kernel(place_ref, far_ref, in_ref, q_ref, local_ref, conv_ref, taps_ref, out_ref):
    members, rows, head = in_ref.shape
    groups = far_ref.shape[0]
    nx, nc, ny, _, lanes = out_ref.shape
    width, chan = lanes // 2, lanes // nx
    length = q_ref.shape[0] // (nx * nc)
    scale = head ** (-0.5)
    place = place_ref[0]
    at_far, at_close = lax.div(place, members), lax.rem(place, members)
    blocks = [far_ref[j] for j in range(groups)] + [in_ref[j] for j in range(members)]
    passed = [j < at_far for j in range(groups)] + [j < at_close for j in range(members)]
    state, level, _ = merged(blocks, passed, width)
    state = jnp.concatenate([state, jnp.zeros((lanes - rows, head), F32)], axis=0).astype(BF16)

    group = head // chan
    each = HOLD // group
    near_rows = in_ref[jnp.maximum(at_close - 1, 0), width : width + 8].astype(F32)
    far_rows = far_ref[jnp.maximum(at_far - 1, 0), width : width + 8].astype(F32)
    last_rows = jnp.where(at_close > 0, near_rows, jnp.where(at_far > 0, far_rows, 0.0))
    last_rows = last_rows[2 : 2 + each]
    prior = jnp.concatenate([last_rows[:, g * chan : (g + 1) * chan] for g in range(group)], axis=0)
    prior = jnp.concatenate([prior, jnp.zeros((HOLD, lanes - chan), F32)], axis=1)
    weights = tap_rows(taps_ref, place_ref[1], place_ref[3], nx, lanes)
    edge = convolve(jnp.concatenate([prior, jnp.zeros((HOLD, lanes), F32)], axis=0), weights)
    half, quarter = length // 2, length // 4
    for r in range(nx * nc):
        here = slice(r * length, (r + 1) * length)
        local = local_ref[here]
        top_here, since = local[:, width + 1 : width + 2], local[:, width + 2 : width + 3]
        carried = since + level
        top = jnp.maximum(carried, top_here)
        local_weight = jnp.exp(top_here - top)
        carried_weight = jnp.exp(carried - top) * scale
        mixed = local_weight * local + carried_weight * dot(q_ref[here], state, NT)
        denom = mixed[:, width : width + 1]
        result = mixed[:, :width] / jnp.maximum(jnp.abs(denom), 1.0)
        x, c = r // nc, r % nc
        memory = jnp.concatenate([result[:half], result[half:]], axis=1)
        branch = []
        for g in range(4):
            at = c * length + g * quarter
            part = conv_ref[at : at + quarter]
            if at == 0:
                part = part + edge
            branch.append(part[:, x * chan : (x + 1) * chan])
        sent = jnp.concatenate([memory, jnp.concatenate(branch, axis=1)], axis=0).astype(BF16)
        for y in range(ny):
            out_ref[x, c, y] = sent


def vmem(count):
    return [pl.BlockSpec(memory_space=pltpu.VMEM)] * count


def layer(
    tokens,
    conv_value_weight,
    conv_gate_weight,
    conv_kernel,
    conv_norm_gain,
    query_weight,
    key_weight,
    value_weight,
    input_gate_weight,
    forget_gate_weight,
    input_offset,
    forget_offset,
    memory_norm_gain,
    conv_out_weight,
    memory_out_weight,
):
    nzh, nzl, nx, nc, ny = (size(a) for a in AXES)
    xi, ci, yi = lax.axis_index("x"), lax.axis_index("c"), lax.axis_index("tp")
    members = nzh * nzl
    zi = lax.axis_index("zh") * nzl + lax.axis_index("zl")
    length, part = tokens.shape
    slab = length * nx * nc
    head = query_weight.shape[1] // nc
    width = head // nx
    chan = conv_value_weight.shape[1] // nc // nx
    rows = query_weight.shape[0]
    wide = 3 * width + 2 * chan

    def from_z(value, ahead):
        return lax.ppermute(value, Z, [(j, (j - ahead) % members) for j in range(members)])

    deep = memory_out_weight.shape[0] + conv_out_weight.shape[0]
    pieces, out_rows = pl.pallas_call(
        piece_kernel,
        out_shape=(
            jax.ShapeDtypeStruct((nx, nc, rows, wide), BF16),
            jax.ShapeDtypeStruct((deep // wide * rows, wide), BF16),
        ),
        in_specs=vmem(7),
        out_specs=vmem(2),
        interpret=INTERPRET,
        name="pieces",
    )(
        query_weight,
        key_weight,
        value_weight,
        conv_value_weight,
        conv_gate_weight,
        memory_out_weight.T,
        conv_out_weight.T,
    )
    offsets = jnp.concatenate([input_offset.T, forget_offset.T], axis=0)
    call_pack = pl.pallas_call(
        pack_kernel,
        out_shape=jax.ShapeDtypeStruct((nx * ny, length + 8, part), BF16),
        in_specs=vmem(4),
        out_specs=pl.BlockSpec(memory_space=pltpu.VMEM),
        interpret=INTERPRET,
        name="pack",
    )
    sent = call_pack(tokens, offsets, conv_norm_gain[None], memory_norm_gain[None])
    mine = exchange(pieces.reshape(nx * nc, rows, wide), ("x", "c"))
    mine = jnp.concatenate([mine.reshape(nx * nc * rows, wide), out_rows], axis=0)
    step = members // 4
    opposite = from_z(mine, 2 * step)
    far = [from_z(mine, -step), mine, from_z(mine, step), opposite]
    own = exchange(sent, ("x", "tp")).reshape(nx, ny, length + 8, part)
    half_shape = (nzh // 2, *mine.shape)
    call_arrange = pl.pallas_call(
        arrange_kernel,
        out_shape=(
            jax.ShapeDtypeStruct((nzh, *mine.shape), BF16),
            jax.ShapeDtypeStruct(half_shape, BF16),
            jax.ShapeDtypeStruct(half_shape, BF16),
        ),
        in_specs=vmem(4),
        out_specs=vmem(3),
        interpret=INTERPRET,
        name="arrange",
    )
    near, *halves = call_arrange(*far)
    sets = [near, from_z(near, 1), from_z(near, -1)]
    sets += [from_z(halves[0], 2), from_z(halves[1], -2)]
    other = swapped(own, "c")

    gate_weight = jnp.pad(
        jnp.concatenate([input_gate_weight, forget_gate_weight], axis=1), ((0, 0), (0, 124))
    )
    place = jnp.stack([zi, ci, yi, xi])
    smem = pl.BlockSpec(memory_space=pltpu.SMEM)
    qk, value, packed, gates, gain, out_part = pl.pallas_call(
        project_kernel,
        out_shape=(
            jax.ShapeDtypeStruct((nx, nx, nc, length, 2 * width), BF16),
            jax.ShapeDtypeStruct((nx, nc, length, 2 * width), BF16),
            jax.ShapeDtypeStruct((nc, length, nx * chan), BF16),
            jax.ShapeDtypeStruct((2, nx * nc, length), F32),
            jax.ShapeDtypeStruct((ny, nc * nx, 2 * width), F32),
            jax.ShapeDtypeStruct((nzh, nzl, rows, deep), BF16),
        ),
        in_specs=[smem] + vmem(8),
        out_specs=vmem(6),
        interpret=INTERPRET,
        name="project",
    )(place, own, other, *sets, gate_weight)
    value = value.reshape(slab, 2 * width)
    all_qk = exchange(qk.reshape(nx, slab, 2 * width), "x")
    out_part = [out_part[0]] + [
        lax.ppermute(out_part[ahead], "tp", [(j, (j + ahead) % ny) for j in range(ny)])
        for ahead in range(1, ny)
    ]
    out_part = jnp.stack(out_part, axis=0)
    out_parts = [out_part] + [
        lax.ppermute(out_part, "x", [(j, (j - ahead) % nx) for j in range(nx)])
        for ahead in range(1, nx)
    ]
    other_parts = [swapped(out, "c") for out in out_parts]

    state_rows = width + 8
    call_slab = pl.pallas_call(
        slab_kernel,
        out_shape=(
            jax.ShapeDtypeStruct((nzl, state_rows, head), BF16),
            jax.ShapeDtypeStruct((slab, head), BF16),
            jax.ShapeDtypeStruct((slab, head), BF16),
        ),
        in_specs=vmem(4),
        out_specs=vmem(3),
        interpret=INTERPRET,
        name="slab_state",
    )
    states, query, key = call_slab(all_qk, value, gates, packed)
    states = exchange(states, "zl")
    call_group = pl.pallas_call(
        group_kernel,
        out_shape=jax.ShapeDtypeStruct((nzh, state_rows, head), BF16),
        in_specs=vmem(1),
        out_specs=pl.BlockSpec(memory_space=pltpu.VMEM),
        interpret=INTERPRET,
        name="group",
    )
    groups = call_group(states)
    groups = exchange(groups, "zh")
    call_local = pl.pallas_call(
        local_kernel,
        out_shape=(
            jax.ShapeDtypeStruct((slab, 2 * width), F32),
            jax.ShapeDtypeStruct((nc * length, nx * chan), F32),
        ),
        in_specs=[smem] + vmem(6),
        out_specs=vmem(2),
        interpret=INTERPRET,
        name="local",
    )
    local, conv = call_local(place, query, key, value, gates, packed, conv_kernel)
    call_cell = pl.pallas_call(
        cell_kernel,
        out_shape=jax.ShapeDtypeStruct((nx, nc, ny, length // 4 * 3, 2 * width), BF16),
        in_specs=[smem] + vmem(6),
        out_specs=pl.BlockSpec(memory_space=pltpu.VMEM),
        interpret=INTERPRET,
        name="cell",
    )
    last = call_cell(place, groups, states, query, local, conv, conv_kernel)
    arrived = exchange(last.reshape(nx * nc * ny, length // 4 * 3, -1), ("x", "c", "tp"))
    arrived = arrived.reshape(nx, nc, ny, length // 4 * 3, -1)
    call_assemble = pl.pallas_call(
        assemble_kernel,
        out_shape=jax.ShapeDtypeStruct((ny, nzl, nx, nc, rows, deep), BF16),
        in_specs=[smem] + vmem(2 * nx),
        out_specs=pl.BlockSpec(memory_space=pltpu.VMEM),
        interpret=INTERPRET,
        name="assemble",
    )
    out_weight = call_assemble(place, *out_parts, *other_parts)
    return pl.pallas_call(
        finish_kernel,
        out_shape=jax.ShapeDtypeStruct((length, part), BF16),
        in_specs=vmem(3),
        out_specs=pl.BlockSpec(memory_space=pltpu.VMEM),
        interpret=INTERPRET,
        name="finish",
    )(arrived, out_weight, gain)


def solution(mesh):
    shape = mesh.shape
    depth = shape["sp"] // 32
    split = Mesh(mesh.devices.reshape(4, depth, 4, 2, shape["tp"]), AXES)
    in_specs = (
        P(SP, "tp"),
        P(SP, "tp"),
        P(SP, "tp"),
        P(None, "tp"),
        P("tp"),
        P(SP, "tp"),
        P(SP, "tp"),
        P(SP, "tp"),
        P(None, "tp"),
        P(None, "tp"),
        P(SP, "tp"),
        P(SP, "tp"),
        P("tp"),
        P("tp", SP),
        P("tp", SP),
    )
    return jax.shard_map(
        layer, mesh=split, in_specs=in_specs, out_specs=P(SP, "tp"), check_vma=False
    )
```

```python
import jax
import jax.numpy as jnp
from jax import lax
from jax.experimental import pallas as pl
from jax.experimental.pallas import tpu as pltpu
from jax.sharding import Mesh
from jax.sharding import PartitionSpec as P

AXES = ("zh", "zl", "x", "c", "tp")
Z = ("zh", "zl")
SP = ("zh", "zl", "x", "c")
EPS = 1e-06
LOW = -1e30
F32 = jnp.float32
BF16 = jnp.bfloat16
INTERPRET = False


def size(axis):
    return lax.axis_size(axis)


def exchange(pieces, axes):
    return lax.all_to_all(pieces, axes, split_axis=0, concat_axis=0, tiled=True)


def swapped(value, axis):
    return lax.ppermute(value, axis, [(0, 1), (1, 0)])


def lane_cumsum(rows):
    lane = lax.broadcasted_iota(jnp.int32, rows.shape, 1)
    step = 1
    while step < rows.shape[1]:
        moved = pltpu.roll(rows, step, 1)
        rows = rows + jnp.where(lane >= step, moved, 0.0)
        step *= 2
    return rows


def columns_of(rows):
    count, length = rows.shape
    square = jnp.concatenate([rows, jnp.zeros((length - count, length), F32)], axis=0)
    return square.T


def dot(a, b, dims):
    return lax.dot_general(a, b, (dims, ((), ())), preferred_element_type=F32)


NN = ((1,), (0,))
NT = ((1,), (1,))
TN = ((0,), (0,))


def joined(parts_ref, start, width, chunk, length):
    picked = [
        parts_ref[j, chunk * length : (chunk + 1) * length, start : start + width]
        for j in range(parts_ref.shape[0])
    ]
    return jnp.concatenate(picked, axis=1)


def three_parts(value):
    high = value.astype(BF16).astype(F32)
    mid = (value - high).astype(BF16).astype(F32)
    return high, mid, value - high - mid


def pack_kernel(tokens_ref, offsets_ref, conv_gain_ref, memory_gain_ref, out_ref):
    length = tokens_ref.shape[0]
    offsets = three_parts(offsets_ref[...])
    conv_gain = three_parts(conv_gain_ref[...])
    memory_gain = three_parts(memory_gain_ref[...])
    rows = [jnp.concatenate([p[k : k + 1] for k in range(p.shape[0])], axis=1) for p in offsets]
    rows += memory_gain
    rows.append(jnp.concatenate(conv_gain[:2], axis=1))
    rows.append(jnp.concatenate([conv_gain[2], jnp.zeros_like(conv_gain[2])], axis=1))
    extra = jnp.concatenate(rows, axis=0).astype(BF16)
    tokens = tokens_ref[...]
    for j in range(out_ref.shape[0]):
        out_ref[j, :length] = tokens
        out_ref[j, length:] = extra


def piece_kernel(
    query_ref, key_ref, value_ref, left_ref, right_ref, memory_ref, conv_ref, out_ref, turn_ref
):
    nx, nc = out_ref.shape[0], out_ref.shape[1]
    rows = memory_ref.shape[0]
    whole = jnp.concatenate([memory_ref[...], conv_ref[...]], axis=1)
    wide = out_ref.shape[3]
    for j in range(whole.shape[1] // wide):
        turn_ref[j * rows : (j + 1) * rows] = whole[:, j * wide : (j + 1) * wide]
    for x in range(nx):
        for c in range(nc):
            at = c * nx + x
            parts = []
            for ref in (query_ref, key_ref, value_ref, left_ref, right_ref):
                width = ref.shape[1] // (nx * nc)
                parts.append(ref[:, at * width : (at + 1) * width])
            out_ref[x, c] = jnp.concatenate(parts, axis=1)


def arrange_kernel(before_ref, mine_ref, after_ref, opposite_ref, near_ref, low_ref, high_ref):
    for ref, at in ((near_ref, 0), (high_ref, 0)):
        ref[at] = before_ref[...]
    for ref, at in ((near_ref, 1), (high_ref, 1), (low_ref, 0)):
        ref[at] = mine_ref[...]
    for ref, at in ((near_ref, 2), (low_ref, 1)):
        ref[at] = after_ref[...]
    near_ref[3] = opposite_ref[...]


def assemble_kernel(place_ref, *refs):
    out_ref = refs[-1]
    nx, ny = out_ref.shape[2], out_ref.shape[0]
    core, column, x_at = place_ref[1], place_ref[2], place_ref[3]
    for ahead in range(nx):
        x = lax.rem(x_at + ahead, nx)
        for c, ref in ((core, refs[ahead]), (1 - core, refs[nx + ahead])):
            for b in range(ny):
                at = lax.rem(column + ny - b, ny)
                for near in range(ref.shape[1]):
                    out_ref[pl.ds(at, 1), near, pl.ds(x, 1), pl.ds(c, 1)] = ref[b, near][
                        None, None, None
                    ]


def project_kernel(
    place_ref, own_ref, other_ref,
    w0_ref, w1_ref, w3_ref, low_ref, high_ref, gate_ref,
    qk_ref, v_ref, glu_ref, gates_ref, memory_gain_ref, conv_gain_ref, out_weight_ref,
):
    nx, ny, _, part = own_ref.shape
    far, tall, wide = w0_ref.shape
    depth, chunks = out_weight_ref.shape[2], out_weight_ref.shape[3] // wide
    rows = tall - depth * chunks
    close = part // rows
    length = glu_ref.shape[1]
    place, core, column = place_ref[0], place_ref[1], place_ref[2]
    tokens_rows = nx * length
    width = qk_ref.shape[4] // 2
    chan = glu_ref.shape[2] // nx
    lane = lax.broadcasted_iota(jnp.int32, (length, width), 1)
    ones = jnp.where(lane == 0, 1.0, 0.0).astype(BF16)
    row = lax.broadcasted_iota(jnp.int32, (2 * nx, length), 0)
    gate_in = jnp.zeros((2 * nx, length), F32)
    forget = jnp.zeros((2 * nx, length), F32)

    members = far * close
    blocks = [
        (ref, i, ahead + close * (i - 1))
        for ref, ahead in ((w0_ref, 0), (w1_ref, 1), (w3_ref, -1))
        for i in range(far)
    ]
    blocks += [(low_ref, i, 2 + close * i) for i in range(far // 2)]
    blocks += [(high_ref, i, -2 + close * (i - 1)) for i in range(far // 2)]
    homes = []
    for ref, i, ahead in blocks:
        home = lax.rem(place + (ahead + members), members)
        y = lax.div(home, close)
        homes.append((y, lax.rem(home, close)))
        behind = lax.rem(y + ny - column, ny)
        out_weight_ref[pl.ds(behind, 1), pl.ds(homes[-1][1], 1)] = jnp.concatenate(
            [ref[i, rows + j * depth : rows + (j + 1) * depth] for j in range(chunks)], axis=1
        )[None, None]
    for half, ref in enumerate((own_ref, other_ref)):
        home = core if half == 0 else 1 - core
        acc = jnp.zeros((tokens_rows, wide), F32)
        pre = jnp.zeros((tokens_rows, gate_ref.shape[1]), F32)
        for pair in range(0, len(blocks), 2):
            left, right, gate_rows = [], [], []
            for at in (pair, pair + 1):
                w_ref, i, _ = blocks[at]
                y, z = homes[at]
                start = pl.multiple_of(z * rows, rows)
                left.append(
                    ref[:, pl.ds(y, 1), :length, pl.ds(start, rows)].reshape(tokens_rows, rows)
                )
                right.append(w_ref[i, :rows])
                gate_rows.append(gate_ref[pl.ds(y * part + start, rows)])
            lhs = jnp.concatenate(left, axis=1)
            acc = acc + dot(lhs, jnp.concatenate(right, axis=0), NN)
            pre = pre + dot(lhs, jnp.concatenate(gate_rows, axis=0), NN)
        glu = []
        for x in range(nx):
            mine = acc[x * length : (x + 1) * length]
            qk = mine[:, : 2 * width].astype(BF16)[None]
            for j in range(qk_ref.shape[0]):
                qk_ref[j, x, pl.ds(home, 1)] = qk
            v_ref[x, pl.ds(home, 1)] = jnp.concatenate(
                [mine[:, 2 * width : 3 * width].astype(BF16), ones], axis=1
            )[None]
            left = mine[:, 3 * width : 3 * width + chan]
            right = mine[:, 3 * width + chan :]
            glu.append(left / (1.0 + jnp.exp(-right)))
        glu_ref[pl.ds(home, 1)] = jnp.concatenate(glu, axis=1).astype(BF16)[None]
        for x in range(nx):
            turned = pre[x * length : (x + 1) * length].T
            extra = ref[x, column, length : length + 8].astype(F32)
            values = extra[0:1] + extra[1:2] + extra[2:3]
            offsets = jnp.where(core == 0, values[:, :length], values[:, length : 2 * length])
            offsets_f = jnp.where(
                core == 0, values[:, 2 * length : 3 * length], values[:, 3 * length : 4 * length]
            )
            at = row == 2 * x + home
            gate_pre = jnp.where(core == 0, turned[0:1], turned[1:2])
            forget_pre = jnp.where(core == 0, turned[2:3], turned[3:4])
            gate_in = jnp.where(at, gate_pre + offsets, gate_in)
            forget = jnp.where(at, forget_pre + offsets_f, forget)
    for b in range(ny):
        extra = own_ref[0, b, length : length + 8].astype(F32)
        memory_gain_ref[b : b + 1] = extra[3:4] + extra[4:5] + extra[5:6]
        half = part // 2
        conv_gain_ref[b : b + 1] = extra[6:7, :half] + extra[6:7, half:] + extra[7:8, :half]
    y = jnp.exp(-jnp.abs(forget))
    small = y * (1.0 - y * (1 / 2 - y * (1 / 3 - y * (1 / 4 - y * (1 / 5)))))
    gates_ref[0] = gate_in
    gates_ref[1] = jnp.minimum(forget, 0.0) - jnp.where(y < 0.03, small, jnp.log(1.0 + y))


def finish_kernel(arrived_ref, weight_ref, memory_gain_ref, conv_gain_ref, out_ref):
    nx, nc, ny, _, lanes = arrived_ref.shape
    width = lanes // 2
    chan = width // 2
    length, part = out_ref.shape
    half = length // 2
    memory, conv = [], []
    for b in range(ny):
        blocks = [arrived_ref[x, c, b].astype(F32) for c in range(nc) for x in range(nx)]
        upper = jnp.concatenate([got[:half, :width] for got in blocks], axis=1)
        lower = jnp.concatenate([got[:half, width:] for got in blocks], axis=1)
        memory.append(jnp.concatenate([upper, lower], axis=0))
        quarters = [
            jnp.concatenate([got[half:, k * chan : (k + 1) * chan] for got in blocks], axis=1)
            for k in range(4)
        ]
        conv.append(jnp.concatenate(quarters, axis=0))

    def mean_of(arrays):
        each = sum(arrays)
        return jnp.sum(each, axis=1, keepdims=True) / (ny * each.shape[1])

    scale = lax.rsqrt(mean_of([m * m for m in memory]) + EPS)
    mean = mean_of(conv)
    spread = lax.rsqrt(mean_of([t * t for t in conv]) - mean * mean + EPS)
    deep = weight_ref.shape[5]
    total = jnp.zeros((length, part), F32)
    for b in range(ny):
        scaled = memory[b] * scale * memory_gain_ref[b : b + 1]
        normed = (conv[b] - mean) * spread * conv_gain_ref[b : b + 1]
        branch = normed / (1.0 + jnp.exp(-normed))
        both = jnp.concatenate([scaled.astype(BF16), branch.astype(BF16)], axis=1)
        total = total + dot(both, weight_ref[b].reshape(part, deep), NT)
    out_ref[...] = total.astype(BF16)


HOLD = 32


def tap_rows(taps_ref, core, x_at, nx, lanes):
    chan = lanes // nx
    weights = taps_ref[...].astype(F32)
    weights = jnp.where(core == 0, weights[:, :lanes], weights[:, lanes:])
    weights = pltpu.roll(weights, lax.rem(lanes - chan * x_at, lanes), 1)
    weights = jnp.where(lax.broadcasted_iota(jnp.int32, weights.shape, 1) < chan, weights, 0.0)
    return sum(pltpu.roll(weights, chan * k, 1) for k in range(1, nx)) + weights


def convolve(extended, weights):
    taps = weights.shape[0]
    length = extended.shape[0] - HOLD
    total = jnp.zeros((length, extended.shape[1]), F32)
    first = HOLD - (taps - 1)
    for shift in range(8):
        moved = extended[shift : shift + length + HOLD - 8] if shift else extended
        for j in range(taps):
            at = first + j
            if at % 8 == shift:
                total = total + moved[at - shift : at - shift + length] * weights[j : j + 1]
    return total


def with_logs(kept, width, level, total):
    row = lax.broadcasted_iota(jnp.int32, kept.shape, 0)
    lane = lax.broadcasted_iota(jnp.int32, kept.shape, 1)
    for at, value in ((0, level), (3, total)):
        for k, part in enumerate(three_parts(value)):
            kept = jnp.where((row == width + 1) & (lane == at + k), part, kept)
    return kept


def read_logs(block, width):
    line = block[width + 1 : width + 2, :128].astype(F32)
    level = line[:, 0:1] + line[:, 1:2] + line[:, 2:3]
    return level, line[:, 3:4] + line[:, 4:5] + line[:, 5:6]


def merged(blocks, passed, width):
    acc = jnp.zeros((1, 1), F32)
    logs = []
    for block, use in zip(blocks[::-1], passed[::-1]):
        level, total = read_logs(block, width)
        logs.insert(0, jnp.where(use, level + acc, LOW))
        acc = acc + jnp.where(use, total, 0.0)
    level = logs[0]
    for log in logs[1:]:
        level = jnp.maximum(level, log)
    state = jnp.zeros(blocks[0].shape, F32)
    for block, use, log in zip(blocks, passed, logs):
        state = state + jnp.where(use, jnp.exp(log - level), 0.0) * block.astype(F32)
    return state, level, acc


def group_kernel(in_ref, out_ref):
    members, rows, _ = in_ref.shape
    width = rows - 8
    blocks = [in_ref[j] for j in range(members)]
    state, level, total = merged(blocks, [True] * members, width)
    last = blocks[-1].astype(F32)
    kept = jnp.concatenate([state[: width + 2], last[width + 2 :]], axis=0)
    kept = with_logs(kept, width, level, total).astype(BF16)
    for j in range(out_ref.shape[0]):
        out_ref[j] = kept


def slab_kernel(
    qk_ref, v_ref, gate_ref, glu_ref, out_ref, q_ref, k_ref,
):
    chunks, length = gate_ref.shape[1], gate_ref.shape[2]
    width = qk_ref.shape[2] // 2
    gate, forget = gate_ref[0], gate_ref[1]
    within = lane_cumsum(forget)
    ends = [within[r : r + 1, length - 1 :] for r in range(chunks)]
    after = [jnp.zeros((1, 1), F32)]
    for r in range(chunks - 1, 0, -1):
        after.insert(0, after[0] + ends[r])
    total = after[0] + ends[0]
    to_end = jnp.concatenate([e + a for e, a in zip(ends, after)], axis=0)
    end_log = to_end - within + gate
    level = jnp.max(jnp.max(end_log, axis=1, keepdims=True), axis=0, keepdims=True)
    fresh = columns_of(jnp.exp(end_log - level))
    state = jnp.zeros((2 * width, width * qk_ref.shape[0]), F32)
    for r in range(chunks):
        q_ref[r * length : (r + 1) * length] = joined(qk_ref, 0, width, r, length)
        key = joined(qk_ref, width, width, r, length)
        k_ref[r * length : (r + 1) * length] = key
        scaled = (fresh[:, r : r + 1] * key.astype(F32)).astype(BF16)
        state = state + dot(v_ref[r * length : (r + 1) * length], scaled, TN)
    rows, head_lanes = out_ref.shape[1], out_ref.shape[2]
    kept = state[:rows]
    kept = with_logs(kept, width, level, total)
    chan = glu_ref.shape[2] // qk_ref.shape[0]
    hold = HOLD
    tail = glu_ref[glu_ref.shape[0] - 1, length - hold :].astype(F32)[:, glu_ref.shape[2] - chan :]
    group = head_lanes // chan
    each = hold // group
    tail = jnp.concatenate([tail[g * each : (g + 1) * each] for g in range(group)], axis=1)
    kept = jnp.concatenate([kept[: width + 2], tail, kept[width + 2 + each :]], axis=0)
    kept = kept.astype(BF16)
    for j in range(out_ref.shape[0]):
        out_ref[j] = kept


def local_kernel(place_ref, q_ref, k_ref, v_ref, gate_ref, glu_ref, taps_ref, out_ref, conv_ref):
    chunks, length = gate_ref.shape[1], gate_ref.shape[2]
    head = q_ref.shape[1]
    lanes = v_ref.shape[1]
    width = lanes // 2
    nx = chunks // glu_ref.shape[0]
    group = glu_ref.shape[0] * glu_ref.shape[1]
    glu = glu_ref[...].reshape(group, lanes).astype(F32)
    lane = lax.broadcasted_iota(jnp.int32, (HOLD, lanes), 1)
    before = pltpu.roll(glu[group - HOLD :], lanes // nx, 1)
    before = jnp.where(lane < lanes // nx, 0.0, before)
    weights = tap_rows(taps_ref, place_ref[1], place_ref[3], nx, lanes)
    conv_ref[...] = convolve(jnp.concatenate([before, glu], axis=0), weights)

    scale = head ** (-0.5)
    gate, forget = gate_ref[0], gate_ref[1]
    within = lane_cumsum(forget)
    turned = columns_of(jnp.concatenate([within, gate], axis=0))
    causal = lax.broadcasted_iota(jnp.int32, (length, length), 0) >= lax.broadcasted_iota(
        jnp.int32, (length, length), 1
    )
    lane = lax.broadcasted_iota(jnp.int32, (length, lanes), 1)
    state = jnp.zeros((lanes, head), F32)
    level = jnp.full((1, 1), LOW, F32)
    passed = jnp.zeros((1, 1), F32)
    for r in range(chunks):
        here = slice(r * length, (r + 1) * length)
        query, key, value = q_ref[here], k_ref[here], v_ref[here]
        within_row, gate_row = within[r : r + 1], gate[r : r + 1]
        within_col = turned[:, r : r + 1]
        gate_col = turned[:, chunks + r : chunks + r + 1]
        log_weight = jnp.where(causal, within_col - within_row + gate_row, -jnp.inf)
        carried = within_col + level
        top = jnp.maximum(carried, jnp.max(log_weight, axis=1, keepdims=True))
        weight = jnp.exp(log_weight - top)
        carried_weight = jnp.exp(carried - top) * scale
        scores = dot(query, key, NT) * (scale * weight)
        numer = dot(scores.astype(BF16), value, NN)
        denom = jnp.sum(scores, axis=1, keepdims=True)
        if r:
            older = dot(query, state.astype(BF16), NT)
            numer = numer + carried_weight * older
            denom = denom + carried_weight * older[:, width : width + 1]
        sent = jnp.where(lane == width, denom, numer)
        sent = jnp.where(lane == width + 1, top, sent)
        out_ref[here] = jnp.where(lane == width + 2, within_col + passed, sent)
        last = within_row[:, length - 1 :]
        passed = passed + last
        end_row = last - within_row + gate_row
        new_level = jnp.maximum(last + level, jnp.max(end_row, axis=1, keepdims=True))
        keep = jnp.exp(last + level - new_level)
        fresh = jnp.exp(last - within_col + gate_col - new_level)
        scaled = (fresh * key.astype(F32)).astype(BF16)
        state = keep * state + dot(value, scaled, TN)
        level = new_level


def cell_kernel(place_ref, far_ref, in_ref, q_ref, local_ref, conv_ref, taps_ref, out_ref):
    members, rows, head = in_ref.shape
    groups = far_ref.shape[0]
    nx, nc, ny, _, lanes = out_ref.shape
    width, chan = lanes // 2, lanes // nx
    length = q_ref.shape[0] // (nx * nc)
    scale = head ** (-0.5)
    place = place_ref[0]
    at_far, at_close = lax.div(place, members), lax.rem(place, members)
    blocks = [far_ref[j] for j in range(groups)] + [in_ref[j] for j in range(members)]
    passed = [j < at_far for j in range(groups)] + [j < at_close for j in range(members)]
    state, level, _ = merged(blocks, passed, width)
    state = jnp.concatenate([state, jnp.zeros((lanes - rows, head), F32)], axis=0).astype(BF16)

    group = head // chan
    each = HOLD // group
    near_rows = in_ref[jnp.maximum(at_close - 1, 0), width : width + 8].astype(F32)
    far_rows = far_ref[jnp.maximum(at_far - 1, 0), width : width + 8].astype(F32)
    last_rows = jnp.where(at_close > 0, near_rows, jnp.where(at_far > 0, far_rows, 0.0))
    last_rows = last_rows[2 : 2 + each]
    prior = jnp.concatenate([last_rows[:, g * chan : (g + 1) * chan] for g in range(group)], axis=0)
    prior = jnp.concatenate([prior, jnp.zeros((HOLD, lanes - chan), F32)], axis=1)
    weights = tap_rows(taps_ref, place_ref[1], place_ref[3], nx, lanes)
    edge = convolve(jnp.concatenate([prior, jnp.zeros((HOLD, lanes), F32)], axis=0), weights)
    half, quarter = length // 2, length // 4
    for r in range(nx * nc):
        here = slice(r * length, (r + 1) * length)
        local = local_ref[here]
        top_here, since = local[:, width + 1 : width + 2], local[:, width + 2 : width + 3]
        carried = since + level
        top = jnp.maximum(carried, top_here)
        local_weight = jnp.exp(top_here - top)
        carried_weight = jnp.exp(carried - top) * scale
        mixed = local_weight * local + carried_weight * dot(q_ref[here], state, NT)
        denom = mixed[:, width : width + 1]
        result = mixed[:, :width] / jnp.maximum(jnp.abs(denom), 1.0)
        x, c = r // nc, r % nc
        memory = jnp.concatenate([result[:half], result[half:]], axis=1)
        branch = []
        for g in range(4):
            at = c * length + g * quarter
            part = conv_ref[at : at + quarter]
            if at == 0:
                part = part + edge
            branch.append(part[:, x * chan : (x + 1) * chan])
        sent = jnp.concatenate([memory, jnp.concatenate(branch, axis=1)], axis=0).astype(BF16)
        for y in range(ny):
            out_ref[x, c, y] = sent


def vmem(count):
    return [pl.BlockSpec(memory_space=pltpu.VMEM)] * count


def layer(
    tokens,
    conv_value_weight,
    conv_gate_weight,
    conv_kernel,
    conv_norm_gain,
    query_weight,
    key_weight,
    value_weight,
    input_gate_weight,
    forget_gate_weight,
    input_offset,
    forget_offset,
    memory_norm_gain,
    conv_out_weight,
    memory_out_weight,
):
    nzh, nzl, nx, nc, ny = (size(a) for a in AXES)
    xi, ci, yi = lax.axis_index("x"), lax.axis_index("c"), lax.axis_index("tp")
    members = nzh * nzl
    zi = lax.axis_index("zh") * nzl + lax.axis_index("zl")
    length, part = tokens.shape
    slab = length * nx * nc
    head = query_weight.shape[1] // nc
    width = head // nx
    chan = conv_value_weight.shape[1] // nc // nx
    rows = query_weight.shape[0]
    wide = 3 * width + 2 * chan

    def from_z(value, ahead):
        return lax.ppermute(value, Z, [(j, (j - ahead) % members) for j in range(members)])

    deep = memory_out_weight.shape[0] + conv_out_weight.shape[0]
    pieces, out_rows = pl.pallas_call(
        piece_kernel,
        out_shape=(
            jax.ShapeDtypeStruct((nx, nc, rows, wide), BF16),
            jax.ShapeDtypeStruct((deep // wide * rows, wide), BF16),
        ),
        in_specs=vmem(7),
        out_specs=vmem(2),
        interpret=INTERPRET,
        name="pieces",
    )(
        query_weight,
        key_weight,
        value_weight,
        conv_value_weight,
        conv_gate_weight,
        memory_out_weight.T,
        conv_out_weight.T,
    )
    offsets = jnp.concatenate([input_offset.T, forget_offset.T], axis=0)
    call_pack = pl.pallas_call(
        pack_kernel,
        out_shape=jax.ShapeDtypeStruct((nx * ny, length + 8, part), BF16),
        in_specs=vmem(4),
        out_specs=pl.BlockSpec(memory_space=pltpu.VMEM),
        interpret=INTERPRET,
        name="pack",
    )
    sent = call_pack(tokens, offsets, conv_norm_gain[None], memory_norm_gain[None])
    mine = exchange(pieces.reshape(nx * nc, rows, wide), ("x", "c"))
    mine = jnp.concatenate([mine.reshape(nx * nc * rows, wide), out_rows], axis=0)
    step = members // 4
    opposite = from_z(mine, 2 * step)
    far = [from_z(mine, -step), mine, from_z(mine, step), opposite]
    own = exchange(sent, ("x", "tp")).reshape(nx, ny, length + 8, part)
    half_shape = (nzh // 2, *mine.shape)
    call_arrange = pl.pallas_call(
        arrange_kernel,
        out_shape=(
            jax.ShapeDtypeStruct((nzh, *mine.shape), BF16),
            jax.ShapeDtypeStruct(half_shape, BF16),
            jax.ShapeDtypeStruct(half_shape, BF16),
        ),
        in_specs=vmem(4),
        out_specs=vmem(3),
        interpret=INTERPRET,
        name="arrange",
    )
    near, *halves = call_arrange(*far)
    sets = [near, from_z(near, 1), from_z(near, -1)]
    sets += [from_z(halves[0], 2), from_z(halves[1], -2)]
    other = swapped(own, "c")

    gate_weight = jnp.pad(
        jnp.concatenate([input_gate_weight, forget_gate_weight], axis=1), ((0, 0), (0, 124))
    )
    place = jnp.stack([zi, ci, yi, xi])
    smem = pl.BlockSpec(memory_space=pltpu.SMEM)
    qk, value, packed, gates, memory_gain, conv_gain, out_part = pl.pallas_call(
        project_kernel,
        out_shape=(
            jax.ShapeDtypeStruct((nx, nx, nc, length, 2 * width), BF16),
            jax.ShapeDtypeStruct((nx, nc, length, 2 * width), BF16),
            jax.ShapeDtypeStruct((nc, length, nx * chan), BF16),
            jax.ShapeDtypeStruct((2, nx * nc, length), F32),
            jax.ShapeDtypeStruct((ny, memory_norm_gain.shape[0]), F32),
            jax.ShapeDtypeStruct((ny, conv_norm_gain.shape[0]), F32),
            jax.ShapeDtypeStruct((nzh, nzl, rows, deep), BF16),
        ),
        in_specs=[smem] + vmem(8),
        out_specs=vmem(7),
        interpret=INTERPRET,
        name="project",
    )(place, own, other, *sets, gate_weight)
    value = value.reshape(slab, 2 * width)
    all_qk = exchange(qk.reshape(nx, slab, 2 * width), "x")
    out_part = [out_part[0]] + [
        lax.ppermute(out_part[ahead], "tp", [(j, (j + ahead) % ny) for j in range(ny)])
        for ahead in range(1, ny)
    ]
    out_part = jnp.stack(out_part, axis=0)

    def from_x(value, ahead):
        return lax.ppermute(value, "x", [(j, (j - ahead) % nx) for j in range(nx)])

    out_parts = [out_part] + [from_x(out_part, ahead) for ahead in (1, 3)]
    out_parts.insert(2, from_x(out_part, 2))
    other_parts = [swapped(out, "c") for out in out_parts]

    state_rows = width + 8
    call_slab = pl.pallas_call(
        slab_kernel,
        out_shape=(
            jax.ShapeDtypeStruct((nzl, state_rows, head), BF16),
            jax.ShapeDtypeStruct((slab, head), BF16),
            jax.ShapeDtypeStruct((slab, head), BF16),
        ),
        in_specs=vmem(4),
        out_specs=vmem(3),
        interpret=INTERPRET,
        name="slab_state",
    )
    states, query, key = call_slab(all_qk, value, gates, packed)
    states = exchange(states, "zl")
    call_group = pl.pallas_call(
        group_kernel,
        out_shape=jax.ShapeDtypeStruct((nzh, state_rows, head), BF16),
        in_specs=vmem(1),
        out_specs=pl.BlockSpec(memory_space=pltpu.VMEM),
        interpret=INTERPRET,
        name="group",
    )
    groups = call_group(states)
    groups = exchange(groups, "zh")
    call_local = pl.pallas_call(
        local_kernel,
        out_shape=(
            jax.ShapeDtypeStruct((slab, 2 * width), F32),
            jax.ShapeDtypeStruct((nc * length, nx * chan), F32),
        ),
        in_specs=[smem] + vmem(6),
        out_specs=vmem(2),
        interpret=INTERPRET,
        name="local",
    )
    local, conv = call_local(place, query, key, value, gates, packed, conv_kernel)
    call_cell = pl.pallas_call(
        cell_kernel,
        out_shape=jax.ShapeDtypeStruct((nx, nc, ny, length // 4 * 3, 2 * width), BF16),
        in_specs=[smem] + vmem(6),
        out_specs=pl.BlockSpec(memory_space=pltpu.VMEM),
        interpret=INTERPRET,
        name="cell",
    )
    last = call_cell(place, groups, states, query, local, conv, conv_kernel)
    arrived = exchange(last.reshape(nx * nc * ny, length // 4 * 3, -1), ("x", "c", "tp"))
    arrived = arrived.reshape(nx, nc, ny, length // 4 * 3, -1)
    call_assemble = pl.pallas_call(
        assemble_kernel,
        out_shape=jax.ShapeDtypeStruct((ny, nzl, nx, nc, rows, deep), BF16),
        in_specs=[smem] + vmem(2 * nx),
        out_specs=pl.BlockSpec(memory_space=pltpu.VMEM),
        interpret=INTERPRET,
        name="assemble",
    )
    out_weight = call_assemble(place, *out_parts, *other_parts)
    return pl.pallas_call(
        finish_kernel,
        out_shape=jax.ShapeDtypeStruct((length, part), BF16),
        in_specs=vmem(4),
        out_specs=pl.BlockSpec(memory_space=pltpu.VMEM),
        interpret=INTERPRET,
        name="finish",
    )(arrived, out_weight, memory_gain, conv_gain)


def solution(mesh):
    shape = mesh.shape
    depth = shape["sp"] // 32
    split = Mesh(mesh.devices.reshape(4, depth, 4, 2, shape["tp"]), AXES)
    in_specs = (
        P(SP, "tp"),
        P(SP, "tp"),
        P(SP, "tp"),
        P(None, "tp"),
        P("tp"),
        P(SP, "tp"),
        P(SP, "tp"),
        P(SP, "tp"),
        P(None, "tp"),
        P(None, "tp"),
        P(SP, "tp"),
        P(SP, "tp"),
        P("tp"),
        P("tp", SP),
        P("tp", SP),
    )
    return jax.shard_map(
        layer, mesh=split, in_specs=in_specs, out_specs=P(SP, "tp"), check_vma=False
    )
```

```python
import jax
import jax.numpy as jnp
from jax import lax
from jax.experimental import pallas as pl
from jax.experimental.pallas import tpu as pltpu
from jax.sharding import Mesh
from jax.sharding import PartitionSpec as P

AXES = ("zh", "zl", "x", "c", "tp")
Z = ("zh", "zl")
SP = ("zh", "zl", "x", "c")
EPS = 1e-06
LOW = -1e30
F32 = jnp.float32
BF16 = jnp.bfloat16
INTERPRET = False


def size(axis):
    return lax.axis_size(axis)


def exchange(pieces, axes):
    return lax.all_to_all(pieces, axes, split_axis=0, concat_axis=0, tiled=True)


def swapped(value, axis):
    return lax.ppermute(value, axis, [(0, 1), (1, 0)])


def lane_cumsum(rows):
    lane = lax.broadcasted_iota(jnp.int32, rows.shape, 1)
    step = 1
    while step < rows.shape[1]:
        moved = pltpu.roll(rows, step, 1)
        rows = rows + jnp.where(lane >= step, moved, 0.0)
        step *= 2
    return rows


def columns_of(rows):
    count, length = rows.shape
    square = jnp.concatenate([rows, jnp.zeros((length - count, length), F32)], axis=0)
    return square.T


def dot(a, b, dims):
    return lax.dot_general(a, b, (dims, ((), ())), preferred_element_type=F32)


NN = ((1,), (0,))
NT = ((1,), (1,))
TN = ((0,), (0,))


def joined(parts_ref, start, width, chunk, length):
    picked = [
        parts_ref[j, chunk * length : (chunk + 1) * length, start : start + width]
        for j in range(parts_ref.shape[0])
    ]
    return jnp.concatenate(picked, axis=1)


def three_parts(value):
    high = value.astype(BF16).astype(F32)
    mid = (value - high).astype(BF16).astype(F32)
    return high, mid, value - high - mid


def pack_kernel(tokens_ref, offsets_ref, conv_gain_ref, memory_gain_ref, out_ref):
    length = tokens_ref.shape[0]
    offsets = three_parts(offsets_ref[...])
    conv_gain = three_parts(conv_gain_ref[...])
    memory_gain = three_parts(memory_gain_ref[...])
    rows = [jnp.concatenate([p[k : k + 1] for k in range(p.shape[0])], axis=1) for p in offsets]
    rows += memory_gain
    rows.append(jnp.concatenate(conv_gain[:2], axis=1))
    rows.append(jnp.concatenate([conv_gain[2], jnp.zeros_like(conv_gain[2])], axis=1))
    extra = jnp.concatenate(rows, axis=0).astype(BF16)
    tokens = tokens_ref[...]
    for j in range(out_ref.shape[0]):
        out_ref[j, :length] = tokens
        out_ref[j, length:] = extra


def piece_kernel(
    query_ref, key_ref, value_ref, left_ref, right_ref, memory_ref, conv_ref, out_ref, turn_ref
):
    nx, nc = out_ref.shape[0], out_ref.shape[1]
    rows = memory_ref.shape[0]
    whole = jnp.concatenate([memory_ref[...], conv_ref[...]], axis=1)
    wide = out_ref.shape[3]
    for j in range(whole.shape[1] // wide):
        turn_ref[j * rows : (j + 1) * rows] = whole[:, j * wide : (j + 1) * wide]
    for x in range(nx):
        for c in range(nc):
            at = c * nx + x
            parts = []
            for ref in (query_ref, key_ref, value_ref, left_ref, right_ref):
                width = ref.shape[1] // (nx * nc)
                parts.append(ref[:, at * width : (at + 1) * width])
            out_ref[x, c] = jnp.concatenate(parts, axis=1)


def arrange_kernel(before_ref, mine_ref, after_ref, opposite_ref, near_ref, low_ref, high_ref):
    for ref, at in ((near_ref, 0), (high_ref, 0)):
        ref[at] = before_ref[...]
    for ref, at in ((near_ref, 1), (high_ref, 1), (low_ref, 0)):
        ref[at] = mine_ref[...]
    for ref, at in ((near_ref, 2), (low_ref, 1)):
        ref[at] = after_ref[...]
    near_ref[3] = opposite_ref[...]


def assemble_kernel(place_ref, *refs):
    out_ref = refs[-1]
    nx, ny = out_ref.shape[2], out_ref.shape[0]
    core, column, x_at = place_ref[1], place_ref[2], place_ref[3]
    for ahead in range(nx):
        x = lax.rem(x_at + ahead, nx)
        for c, ref in ((core, refs[ahead]), (1 - core, refs[nx + ahead])):
            for b in range(ny):
                at = lax.rem(column + ny - b, ny)
                for near in range(ref.shape[1]):
                    out_ref[pl.ds(at, 1), near, pl.ds(x, 1), pl.ds(c, 1)] = ref[b, near][
                        None, None, None
                    ]


def project_kernel(
    place_ref, own_ref, other_ref,
    w0_ref, w1_ref, w3_ref, low_ref, high_ref, gate_ref,
    qk_ref, v_ref, glu_ref, gates_ref, memory_gain_ref, conv_gain_ref, out_weight_ref,
):
    nx, ny, _, part = own_ref.shape
    far, tall, wide = w0_ref.shape
    depth, chunks = out_weight_ref.shape[2], out_weight_ref.shape[3] // wide
    rows = tall - depth * chunks
    close = part // rows
    length = glu_ref.shape[1]
    place, core, column = place_ref[0], place_ref[1], place_ref[2]
    tokens_rows = nx * length
    width = qk_ref.shape[4] // 2
    chan = glu_ref.shape[2] // nx
    lane = lax.broadcasted_iota(jnp.int32, (length, width), 1)
    ones = jnp.where(lane == 0, 1.0, 0.0).astype(BF16)
    row = lax.broadcasted_iota(jnp.int32, (2 * nx, length), 0)
    gate_in = jnp.zeros((2 * nx, length), F32)
    forget = jnp.zeros((2 * nx, length), F32)

    members = far * close
    blocks = [
        (ref, i, ahead + close * (i - 1))
        for ref, ahead in ((w0_ref, 0), (w1_ref, 1), (w3_ref, -1))
        for i in range(far)
    ]
    blocks += [(low_ref, i, 2 + close * i) for i in range(far // 2)]
    blocks += [(high_ref, i, -2 + close * (i - 1)) for i in range(far // 2)]
    homes = []
    for ref, i, ahead in blocks:
        home = lax.rem(place + (ahead + members), members)
        y = lax.div(home, close)
        homes.append((y, lax.rem(home, close)))
        behind = lax.rem(y + ny - column, ny)
        out_weight_ref[pl.ds(behind, 1), pl.ds(homes[-1][1], 1)] = jnp.concatenate(
            [ref[i, rows + j * depth : rows + (j + 1) * depth] for j in range(chunks)], axis=1
        )[None, None]
    right = []
    for (w_ref, i, _), (y, z) in zip(blocks, homes):
        start = pl.multiple_of(y * part + z * rows, rows)
        right.append(jnp.concatenate([w_ref[i, :rows], gate_ref[pl.ds(start, rows)]], axis=1))
    right = jnp.concatenate(right, axis=0)
    for half, ref in enumerate((own_ref, other_ref)):
        home = core if half == 0 else 1 - core
        left = []
        for y, z in homes:
            lanes = pl.ds(pl.multiple_of(z * rows, rows), rows)
            left.append(ref[:, pl.ds(y, 1), :length, lanes].reshape(tokens_rows, rows))
        acc = dot(jnp.concatenate(left, axis=1), right, NN)
        pre = acc[:, wide:]
        glu = []
        for x in range(nx):
            mine = acc[x * length : (x + 1) * length]
            qk = mine[:, : 2 * width].astype(BF16)[None]
            for j in range(qk_ref.shape[0]):
                qk_ref[j, x, pl.ds(home, 1)] = qk
            v_ref[x, pl.ds(home, 1)] = jnp.concatenate(
                [mine[:, 2 * width : 3 * width].astype(BF16), ones], axis=1
            )[None]
            left = mine[:, 3 * width : 3 * width + chan]
            gates_side = mine[:, 3 * width + chan : wide]
            glu.append(left / (1.0 + jnp.exp(-gates_side)))
        glu_ref[pl.ds(home, 1)] = jnp.concatenate(glu, axis=1).astype(BF16)[None]
        for x in range(nx):
            turned = pre[x * length : (x + 1) * length].T
            extra = ref[x, column, length : length + 8].astype(F32)
            values = extra[0:1] + extra[1:2] + extra[2:3]
            offsets = jnp.where(core == 0, values[:, :length], values[:, length : 2 * length])
            offsets_f = jnp.where(
                core == 0, values[:, 2 * length : 3 * length], values[:, 3 * length : 4 * length]
            )
            at = row == 2 * x + home
            gate_pre = jnp.where(core == 0, turned[0:1], turned[1:2])
            forget_pre = jnp.where(core == 0, turned[2:3], turned[3:4])
            gate_in = jnp.where(at, gate_pre + offsets, gate_in)
            forget = jnp.where(at, forget_pre + offsets_f, forget)
    for b in range(ny):
        extra = own_ref[0, b, length : length + 8].astype(F32)
        memory_gain_ref[b : b + 1] = extra[3:4] + extra[4:5] + extra[5:6]
        half = part // 2
        conv_gain_ref[b : b + 1] = extra[6:7, :half] + extra[6:7, half:] + extra[7:8, :half]
    y = jnp.exp(-jnp.abs(forget))
    small = y * (1.0 - y * (1 / 2 - y * (1 / 3 - y * (1 / 4 - y * (1 / 5)))))
    gates_ref[0] = gate_in
    gates_ref[1] = jnp.minimum(forget, 0.0) - jnp.where(y < 0.03, small, jnp.log(1.0 + y))


def finish_kernel(arrived_ref, weight_ref, memory_gain_ref, conv_gain_ref, out_ref):
    nx, nc, ny, _, lanes = arrived_ref.shape
    width = lanes // 2
    chan = width // 2
    length, part = out_ref.shape
    half = length // 2
    memory, conv = [], []
    for b in range(ny):
        blocks = [arrived_ref[x, c, b].astype(F32) for c in range(nc) for x in range(nx)]
        upper = jnp.concatenate([got[:half, :width] for got in blocks], axis=1)
        lower = jnp.concatenate([got[:half, width:] for got in blocks], axis=1)
        memory.append(jnp.concatenate([upper, lower], axis=0))
        quarters = [
            jnp.concatenate([got[half:, k * chan : (k + 1) * chan] for got in blocks], axis=1)
            for k in range(4)
        ]
        conv.append(jnp.concatenate(quarters, axis=0))

    def mean_of(arrays):
        each = sum(arrays)
        return jnp.sum(each, axis=1, keepdims=True) / (ny * each.shape[1])

    scale = lax.rsqrt(mean_of([m * m for m in memory]) + EPS)
    mean = mean_of(conv)
    spread = lax.rsqrt(mean_of([t * t for t in conv]) - mean * mean + EPS)
    deep = weight_ref.shape[5]
    total = jnp.zeros((length, part), F32)
    for b in range(ny):
        scaled = memory[b] * scale * memory_gain_ref[b : b + 1]
        normed = (conv[b] - mean) * spread * conv_gain_ref[b : b + 1]
        branch = normed / (1.0 + jnp.exp(-normed))
        both = jnp.concatenate([scaled.astype(BF16), branch.astype(BF16)], axis=1)
        total = total + dot(both, weight_ref[b].reshape(part, deep), NT)
    out_ref[...] = total.astype(BF16)


HOLD = 32


def tap_rows(taps_ref, core, x_at, nx, lanes):
    chan = lanes // nx
    weights = taps_ref[...].astype(F32)
    weights = jnp.where(core == 0, weights[:, :lanes], weights[:, lanes:])
    weights = pltpu.roll(weights, lax.rem(lanes - chan * x_at, lanes), 1)
    weights = jnp.where(lax.broadcasted_iota(jnp.int32, weights.shape, 1) < chan, weights, 0.0)
    return sum(pltpu.roll(weights, chan * k, 1) for k in range(1, nx)) + weights


def convolve(extended, weights):
    taps = weights.shape[0]
    length = extended.shape[0] - HOLD
    total = jnp.zeros((length, extended.shape[1]), F32)
    first = HOLD - (taps - 1)
    for shift in range(8):
        moved = extended[shift : shift + length + HOLD - 8] if shift else extended
        for j in range(taps):
            at = first + j
            if at % 8 == shift:
                total = total + moved[at - shift : at - shift + length] * weights[j : j + 1]
    return total


def with_logs(kept, width, level, total):
    row = lax.broadcasted_iota(jnp.int32, kept.shape, 0)
    lane = lax.broadcasted_iota(jnp.int32, kept.shape, 1)
    for at, value in ((0, level), (3, total)):
        for k, part in enumerate(three_parts(value)):
            kept = jnp.where((row == width + 1) & (lane == at + k), part, kept)
    return kept


def read_logs(block, width):
    line = block[width + 1 : width + 2, :128].astype(F32)
    level = line[:, 0:1] + line[:, 1:2] + line[:, 2:3]
    return level, line[:, 3:4] + line[:, 4:5] + line[:, 5:6]


def merged(blocks, passed, width):
    acc = jnp.zeros((1, 1), F32)
    logs = []
    for block, use in zip(blocks[::-1], passed[::-1]):
        level, total = read_logs(block, width)
        logs.insert(0, jnp.where(use, level + acc, LOW))
        acc = acc + jnp.where(use, total, 0.0)
    level = logs[0]
    for log in logs[1:]:
        level = jnp.maximum(level, log)
    state = jnp.zeros(blocks[0].shape, F32)
    for block, use, log in zip(blocks, passed, logs):
        state = state + jnp.where(use, jnp.exp(log - level), 0.0) * block.astype(F32)
    return state, level, acc


def group_kernel(in_ref, out_ref):
    members, rows, _ = in_ref.shape
    width = rows - 8
    blocks = [in_ref[j] for j in range(members)]
    state, level, total = merged(blocks, [True] * members, width)
    last = blocks[-1].astype(F32)
    kept = jnp.concatenate([state[: width + 2], last[width + 2 :]], axis=0)
    kept = with_logs(kept, width, level, total).astype(BF16)
    for j in range(out_ref.shape[0]):
        out_ref[j] = kept


def slab_kernel(
    qk_ref, v_ref, gate_ref, glu_ref, out_ref, q_ref, k_ref,
):
    chunks, length = gate_ref.shape[1], gate_ref.shape[2]
    width = qk_ref.shape[2] // 2
    gate, forget = gate_ref[0], gate_ref[1]
    within = lane_cumsum(forget)
    ends = [within[r : r + 1, length - 1 :] for r in range(chunks)]
    after = [jnp.zeros((1, 1), F32)]
    for r in range(chunks - 1, 0, -1):
        after.insert(0, after[0] + ends[r])
    total = after[0] + ends[0]
    to_end = jnp.concatenate([e + a for e, a in zip(ends, after)], axis=0)
    end_log = to_end - within + gate
    level = jnp.max(jnp.max(end_log, axis=1, keepdims=True), axis=0, keepdims=True)
    fresh = columns_of(jnp.exp(end_log - level))
    state = jnp.zeros((2 * width, width * qk_ref.shape[0]), F32)
    for r in range(chunks):
        q_ref[r * length : (r + 1) * length] = joined(qk_ref, 0, width, r, length)
        key = joined(qk_ref, width, width, r, length)
        k_ref[r * length : (r + 1) * length] = key
        scaled = (fresh[:, r : r + 1] * key.astype(F32)).astype(BF16)
        state = state + dot(v_ref[r * length : (r + 1) * length], scaled, TN)
    rows, head_lanes = out_ref.shape[1], out_ref.shape[2]
    kept = state[:rows]
    kept = with_logs(kept, width, level, total)
    chan = glu_ref.shape[2] // qk_ref.shape[0]
    hold = HOLD
    tail = glu_ref[glu_ref.shape[0] - 1, length - hold :].astype(F32)[:, glu_ref.shape[2] - chan :]
    group = head_lanes // chan
    each = hold // group
    tail = jnp.concatenate([tail[g * each : (g + 1) * each] for g in range(group)], axis=1)
    kept = jnp.concatenate([kept[: width + 2], tail, kept[width + 2 + each :]], axis=0)
    kept = kept.astype(BF16)
    for j in range(out_ref.shape[0]):
        out_ref[j] = kept


def local_kernel(place_ref, q_ref, k_ref, v_ref, gate_ref, glu_ref, taps_ref, out_ref, conv_ref):
    chunks, length = gate_ref.shape[1], gate_ref.shape[2]
    head = q_ref.shape[1]
    lanes = v_ref.shape[1]
    width = lanes // 2
    nx = chunks // glu_ref.shape[0]
    group = glu_ref.shape[0] * glu_ref.shape[1]
    glu = glu_ref[...].reshape(group, lanes).astype(F32)
    lane = lax.broadcasted_iota(jnp.int32, (HOLD, lanes), 1)
    before = pltpu.roll(glu[group - HOLD :], lanes // nx, 1)
    before = jnp.where(lane < lanes // nx, 0.0, before)
    weights = tap_rows(taps_ref, place_ref[1], place_ref[3], nx, lanes)
    conv_ref[...] = convolve(jnp.concatenate([before, glu], axis=0), weights)

    scale = head ** (-0.5)
    gate, forget = gate_ref[0], gate_ref[1]
    within = lane_cumsum(forget)
    turned = columns_of(jnp.concatenate([within, gate], axis=0))
    causal = lax.broadcasted_iota(jnp.int32, (length, length), 0) >= lax.broadcasted_iota(
        jnp.int32, (length, length), 1
    )
    lane = lax.broadcasted_iota(jnp.int32, (length, lanes), 1)
    state = jnp.zeros((lanes, head), F32)
    level = jnp.full((1, 1), LOW, F32)
    passed = jnp.zeros((1, 1), F32)
    for r in range(chunks):
        here = slice(r * length, (r + 1) * length)
        query, key, value = q_ref[here], k_ref[here], v_ref[here]
        within_row, gate_row = within[r : r + 1], gate[r : r + 1]
        within_col = turned[:, r : r + 1]
        gate_col = turned[:, chunks + r : chunks + r + 1]
        log_weight = jnp.where(causal, within_col - within_row + gate_row, -jnp.inf)
        carried = within_col + level
        top = jnp.maximum(carried, jnp.max(log_weight, axis=1, keepdims=True))
        weight = jnp.exp(log_weight - top)
        carried_weight = jnp.exp(carried - top) * scale
        scores = dot(query, key, NT) * (scale * weight)
        numer = dot(scores.astype(BF16), value, NN)
        denom = jnp.sum(scores, axis=1, keepdims=True)
        if r:
            older = dot(query, state.astype(BF16), NT)
            numer = numer + carried_weight * older
            denom = denom + carried_weight * older[:, width : width + 1]
        sent = jnp.where(lane == width, denom, numer)
        sent = jnp.where(lane == width + 1, top, sent)
        out_ref[here] = jnp.where(lane == width + 2, within_col + passed, sent)
        last = within_row[:, length - 1 :]
        passed = passed + last
        end_row = last - within_row + gate_row
        new_level = jnp.maximum(last + level, jnp.max(end_row, axis=1, keepdims=True))
        keep = jnp.exp(last + level - new_level)
        fresh = jnp.exp(last - within_col + gate_col - new_level)
        scaled = (fresh * key.astype(F32)).astype(BF16)
        state = keep * state + dot(value, scaled, TN)
        level = new_level


def cell_kernel(place_ref, far_ref, in_ref, q_ref, local_ref, conv_ref, taps_ref, out_ref):
    members, rows, head = in_ref.shape
    groups = far_ref.shape[0]
    nx, nc, ny, _, lanes = out_ref.shape
    width, chan = lanes // 2, lanes // nx
    length = q_ref.shape[0] // (nx * nc)
    scale = head ** (-0.5)
    place = place_ref[0]
    at_far, at_close = lax.div(place, members), lax.rem(place, members)
    blocks = [far_ref[j] for j in range(groups)] + [in_ref[j] for j in range(members)]
    passed = [j < at_far for j in range(groups)] + [j < at_close for j in range(members)]
    state, level, _ = merged(blocks, passed, width)
    state = jnp.concatenate([state, jnp.zeros((lanes - rows, head), F32)], axis=0).astype(BF16)

    group = head // chan
    each = HOLD // group
    near_rows = in_ref[jnp.maximum(at_close - 1, 0), width : width + 8].astype(F32)
    far_rows = far_ref[jnp.maximum(at_far - 1, 0), width : width + 8].astype(F32)
    last_rows = jnp.where(at_close > 0, near_rows, jnp.where(at_far > 0, far_rows, 0.0))
    last_rows = last_rows[2 : 2 + each]
    prior = jnp.concatenate([last_rows[:, g * chan : (g + 1) * chan] for g in range(group)], axis=0)
    prior = jnp.concatenate([prior, jnp.zeros((HOLD, lanes - chan), F32)], axis=1)
    weights = tap_rows(taps_ref, place_ref[1], place_ref[3], nx, lanes)
    edge = convolve(jnp.concatenate([prior, jnp.zeros((HOLD, lanes), F32)], axis=0), weights)
    half, quarter = length // 2, length // 4
    for r in range(nx * nc):
        here = slice(r * length, (r + 1) * length)
        local = local_ref[here]
        top_here, since = local[:, width + 1 : width + 2], local[:, width + 2 : width + 3]
        carried = since + level
        top = jnp.maximum(carried, top_here)
        local_weight = jnp.exp(top_here - top)
        carried_weight = jnp.exp(carried - top) * scale
        mixed = local_weight * local + carried_weight * dot(q_ref[here], state, NT)
        denom = mixed[:, width : width + 1]
        result = mixed[:, :width] / jnp.maximum(jnp.abs(denom), 1.0)
        x, c = r // nc, r % nc
        memory = jnp.concatenate([result[:half], result[half:]], axis=1)
        branch = []
        for g in range(4):
            at = c * length + g * quarter
            part = conv_ref[at : at + quarter]
            if at == 0:
                part = part + edge
            branch.append(part[:, x * chan : (x + 1) * chan])
        sent = jnp.concatenate([memory, jnp.concatenate(branch, axis=1)], axis=0).astype(BF16)
        for y in range(ny):
            out_ref[x, c, y] = sent


def vmem(count):
    return [pl.BlockSpec(memory_space=pltpu.VMEM)] * count


def layer(
    tokens,
    conv_value_weight,
    conv_gate_weight,
    conv_kernel,
    conv_norm_gain,
    query_weight,
    key_weight,
    value_weight,
    input_gate_weight,
    forget_gate_weight,
    input_offset,
    forget_offset,
    memory_norm_gain,
    conv_out_weight,
    memory_out_weight,
):
    nzh, nzl, nx, nc, ny = (size(a) for a in AXES)
    xi, ci, yi = lax.axis_index("x"), lax.axis_index("c"), lax.axis_index("tp")
    members = nzh * nzl
    zi = lax.axis_index("zh") * nzl + lax.axis_index("zl")
    length, part = tokens.shape
    slab = length * nx * nc
    head = query_weight.shape[1] // nc
    width = head // nx
    chan = conv_value_weight.shape[1] // nc // nx
    rows = query_weight.shape[0]
    wide = 3 * width + 2 * chan

    def from_z(value, ahead):
        return lax.ppermute(value, Z, [(j, (j - ahead) % members) for j in range(members)])

    deep = memory_out_weight.shape[0] + conv_out_weight.shape[0]
    pieces, out_rows = pl.pallas_call(
        piece_kernel,
        out_shape=(
            jax.ShapeDtypeStruct((nx, nc, rows, wide), BF16),
            jax.ShapeDtypeStruct((deep // wide * rows, wide), BF16),
        ),
        in_specs=vmem(7),
        out_specs=vmem(2),
        interpret=INTERPRET,
        name="pieces",
    )(
        query_weight,
        key_weight,
        value_weight,
        conv_value_weight,
        conv_gate_weight,
        memory_out_weight.T,
        conv_out_weight.T,
    )
    offsets = jnp.concatenate([input_offset.T, forget_offset.T], axis=0)
    call_pack = pl.pallas_call(
        pack_kernel,
        out_shape=jax.ShapeDtypeStruct((nx * ny, length + 8, part), BF16),
        in_specs=vmem(4),
        out_specs=pl.BlockSpec(memory_space=pltpu.VMEM),
        interpret=INTERPRET,
        name="pack",
    )
    sent = call_pack(tokens, offsets, conv_norm_gain[None], memory_norm_gain[None])
    mine = exchange(pieces.reshape(nx * nc, rows, wide), ("x", "c"))
    mine = jnp.concatenate([mine.reshape(nx * nc * rows, wide), out_rows], axis=0)
    step = members // 4
    opposite = from_z(mine, 2 * step)
    far = [from_z(mine, -step), mine, from_z(mine, step), opposite]
    own = exchange(sent, ("x", "tp")).reshape(nx, ny, length + 8, part)
    half_shape = (nzh // 2, *mine.shape)
    call_arrange = pl.pallas_call(
        arrange_kernel,
        out_shape=(
            jax.ShapeDtypeStruct((nzh, *mine.shape), BF16),
            jax.ShapeDtypeStruct(half_shape, BF16),
            jax.ShapeDtypeStruct(half_shape, BF16),
        ),
        in_specs=vmem(4),
        out_specs=vmem(3),
        interpret=INTERPRET,
        name="arrange",
    )
    near, *halves = call_arrange(*far)
    sets = [near, from_z(near, 1), from_z(near, -1)]
    sets += [from_z(halves[0], 2), from_z(halves[1], -2)]
    other = swapped(own, "c")

    gate_weight = jnp.pad(
        jnp.concatenate([input_gate_weight, forget_gate_weight], axis=1), ((0, 0), (0, 124))
    )
    place = jnp.stack([zi, ci, yi, xi])
    smem = pl.BlockSpec(memory_space=pltpu.SMEM)
    qk, value, packed, gates, memory_gain, conv_gain, out_part = pl.pallas_call(
        project_kernel,
        out_shape=(
            jax.ShapeDtypeStruct((nx, nx, nc, length, 2 * width), BF16),
            jax.ShapeDtypeStruct((nx, nc, length, 2 * width), BF16),
            jax.ShapeDtypeStruct((nc, length, nx * chan), BF16),
            jax.ShapeDtypeStruct((2, nx * nc, length), F32),
            jax.ShapeDtypeStruct((ny, memory_norm_gain.shape[0]), F32),
            jax.ShapeDtypeStruct((ny, conv_norm_gain.shape[0]), F32),
            jax.ShapeDtypeStruct((nzh, nzl, rows, deep), BF16),
        ),
        in_specs=[smem] + vmem(8),
        out_specs=vmem(7),
        interpret=INTERPRET,
        name="project",
    )(place, own, other, *sets, gate_weight)
    value = value.reshape(slab, 2 * width)
    all_qk = exchange(qk.reshape(nx, slab, 2 * width), "x")
    out_part = [out_part[0]] + [
        lax.ppermute(out_part[ahead], "tp", [(j, (j + ahead) % ny) for j in range(ny)])
        for ahead in range(1, ny)
    ]
    out_part = jnp.stack(out_part, axis=0)

    def from_x(value, ahead):
        return lax.ppermute(value, "x", [(j, (j - ahead) % nx) for j in range(nx)])

    out_parts = [out_part, from_x(out_part, 1)]
    from_last = from_x(out_part, 3)
    out_parts += [from_x(out_part, 2), from_last]
    other_parts = [swapped(out, "c") for out in out_parts[:2]]
    other_parts += [swapped(out, "c") for out in out_parts[2:]]

    state_rows = width + 8
    call_slab = pl.pallas_call(
        slab_kernel,
        out_shape=(
            jax.ShapeDtypeStruct((nzl, state_rows, head), BF16),
            jax.ShapeDtypeStruct((slab, head), BF16),
            jax.ShapeDtypeStruct((slab, head), BF16),
        ),
        in_specs=vmem(4),
        out_specs=vmem(3),
        interpret=INTERPRET,
        name="slab_state",
    )
    states, query, key = call_slab(all_qk, value, gates, packed)
    states = exchange(states, "zl")
    call_group = pl.pallas_call(
        group_kernel,
        out_shape=jax.ShapeDtypeStruct((nzh, state_rows, head), BF16),
        in_specs=vmem(1),
        out_specs=pl.BlockSpec(memory_space=pltpu.VMEM),
        interpret=INTERPRET,
        name="group",
    )
    groups = call_group(states)
    groups = exchange(groups, "zh")
    call_local = pl.pallas_call(
        local_kernel,
        out_shape=(
            jax.ShapeDtypeStruct((slab, 2 * width), F32),
            jax.ShapeDtypeStruct((nc * length, nx * chan), F32),
        ),
        in_specs=[smem] + vmem(6),
        out_specs=vmem(2),
        interpret=INTERPRET,
        name="local",
    )
    local, conv = call_local(place, query, key, value, gates, packed, conv_kernel)
    call_cell = pl.pallas_call(
        cell_kernel,
        out_shape=jax.ShapeDtypeStruct((nx, nc, ny, length // 4 * 3, 2 * width), BF16),
        in_specs=[smem] + vmem(6),
        out_specs=pl.BlockSpec(memory_space=pltpu.VMEM),
        interpret=INTERPRET,
        name="cell",
    )
    last = call_cell(place, groups, states, query, local, conv, conv_kernel)
    arrived = exchange(last.reshape(nx * nc * ny, length // 4 * 3, -1), ("x", "c", "tp"))
    arrived = arrived.reshape(nx, nc, ny, length // 4 * 3, -1)
    call_assemble = pl.pallas_call(
        assemble_kernel,
        out_shape=jax.ShapeDtypeStruct((ny, nzl, nx, nc, rows, deep), BF16),
        in_specs=[smem] + vmem(2 * nx),
        out_specs=pl.BlockSpec(memory_space=pltpu.VMEM),
        interpret=INTERPRET,
        name="assemble",
    )
    out_weight = call_assemble(place, *out_parts, *other_parts)
    return pl.pallas_call(
        finish_kernel,
        out_shape=jax.ShapeDtypeStruct((length, part), BF16),
        in_specs=vmem(4),
        out_specs=pl.BlockSpec(memory_space=pltpu.VMEM),
        interpret=INTERPRET,
        name="finish",
    )(arrived, out_weight, memory_gain, conv_gain)


def solution(mesh):
    shape = mesh.shape
    depth = shape["sp"] // 32
    split = Mesh(mesh.devices.reshape(4, depth, 4, 2, shape["tp"]), AXES)
    in_specs = (
        P(SP, "tp"),
        P(SP, "tp"),
        P(SP, "tp"),
        P(None, "tp"),
        P("tp"),
        P(SP, "tp"),
        P(SP, "tp"),
        P(SP, "tp"),
        P(None, "tp"),
        P(None, "tp"),
        P(SP, "tp"),
        P(SP, "tp"),
        P("tp"),
        P("tp", SP),
        P("tp", SP),
    )
    return jax.shard_map(
        layer, mesh=split, in_specs=in_specs, out_specs=P(SP, "tp"), check_vma=False
    )
```

```python
import jax
import jax.numpy as jnp
from jax import lax
from jax.experimental import pallas as pl
from jax.experimental.pallas import tpu as pltpu
from jax.sharding import Mesh
from jax.sharding import PartitionSpec as P

AXES = ("zh", "zl", "x", "c", "tp")
Z = ("zh", "zl")
SP = ("zh", "zl", "x", "c")
EPS = 1e-06
LOW = -1e30
F32 = jnp.float32
BF16 = jnp.bfloat16
INTERPRET = False


def size(axis):
    return lax.axis_size(axis)


def exchange(pieces, axes):
    return lax.all_to_all(pieces, axes, split_axis=0, concat_axis=0, tiled=True)


def swapped(value, axis):
    return lax.ppermute(value, axis, [(0, 1), (1, 0)])


def lane_cumsum(rows):
    lane = lax.broadcasted_iota(jnp.int32, rows.shape, 1)
    step = 1
    while step < rows.shape[1]:
        moved = pltpu.roll(rows, step, 1)
        rows = rows + jnp.where(lane >= step, moved, 0.0)
        step *= 2
    return rows


def columns_of(rows):
    count, length = rows.shape
    square = jnp.concatenate([rows, jnp.zeros((length - count, length), F32)], axis=0)
    return square.T


def dot(a, b, dims):
    return lax.dot_general(a, b, (dims, ((), ())), preferred_element_type=F32)


NN = ((1,), (0,))
NT = ((1,), (1,))
TN = ((0,), (0,))


def joined(parts_ref, start, width, chunk, length):
    picked = [
        parts_ref[j, chunk * length : (chunk + 1) * length, start : start + width]
        for j in range(parts_ref.shape[0])
    ]
    return jnp.concatenate(picked, axis=1)


def three_parts(value):
    high = value.astype(BF16).astype(F32)
    mid = (value - high).astype(BF16).astype(F32)
    return high, mid, value - high - mid


def pack_kernel(tokens_ref, offsets_ref, conv_gain_ref, memory_gain_ref, out_ref):
    length = tokens_ref.shape[0]
    offsets = three_parts(offsets_ref[...])
    conv_gain = three_parts(conv_gain_ref[...])
    memory_gain = three_parts(memory_gain_ref[...])
    rows = [jnp.concatenate([p[k : k + 1] for k in range(p.shape[0])], axis=1) for p in offsets]
    rows += memory_gain
    rows.append(jnp.concatenate(conv_gain[:2], axis=1))
    rows.append(jnp.concatenate([conv_gain[2], jnp.zeros_like(conv_gain[2])], axis=1))
    extra = jnp.concatenate(rows, axis=0).astype(BF16)
    tokens = tokens_ref[...]
    for j in range(out_ref.shape[0]):
        out_ref[j, :length] = tokens
        out_ref[j, length:] = extra


def piece_kernel(
    query_ref, key_ref, value_ref, left_ref, right_ref, memory_ref, conv_ref, out_ref, turn_ref
):
    nx, nc = out_ref.shape[0], out_ref.shape[1]
    rows = memory_ref.shape[0]
    whole = jnp.concatenate([memory_ref[...], conv_ref[...]], axis=1)
    wide = out_ref.shape[3]
    for j in range(whole.shape[1] // wide):
        turn_ref[j * rows : (j + 1) * rows] = whole[:, j * wide : (j + 1) * wide]
    for x in range(nx):
        for c in range(nc):
            at = c * nx + x
            parts = []
            for ref in (query_ref, key_ref, value_ref, left_ref, right_ref):
                width = ref.shape[1] // (nx * nc)
                parts.append(ref[:, at * width : (at + 1) * width])
            out_ref[x, c] = jnp.concatenate(parts, axis=1)


def arrange_kernel(before_ref, mine_ref, after_ref, opposite_ref, near_ref, low_ref, high_ref):
    for ref, at in ((near_ref, 0), (high_ref, 0)):
        ref[at] = before_ref[...]
    for ref, at in ((near_ref, 1), (high_ref, 1), (low_ref, 0)):
        ref[at] = mine_ref[...]
    for ref, at in ((near_ref, 2), (low_ref, 1)):
        ref[at] = after_ref[...]
    near_ref[3] = opposite_ref[...]


def assemble_kernel(place_ref, *refs):
    out_ref = refs[-1]
    nx, ny = out_ref.shape[2], out_ref.shape[0]
    core, column, x_at = place_ref[1], place_ref[2], place_ref[3]
    for ahead in range(nx):
        x = lax.rem(x_at + ahead, nx)
        for c, ref in ((core, refs[ahead]), (1 - core, refs[nx + ahead])):
            for b in range(ny):
                at = lax.rem(column + ny - b, ny)
                for near in range(ref.shape[1]):
                    out_ref[pl.ds(at, 1), near, pl.ds(x, 1), pl.ds(c, 1)] = ref[b, near][
                        None, None, None
                    ]


def project_kernel(
    place_ref, own_ref, other_ref,
    w0_ref, w1_ref, w3_ref, low_ref, high_ref, gate_ref,
    qk_ref, v_ref, glu_ref, gates_ref, memory_gain_ref, conv_gain_ref, out_weight_ref,
):
    nx, ny, _, part = own_ref.shape
    far, tall, wide = w0_ref.shape
    depth, chunks = out_weight_ref.shape[2], out_weight_ref.shape[3] // wide
    rows = tall - depth * chunks
    close = part // rows
    length = glu_ref.shape[1]
    place, core, column = place_ref[0], place_ref[1], place_ref[2]
    tokens_rows = nx * length
    width = qk_ref.shape[4] // 2
    chan = glu_ref.shape[2] // nx
    lane = lax.broadcasted_iota(jnp.int32, (length, width), 1)
    ones = jnp.where(lane == 0, 1.0, 0.0).astype(BF16)
    row = lax.broadcasted_iota(jnp.int32, (2 * nx, length), 0)
    gate_in = jnp.zeros((2 * nx, length), F32)
    forget = jnp.zeros((2 * nx, length), F32)

    members = far * close
    blocks = [
        (ref, i, ahead + close * (i - 1))
        for ref, ahead in ((w0_ref, 0), (w1_ref, 1), (w3_ref, -1))
        for i in range(far)
    ]
    blocks += [(low_ref, i, 2 + close * i) for i in range(far // 2)]
    blocks += [(high_ref, i, -2 + close * (i - 1)) for i in range(far // 2)]
    homes = []
    for ref, i, ahead in blocks:
        home = lax.rem(place + (ahead + members), members)
        y = lax.div(home, close)
        homes.append((y, lax.rem(home, close)))
        behind = lax.rem(y + ny - column, ny)
        out_weight_ref[pl.ds(behind, 1), pl.ds(homes[-1][1], 1)] = jnp.concatenate(
            [ref[i, rows + j * depth : rows + (j + 1) * depth] for j in range(chunks)], axis=1
        )[None, None]
    right = []
    for (w_ref, i, _), (y, z) in zip(blocks, homes):
        start = pl.multiple_of(y * part + z * rows, rows)
        right.append(jnp.concatenate([w_ref[i, :rows], gate_ref[pl.ds(start, rows)]], axis=1))
    right = jnp.concatenate(right, axis=0)
    for half, ref in enumerate((own_ref, other_ref)):
        home = core if half == 0 else 1 - core
        left = []
        for y, z in homes:
            lanes = pl.ds(pl.multiple_of(z * rows, rows), rows)
            left.append(ref[:, pl.ds(y, 1), :length, lanes].reshape(tokens_rows, rows))
        acc = dot(jnp.concatenate(left, axis=1), right, NN)
        pre = acc[:, wide:]
        glu = []
        for x in range(nx):
            mine = acc[x * length : (x + 1) * length]
            qk = mine[:, : 2 * width].astype(BF16)[None]
            for j in range(qk_ref.shape[0]):
                qk_ref[j, x, pl.ds(home, 1)] = qk
            v_ref[x, pl.ds(home, 1)] = jnp.concatenate(
                [mine[:, 2 * width : 3 * width].astype(BF16), ones], axis=1
            )[None]
            left = mine[:, 3 * width : 3 * width + chan]
            gates_side = mine[:, 3 * width + chan : wide]
            glu.append(left / (1.0 + jnp.exp(-gates_side)))
        glu_ref[pl.ds(home, 1)] = jnp.concatenate(glu, axis=1).astype(BF16)[None]
        for x in range(nx):
            turned = pre[x * length : (x + 1) * length].T
            extra = ref[x, column, length : length + 8].astype(F32)
            values = extra[0:1] + extra[1:2] + extra[2:3]
            offsets = jnp.where(core == 0, values[:, :length], values[:, length : 2 * length])
            offsets_f = jnp.where(
                core == 0, values[:, 2 * length : 3 * length], values[:, 3 * length : 4 * length]
            )
            at = row == 2 * x + home
            gate_pre = jnp.where(core == 0, turned[0:1], turned[1:2])
            forget_pre = jnp.where(core == 0, turned[2:3], turned[3:4])
            gate_in = jnp.where(at, gate_pre + offsets, gate_in)
            forget = jnp.where(at, forget_pre + offsets_f, forget)
    for b in range(ny):
        extra = own_ref[0, b, length : length + 8].astype(F32)
        memory_gain_ref[b : b + 1] = extra[3:4] + extra[4:5] + extra[5:6]
        half = part // 2
        conv_gain_ref[b : b + 1] = extra[6:7, :half] + extra[6:7, half:] + extra[7:8, :half]
    y = jnp.exp(-jnp.abs(forget))
    small = y * (1.0 - y * (1 / 2 - y * (1 / 3 - y * (1 / 4 - y * (1 / 5)))))
    gates_ref[0] = gate_in
    gates_ref[1] = jnp.minimum(forget, 0.0) - jnp.where(y < 0.03, small, jnp.log(1.0 + y))


def finish_kernel(arrived_ref, weight_ref, memory_gain_ref, conv_gain_ref, out_ref):
    nx, nc, ny, _, lanes = arrived_ref.shape
    width = lanes // 2
    chan = width // 2
    length, part = out_ref.shape
    half = length // 2
    memory, conv = [], []
    for b in range(ny):
        blocks = [arrived_ref[x, c, b].astype(F32) for c in range(nc) for x in range(nx)]
        upper = jnp.concatenate([got[:half, :width] for got in blocks], axis=1)
        lower = jnp.concatenate([got[:half, width:] for got in blocks], axis=1)
        memory.append(jnp.concatenate([upper, lower], axis=0))
        quarters = [
            jnp.concatenate([got[half:, k * chan : (k + 1) * chan] for got in blocks], axis=1)
            for k in range(4)
        ]
        conv.append(jnp.concatenate(quarters, axis=0))

    def mean_of(arrays):
        each = sum(arrays)
        return jnp.sum(each, axis=1, keepdims=True) / (ny * each.shape[1])

    scale = lax.rsqrt(mean_of([m * m for m in memory]) + EPS)
    mean = mean_of(conv)
    spread = lax.rsqrt(mean_of([t * t for t in conv]) - mean * mean + EPS)
    deep = weight_ref.shape[5]
    total = jnp.zeros((length, part), F32)
    for b in range(ny):
        scaled = memory[b] * scale * memory_gain_ref[b : b + 1]
        normed = (conv[b] - mean) * spread * conv_gain_ref[b : b + 1]
        branch = normed / (1.0 + jnp.exp(-normed))
        both = jnp.concatenate([scaled.astype(BF16), branch.astype(BF16)], axis=1)
        total = total + dot(both, weight_ref[b].reshape(part, deep), NT)
    out_ref[...] = total.astype(BF16)


HOLD = 32


def tap_rows(taps_ref, core, x_at, nx, lanes):
    chan = lanes // nx
    weights = taps_ref[...].astype(F32)
    weights = jnp.where(core == 0, weights[:, :lanes], weights[:, lanes:])
    weights = pltpu.roll(weights, lax.rem(lanes - chan * x_at, lanes), 1)
    weights = jnp.where(lax.broadcasted_iota(jnp.int32, weights.shape, 1) < chan, weights, 0.0)
    return sum(pltpu.roll(weights, chan * k, 1) for k in range(1, nx)) + weights


def convolve(extended, weights):
    taps = weights.shape[0]
    length = extended.shape[0] - HOLD
    total = jnp.zeros((length, extended.shape[1]), F32)
    first = HOLD - (taps - 1)
    for shift in range(8):
        moved = extended[shift : shift + length + HOLD - 8] if shift else extended
        for j in range(taps):
            at = first + j
            if at % 8 == shift:
                total = total + moved[at - shift : at - shift + length] * weights[j : j + 1]
    return total


def with_logs(kept, width, level, total):
    row = lax.broadcasted_iota(jnp.int32, kept.shape, 0)
    lane = lax.broadcasted_iota(jnp.int32, kept.shape, 1)
    for at, value in ((0, level), (3, total)):
        for k, part in enumerate(three_parts(value)):
            kept = jnp.where((row == width + 1) & (lane == at + k), part, kept)
    return kept


def read_logs(block, width):
    line = block[width + 1 : width + 2, :128].astype(F32)
    level = line[:, 0:1] + line[:, 1:2] + line[:, 2:3]
    return level, line[:, 3:4] + line[:, 4:5] + line[:, 5:6]


def merged(blocks, passed, width):
    acc = jnp.zeros((1, 1), F32)
    logs = []
    for block, use in zip(blocks[::-1], passed[::-1]):
        level, total = read_logs(block, width)
        logs.insert(0, jnp.where(use, level + acc, LOW))
        acc = acc + jnp.where(use, total, 0.0)
    level = logs[0]
    for log in logs[1:]:
        level = jnp.maximum(level, log)
    state = jnp.zeros(blocks[0].shape, F32)
    for block, use, log in zip(blocks, passed, logs):
        state = state + jnp.where(use, jnp.exp(log - level), 0.0) * block.astype(F32)
    return state, level, acc


def slab_kernel(
    qk_ref, v_ref, gate_ref, glu_ref, out_ref, q_ref, k_ref,
):
    chunks, length = gate_ref.shape[1], gate_ref.shape[2]
    width = qk_ref.shape[2] // 2
    gate, forget = gate_ref[0], gate_ref[1]
    within = lane_cumsum(forget)
    ends = [within[r : r + 1, length - 1 :] for r in range(chunks)]
    after = [jnp.zeros((1, 1), F32)]
    for r in range(chunks - 1, 0, -1):
        after.insert(0, after[0] + ends[r])
    total = after[0] + ends[0]
    to_end = jnp.concatenate([e + a for e, a in zip(ends, after)], axis=0)
    end_log = to_end - within + gate
    level = jnp.max(jnp.max(end_log, axis=1, keepdims=True), axis=0, keepdims=True)
    fresh = columns_of(jnp.exp(end_log - level))
    state = jnp.zeros((2 * width, width * qk_ref.shape[0]), F32)
    for r in range(chunks):
        q_ref[r * length : (r + 1) * length] = joined(qk_ref, 0, width, r, length)
        key = joined(qk_ref, width, width, r, length)
        k_ref[r * length : (r + 1) * length] = key
        scaled = (fresh[:, r : r + 1] * key.astype(F32)).astype(BF16)
        state = state + dot(v_ref[r * length : (r + 1) * length], scaled, TN)
    rows, head_lanes = out_ref.shape[1], out_ref.shape[2]
    kept = state[:rows]
    kept = with_logs(kept, width, level, total)
    chan = glu_ref.shape[2] // qk_ref.shape[0]
    hold = HOLD
    tail = glu_ref[glu_ref.shape[0] - 1, length - hold :].astype(F32)[:, glu_ref.shape[2] - chan :]
    group = head_lanes // chan
    each = hold // group
    tail = jnp.concatenate([tail[g * each : (g + 1) * each] for g in range(group)], axis=1)
    kept = jnp.concatenate([kept[: width + 2], tail, kept[width + 2 + each :]], axis=0)
    kept = kept.astype(BF16)
    for j in range(out_ref.shape[0]):
        out_ref[j] = kept


def local_kernel(place_ref, q_ref, k_ref, v_ref, gate_ref, glu_ref, taps_ref, out_ref, conv_ref):
    chunks, length = gate_ref.shape[1], gate_ref.shape[2]
    head = q_ref.shape[1]
    lanes = v_ref.shape[1]
    width = lanes // 2
    nx = chunks // glu_ref.shape[0]
    group = glu_ref.shape[0] * glu_ref.shape[1]
    glu = glu_ref[...].reshape(group, lanes).astype(F32)
    lane = lax.broadcasted_iota(jnp.int32, (HOLD, lanes), 1)
    before = pltpu.roll(glu[group - HOLD :], lanes // nx, 1)
    before = jnp.where(lane < lanes // nx, 0.0, before)
    weights = tap_rows(taps_ref, place_ref[1], place_ref[3], nx, lanes)
    conv_ref[...] = convolve(jnp.concatenate([before, glu], axis=0), weights)

    scale = head ** (-0.5)
    gate, forget = gate_ref[0], gate_ref[1]
    within = lane_cumsum(forget)
    turned = columns_of(jnp.concatenate([within, gate], axis=0))
    causal = lax.broadcasted_iota(jnp.int32, (length, length), 0) >= lax.broadcasted_iota(
        jnp.int32, (length, length), 1
    )
    lane = lax.broadcasted_iota(jnp.int32, (length, lanes), 1)
    state = jnp.zeros((lanes, head), F32)
    level = jnp.full((1, 1), LOW, F32)
    passed = jnp.zeros((1, 1), F32)
    for r in range(chunks):
        here = slice(r * length, (r + 1) * length)
        query, key, value = q_ref[here], k_ref[here], v_ref[here]
        within_row, gate_row = within[r : r + 1], gate[r : r + 1]
        within_col = turned[:, r : r + 1]
        gate_col = turned[:, chunks + r : chunks + r + 1]
        log_weight = jnp.where(causal, within_col - within_row + gate_row, -jnp.inf)
        carried = within_col + level
        top = jnp.maximum(carried, jnp.max(log_weight, axis=1, keepdims=True))
        weight = jnp.exp(log_weight - top)
        carried_weight = jnp.exp(carried - top) * scale
        scores = dot(query, key, NT) * (scale * weight)
        numer = dot(scores.astype(BF16), value, NN)
        denom = jnp.sum(scores, axis=1, keepdims=True)
        if r:
            older = dot(query, state.astype(BF16), NT)
            numer = numer + carried_weight * older
            denom = denom + carried_weight * older[:, width : width + 1]
        sent = jnp.where(lane == width, denom, numer)
        sent = jnp.where(lane == width + 1, top, sent)
        out_ref[here] = jnp.where(lane == width + 2, within_col + passed, sent)
        last = within_row[:, length - 1 :]
        passed = passed + last
        end_row = last - within_row + gate_row
        new_level = jnp.maximum(last + level, jnp.max(end_row, axis=1, keepdims=True))
        keep = jnp.exp(last + level - new_level)
        fresh = jnp.exp(last - within_col + gate_col - new_level)
        scaled = (fresh * key.astype(F32)).astype(BF16)
        state = keep * state + dot(value, scaled, TN)
        level = new_level


def cell_kernel(place_ref, in_ref, q_ref, local_ref, conv_ref, taps_ref, out_ref):
    members, rows, head = in_ref.shape
    nx, nc, ny, _, lanes = out_ref.shape
    width, chan = lanes // 2, lanes // nx
    length = q_ref.shape[0] // (nx * nc)
    scale = head ** (-0.5)
    place = place_ref[0]
    blocks = [in_ref[j] for j in range(members)]
    passed = [j < place for j in range(members)]
    state, level, _ = merged(blocks, passed, width)
    state = jnp.concatenate([state, jnp.zeros((lanes - rows, head), F32)], axis=0).astype(BF16)

    group = head // chan
    each = HOLD // group
    last_rows = in_ref[jnp.maximum(place - 1, 0), width : width + 8].astype(F32)
    last_rows = jnp.where(place > 0, last_rows, 0.0)
    last_rows = last_rows[2 : 2 + each]
    prior = jnp.concatenate([last_rows[:, g * chan : (g + 1) * chan] for g in range(group)], axis=0)
    prior = jnp.concatenate([prior, jnp.zeros((HOLD, lanes - chan), F32)], axis=1)
    weights = tap_rows(taps_ref, place_ref[1], place_ref[3], nx, lanes)
    edge = convolve(jnp.concatenate([prior, jnp.zeros((HOLD, lanes), F32)], axis=0), weights)
    half, quarter = length // 2, length // 4
    for r in range(nx * nc):
        here = slice(r * length, (r + 1) * length)
        local = local_ref[here]
        top_here, since = local[:, width + 1 : width + 2], local[:, width + 2 : width + 3]
        carried = since + level
        top = jnp.maximum(carried, top_here)
        local_weight = jnp.exp(top_here - top)
        carried_weight = jnp.exp(carried - top) * scale
        mixed = local_weight * local + carried_weight * dot(q_ref[here], state, NT)
        denom = mixed[:, width : width + 1]
        result = mixed[:, :width] / jnp.maximum(jnp.abs(denom), 1.0)
        x, c = r // nc, r % nc
        memory = jnp.concatenate([result[:half], result[half:]], axis=1)
        branch = []
        for g in range(4):
            at = c * length + g * quarter
            part = conv_ref[at : at + quarter]
            if at == 0:
                part = part + edge
            branch.append(part[:, x * chan : (x + 1) * chan])
        sent = jnp.concatenate([memory, jnp.concatenate(branch, axis=1)], axis=0).astype(BF16)
        for y in range(ny):
            out_ref[x, c, y] = sent


def vmem(count):
    return [pl.BlockSpec(memory_space=pltpu.VMEM)] * count


def layer(
    tokens,
    conv_value_weight,
    conv_gate_weight,
    conv_kernel,
    conv_norm_gain,
    query_weight,
    key_weight,
    value_weight,
    input_gate_weight,
    forget_gate_weight,
    input_offset,
    forget_offset,
    memory_norm_gain,
    conv_out_weight,
    memory_out_weight,
):
    nzh, nzl, nx, nc, ny = (size(a) for a in AXES)
    xi, ci, yi = lax.axis_index("x"), lax.axis_index("c"), lax.axis_index("tp")
    members = nzh * nzl
    zi = lax.axis_index("zh") * nzl + lax.axis_index("zl")
    length, part = tokens.shape
    slab = length * nx * nc
    head = query_weight.shape[1] // nc
    width = head // nx
    chan = conv_value_weight.shape[1] // nc // nx
    rows = query_weight.shape[0]
    wide = 3 * width + 2 * chan

    def from_z(value, ahead):
        return lax.ppermute(value, Z, [(j, (j - ahead) % members) for j in range(members)])

    deep = memory_out_weight.shape[0] + conv_out_weight.shape[0]
    pieces, out_rows = pl.pallas_call(
        piece_kernel,
        out_shape=(
            jax.ShapeDtypeStruct((nx, nc, rows, wide), BF16),
            jax.ShapeDtypeStruct((deep // wide * rows, wide), BF16),
        ),
        in_specs=vmem(7),
        out_specs=vmem(2),
        interpret=INTERPRET,
        name="pieces",
    )(
        query_weight,
        key_weight,
        value_weight,
        conv_value_weight,
        conv_gate_weight,
        memory_out_weight.T,
        conv_out_weight.T,
    )
    offsets = jnp.concatenate([input_offset.T, forget_offset.T], axis=0)
    call_pack = pl.pallas_call(
        pack_kernel,
        out_shape=jax.ShapeDtypeStruct((nx * ny, length + 8, part), BF16),
        in_specs=vmem(4),
        out_specs=pl.BlockSpec(memory_space=pltpu.VMEM),
        interpret=INTERPRET,
        name="pack",
    )
    sent = call_pack(tokens, offsets, conv_norm_gain[None], memory_norm_gain[None])
    mine = exchange(pieces.reshape(nx * nc, rows, wide), ("x", "c"))
    mine = jnp.concatenate([mine.reshape(nx * nc * rows, wide), out_rows], axis=0)
    step = members // 4
    opposite = from_z(mine, 2 * step)
    far = [from_z(mine, -step), mine, from_z(mine, step), opposite]
    own = exchange(sent, ("x", "tp")).reshape(nx, ny, length + 8, part)
    half_shape = (nzh // 2, *mine.shape)
    call_arrange = pl.pallas_call(
        arrange_kernel,
        out_shape=(
            jax.ShapeDtypeStruct((nzh, *mine.shape), BF16),
            jax.ShapeDtypeStruct(half_shape, BF16),
            jax.ShapeDtypeStruct(half_shape, BF16),
        ),
        in_specs=vmem(4),
        out_specs=vmem(3),
        interpret=INTERPRET,
        name="arrange",
    )
    near, *halves = call_arrange(*far)
    sets = [near, from_z(near, 1), from_z(near, -1)]
    sets += [from_z(halves[0], 2), from_z(halves[1], -2)]
    other = swapped(own, "c")

    gate_weight = jnp.pad(
        jnp.concatenate([input_gate_weight, forget_gate_weight], axis=1), ((0, 0), (0, 124))
    )
    place = jnp.stack([zi, ci, yi, xi])
    smem = pl.BlockSpec(memory_space=pltpu.SMEM)
    qk, value, packed, gates, memory_gain, conv_gain, out_part = pl.pallas_call(
        project_kernel,
        out_shape=(
            jax.ShapeDtypeStruct((nx, nx, nc, length, 2 * width), BF16),
            jax.ShapeDtypeStruct((nx, nc, length, 2 * width), BF16),
            jax.ShapeDtypeStruct((nc, length, nx * chan), BF16),
            jax.ShapeDtypeStruct((2, nx * nc, length), F32),
            jax.ShapeDtypeStruct((ny, memory_norm_gain.shape[0]), F32),
            jax.ShapeDtypeStruct((ny, conv_norm_gain.shape[0]), F32),
            jax.ShapeDtypeStruct((nzh, nzl, rows, deep), BF16),
        ),
        in_specs=[smem] + vmem(8),
        out_specs=vmem(7),
        interpret=INTERPRET,
        name="project",
    )(place, own, other, *sets, gate_weight)
    value = value.reshape(slab, 2 * width)
    all_qk = exchange(qk.reshape(nx, slab, 2 * width), "x")
    out_part = [out_part[0]] + [
        lax.ppermute(out_part[ahead], "tp", [(j, (j + ahead) % ny) for j in range(ny)])
        for ahead in range(1, ny)
    ]
    out_part = jnp.stack(out_part, axis=0)

    def from_x(value, ahead):
        return lax.ppermute(value, "x", [(j, (j - ahead) % nx) for j in range(nx)])

    out_parts = [out_part, from_x(out_part, 1)]
    from_last = from_x(out_part, 3)
    out_parts += [from_x(out_part, 2), from_last]
    other_parts = [swapped(out, "c") for out in out_parts[:2]]
    other_parts += [swapped(out, "c") for out in out_parts[2:]]

    state_rows = width + 8
    call_slab = pl.pallas_call(
        slab_kernel,
        out_shape=(
            jax.ShapeDtypeStruct((members, state_rows, head), BF16),
            jax.ShapeDtypeStruct((slab, head), BF16),
            jax.ShapeDtypeStruct((slab, head), BF16),
        ),
        in_specs=vmem(4),
        out_specs=vmem(3),
        interpret=INTERPRET,
        name="slab_state",
    )
    states, query, key = call_slab(all_qk, value, gates, packed)
    states = exchange(states, Z)
    call_local = pl.pallas_call(
        local_kernel,
        out_shape=(
            jax.ShapeDtypeStruct((slab, 2 * width), F32),
            jax.ShapeDtypeStruct((nc * length, nx * chan), F32),
        ),
        in_specs=[smem] + vmem(6),
        out_specs=vmem(2),
        interpret=INTERPRET,
        name="local",
    )
    local, conv = call_local(place, query, key, value, gates, packed, conv_kernel)
    call_cell = pl.pallas_call(
        cell_kernel,
        out_shape=jax.ShapeDtypeStruct((nx, nc, ny, length // 4 * 3, 2 * width), BF16),
        in_specs=[smem] + vmem(5),
        out_specs=pl.BlockSpec(memory_space=pltpu.VMEM),
        interpret=INTERPRET,
        name="cell",
    )
    last = call_cell(place, states, query, local, conv, conv_kernel)
    arrived = exchange(last.reshape(nx * nc * ny, length // 4 * 3, -1), ("x", "c", "tp"))
    arrived = arrived.reshape(nx, nc, ny, length // 4 * 3, -1)
    call_assemble = pl.pallas_call(
        assemble_kernel,
        out_shape=jax.ShapeDtypeStruct((ny, nzl, nx, nc, rows, deep), BF16),
        in_specs=[smem] + vmem(2 * nx),
        out_specs=pl.BlockSpec(memory_space=pltpu.VMEM),
        interpret=INTERPRET,
        name="assemble",
    )
    out_weight = call_assemble(place, *out_parts, *other_parts)
    return pl.pallas_call(
        finish_kernel,
        out_shape=jax.ShapeDtypeStruct((length, part), BF16),
        in_specs=vmem(4),
        out_specs=pl.BlockSpec(memory_space=pltpu.VMEM),
        interpret=INTERPRET,
        name="finish",
    )(arrived, out_weight, memory_gain, conv_gain)


def solution(mesh):
    shape = mesh.shape
    depth = shape["sp"] // 32
    split = Mesh(mesh.devices.reshape(4, depth, 4, 2, shape["tp"]), AXES)
    in_specs = (
        P(SP, "tp"),
        P(SP, "tp"),
        P(SP, "tp"),
        P(None, "tp"),
        P("tp"),
        P(SP, "tp"),
        P(SP, "tp"),
        P(SP, "tp"),
        P(None, "tp"),
        P(None, "tp"),
        P(SP, "tp"),
        P(SP, "tp"),
        P("tp"),
        P("tp", SP),
        P("tp", SP),
    )
    return jax.shard_map(
        layer, mesh=split, in_specs=in_specs, out_specs=P(SP, "tp"), check_vma=False
    )
```

```python
import jax
import jax.numpy as jnp
from jax import lax
from jax.experimental import pallas as pl
from jax.experimental.pallas import tpu as pltpu
from jax.sharding import Mesh
from jax.sharding import PartitionSpec as P

AXES = ("zh", "zl", "x", "c", "tp")
Z = ("zh", "zl")
SP = ("zh", "zl", "x", "c")
EPS = 1e-06
LOW = -1e30
F32 = jnp.float32
BF16 = jnp.bfloat16
INTERPRET = False


def size(axis):
    return lax.axis_size(axis)


def exchange(pieces, axes):
    return lax.all_to_all(pieces, axes, split_axis=0, concat_axis=0, tiled=True)


def swapped(value, axis):
    return lax.ppermute(value, axis, [(0, 1), (1, 0)])


def lane_cumsum(rows):
    lane = lax.broadcasted_iota(jnp.int32, rows.shape, 1)
    step = 1
    while step < rows.shape[1]:
        moved = pltpu.roll(rows, step, 1)
        rows = rows + jnp.where(lane >= step, moved, 0.0)
        step *= 2
    return rows


def columns_of(rows):
    count, length = rows.shape
    square = jnp.concatenate([rows, jnp.zeros((length - count, length), F32)], axis=0)
    return square.T


def dot(a, b, dims):
    return lax.dot_general(a, b, (dims, ((), ())), preferred_element_type=F32)


NN = ((1,), (0,))
NT = ((1,), (1,))
TN = ((0,), (0,))


def joined(parts_ref, start, width, chunk, length):
    picked = [
        parts_ref[j, chunk * length : (chunk + 1) * length, start : start + width]
        for j in range(parts_ref.shape[0])
    ]
    return jnp.concatenate(picked, axis=1)


def three_parts(value):
    high = value.astype(BF16).astype(F32)
    mid = (value - high).astype(BF16).astype(F32)
    return high, mid, value - high - mid


def pack_kernel(tokens_ref, offsets_ref, conv_gain_ref, memory_gain_ref, out_ref):
    length = tokens_ref.shape[0]
    offsets = three_parts(offsets_ref[...])
    conv_gain = three_parts(conv_gain_ref[...])
    memory_gain = three_parts(memory_gain_ref[...])
    rows = [jnp.concatenate([p[k : k + 1] for k in range(p.shape[0])], axis=1) for p in offsets]
    rows += memory_gain
    rows.append(jnp.concatenate(conv_gain[:2], axis=1))
    rows.append(jnp.concatenate([conv_gain[2], jnp.zeros_like(conv_gain[2])], axis=1))
    extra = jnp.concatenate(rows, axis=0).astype(BF16)
    tokens = tokens_ref[...]
    for j in range(out_ref.shape[0]):
        out_ref[j, :length] = tokens
        out_ref[j, length:] = extra


def piece_kernel(
    query_ref, key_ref, value_ref, left_ref, right_ref, memory_ref, conv_ref, out_ref, turn_ref
):
    nx, nc = out_ref.shape[0], out_ref.shape[1]
    rows = memory_ref.shape[0]
    whole = jnp.concatenate([memory_ref[...], conv_ref[...]], axis=1)
    wide = out_ref.shape[3]
    for j in range(whole.shape[1] // wide):
        turn_ref[j * rows : (j + 1) * rows] = whole[:, j * wide : (j + 1) * wide]
    for x in range(nx):
        for c in range(nc):
            at = c * nx + x
            parts = []
            for ref in (query_ref, key_ref, value_ref, left_ref, right_ref):
                width = ref.shape[1] // (nx * nc)
                parts.append(ref[:, at * width : (at + 1) * width])
            out_ref[x, c] = jnp.concatenate(parts, axis=1)


def assemble_kernel(place_ref, *refs):
    out_ref = refs[-1]
    nx, ny = out_ref.shape[2], out_ref.shape[0]
    core, column, x_at = place_ref[1], place_ref[2], place_ref[3]
    for ahead in range(nx):
        x = lax.rem(x_at + ahead, nx)
        for c, ref in ((core, refs[ahead]), (1 - core, refs[nx + ahead])):
            for b in range(ny):
                at = lax.rem(column + ny - b, ny)
                for near in range(ref.shape[1]):
                    out_ref[pl.ds(at, 1), near, pl.ds(x, 1), pl.ds(c, 1)] = ref[b, near][
                        None, None, None
                    ]


def project_kernel(
    place_ref, own_ref, other_ref,
    w0_ref, w1_ref, w3_ref, low_ref, high_ref, gate_ref,
    qk_ref, v_ref, glu_ref, gates_ref, memory_gain_ref, conv_gain_ref, out_weight_ref,
):
    nx, ny, _, part = own_ref.shape
    far, tall, wide = w0_ref.shape
    depth, chunks = out_weight_ref.shape[2], out_weight_ref.shape[3] // wide
    rows = tall - depth * chunks
    close = part // rows
    length = glu_ref.shape[1]
    place, core, column = place_ref[0], place_ref[1], place_ref[2]
    tokens_rows = nx * length
    width = qk_ref.shape[4] // 2
    chan = glu_ref.shape[2] // nx
    lane = lax.broadcasted_iota(jnp.int32, (length, width), 1)
    ones = jnp.where(lane == 0, 1.0, 0.0).astype(BF16)
    row = lax.broadcasted_iota(jnp.int32, (2 * nx, length), 0)
    gate_in = jnp.zeros((2 * nx, length), F32)
    forget = jnp.zeros((2 * nx, length), F32)

    members = far * close
    blocks = [
        (ref, i, ahead + close * (i - 1))
        for ref, ahead in ((w0_ref, 0), (w1_ref, 1), (w3_ref, -1))
        for i in range(far)
    ]
    blocks += [(low_ref, i, 2 + close * i) for i in range(far // 2)]
    blocks += [(high_ref, i, -2 + close * (i - 1)) for i in range(far // 2)]
    homes = []
    for ref, i, ahead in blocks:
        home = lax.rem(place + (ahead + members), members)
        y = lax.div(home, close)
        homes.append((y, lax.rem(home, close)))
        behind = lax.rem(y + ny - column, ny)
        out_weight_ref[pl.ds(behind, 1), pl.ds(homes[-1][1], 1)] = jnp.concatenate(
            [ref[i, rows + j * depth : rows + (j + 1) * depth] for j in range(chunks)], axis=1
        )[None, None]
    right = []
    for (w_ref, i, _), (y, z) in zip(blocks, homes):
        start = pl.multiple_of(y * part + z * rows, rows)
        right.append(jnp.concatenate([w_ref[i, :rows], gate_ref[pl.ds(start, rows)]], axis=1))
    right = jnp.concatenate(right, axis=0)
    for half, ref in enumerate((own_ref, other_ref)):
        home = core if half == 0 else 1 - core
        left = []
        for y, z in homes:
            lanes = pl.ds(pl.multiple_of(z * rows, rows), rows)
            left.append(ref[:, pl.ds(y, 1), :length, lanes].reshape(tokens_rows, rows))
        acc = dot(jnp.concatenate(left, axis=1), right, NN)
        pre = acc[:, wide:]
        glu = []
        for x in range(nx):
            mine = acc[x * length : (x + 1) * length]
            qk = mine[:, : 2 * width].astype(BF16)[None]
            for j in range(qk_ref.shape[0]):
                qk_ref[j, x, pl.ds(home, 1)] = qk
            v_ref[x, pl.ds(home, 1)] = jnp.concatenate(
                [mine[:, 2 * width : 3 * width].astype(BF16), ones], axis=1
            )[None]
            left = mine[:, 3 * width : 3 * width + chan]
            gates_side = mine[:, 3 * width + chan : wide]
            glu.append(left / (1.0 + jnp.exp(-gates_side)))
        glu_ref[pl.ds(home, 1)] = jnp.concatenate(glu, axis=1).astype(BF16)[None]
        for x in range(nx):
            turned = pre[x * length : (x + 1) * length].T
            extra = ref[x, column, length : length + 8].astype(F32)
            values = extra[0:1] + extra[1:2] + extra[2:3]
            offsets = jnp.where(core == 0, values[:, :length], values[:, length : 2 * length])
            offsets_f = jnp.where(
                core == 0, values[:, 2 * length : 3 * length], values[:, 3 * length : 4 * length]
            )
            at = row == 2 * x + home
            gate_pre = jnp.where(core == 0, turned[0:1], turned[1:2])
            forget_pre = jnp.where(core == 0, turned[2:3], turned[3:4])
            gate_in = jnp.where(at, gate_pre + offsets, gate_in)
            forget = jnp.where(at, forget_pre + offsets_f, forget)
    for b in range(ny):
        extra = own_ref[0, b, length : length + 8].astype(F32)
        memory_gain_ref[b : b + 1] = extra[3:4] + extra[4:5] + extra[5:6]
        half = part // 2
        conv_gain_ref[b : b + 1] = extra[6:7, :half] + extra[6:7, half:] + extra[7:8, :half]
    y = jnp.exp(-jnp.abs(forget))
    small = y * (1.0 - y * (1 / 2 - y * (1 / 3 - y * (1 / 4 - y * (1 / 5)))))
    gates_ref[0] = gate_in
    gates_ref[1] = jnp.minimum(forget, 0.0) - jnp.where(y < 0.03, small, jnp.log(1.0 + y))


def finish_kernel(arrived_ref, weight_ref, memory_gain_ref, conv_gain_ref, out_ref):
    nx, nc, ny, _, lanes = arrived_ref.shape
    width = lanes // 2
    chan = width // 2
    length, part = out_ref.shape
    half = length // 2
    memory, conv = [], []
    for b in range(ny):
        blocks = [arrived_ref[x, c, b].astype(F32) for c in range(nc) for x in range(nx)]
        upper = jnp.concatenate([got[:half, :width] for got in blocks], axis=1)
        lower = jnp.concatenate([got[:half, width:] for got in blocks], axis=1)
        memory.append(jnp.concatenate([upper, lower], axis=0))
        quarters = [
            jnp.concatenate([got[half:, k * chan : (k + 1) * chan] for got in blocks], axis=1)
            for k in range(4)
        ]
        conv.append(jnp.concatenate(quarters, axis=0))

    def mean_of(arrays):
        each = sum(arrays)
        return jnp.sum(each, axis=1, keepdims=True) / (ny * each.shape[1])

    scale = lax.rsqrt(mean_of([m * m for m in memory]) + EPS)
    mean = mean_of(conv)
    spread = lax.rsqrt(mean_of([t * t for t in conv]) - mean * mean + EPS)
    deep = weight_ref.shape[5]
    total = jnp.zeros((length, part), F32)
    for b in range(ny):
        scaled = memory[b] * scale * memory_gain_ref[b : b + 1]
        normed = (conv[b] - mean) * spread * conv_gain_ref[b : b + 1]
        branch = normed / (1.0 + jnp.exp(-normed))
        both = jnp.concatenate([scaled.astype(BF16), branch.astype(BF16)], axis=1)
        total = total + dot(both, weight_ref[b].reshape(part, deep), NT)
    out_ref[...] = total.astype(BF16)


HOLD = 32


def tap_rows(taps_ref, core, x_at, nx, lanes):
    chan = lanes // nx
    weights = taps_ref[...].astype(F32)
    weights = jnp.where(core == 0, weights[:, :lanes], weights[:, lanes:])
    weights = pltpu.roll(weights, lax.rem(lanes - chan * x_at, lanes), 1)
    weights = jnp.where(lax.broadcasted_iota(jnp.int32, weights.shape, 1) < chan, weights, 0.0)
    return sum(pltpu.roll(weights, chan * k, 1) for k in range(1, nx)) + weights


def convolve(extended, weights):
    taps = weights.shape[0]
    length = extended.shape[0] - HOLD
    total = jnp.zeros((length, extended.shape[1]), F32)
    first = HOLD - (taps - 1)
    for shift in range(8):
        moved = extended[shift : shift + length + HOLD - 8] if shift else extended
        for j in range(taps):
            at = first + j
            if at % 8 == shift:
                total = total + moved[at - shift : at - shift + length] * weights[j : j + 1]
    return total


def with_logs(kept, width, level, total):
    row = lax.broadcasted_iota(jnp.int32, kept.shape, 0)
    lane = lax.broadcasted_iota(jnp.int32, kept.shape, 1)
    for at, value in ((0, level), (3, total)):
        for k, part in enumerate(three_parts(value)):
            kept = jnp.where((row == width + 1) & (lane == at + k), part, kept)
    return kept


def read_logs(block, width):
    line = block[width + 1 : width + 2, :128].astype(F32)
    level = line[:, 0:1] + line[:, 1:2] + line[:, 2:3]
    return level, line[:, 3:4] + line[:, 4:5] + line[:, 5:6]


def merged(blocks, passed, width):
    acc = jnp.zeros((1, 1), F32)
    logs = []
    for block, use in zip(blocks[::-1], passed[::-1]):
        level, total = read_logs(block, width)
        logs.insert(0, jnp.where(use, level + acc, LOW))
        acc = acc + jnp.where(use, total, 0.0)
    level = logs[0]
    for log in logs[1:]:
        level = jnp.maximum(level, log)
    state = jnp.zeros(blocks[0].shape, F32)
    for block, use, log in zip(blocks, passed, logs):
        state = state + jnp.where(use, jnp.exp(log - level), 0.0) * block.astype(F32)
    return state, level, acc


def group_kernel(in_ref, out_ref):
    members, rows, _ = in_ref.shape
    width = rows - 8
    blocks = [in_ref[j] for j in range(members)]
    state, level, total = merged(blocks, [True] * members, width)
    last = blocks[-1].astype(F32)
    kept = jnp.concatenate([state[: width + 2], last[width + 2 :]], axis=0)
    kept = with_logs(kept, width, level, total).astype(BF16)
    for j in range(out_ref.shape[0]):
        out_ref[j] = kept


def slab_kernel(
    qk_ref, v_ref, gate_ref, glu_ref, out_ref,
):
    chunks, length = gate_ref.shape[1], gate_ref.shape[2]
    width = qk_ref.shape[2] // 2
    gate, forget = gate_ref[0], gate_ref[1]
    within = lane_cumsum(forget)
    ends = [within[r : r + 1, length - 1 :] for r in range(chunks)]
    after = [jnp.zeros((1, 1), F32)]
    for r in range(chunks - 1, 0, -1):
        after.insert(0, after[0] + ends[r])
    total = after[0] + ends[0]
    to_end = jnp.concatenate([e + a for e, a in zip(ends, after)], axis=0)
    end_log = to_end - within + gate
    level = jnp.max(jnp.max(end_log, axis=1, keepdims=True), axis=0, keepdims=True)
    fresh = columns_of(jnp.exp(end_log - level))
    state = jnp.zeros((2 * width, width * qk_ref.shape[0]), F32)
    for r in range(chunks):
        key = joined(qk_ref, width, width, r, length)
        scaled = (fresh[:, r : r + 1] * key.astype(F32)).astype(BF16)
        state = state + dot(v_ref[r * length : (r + 1) * length], scaled, TN)
    rows, head_lanes = out_ref.shape[1], out_ref.shape[2]
    kept = state[:rows]
    kept = with_logs(kept, width, level, total)
    chan = glu_ref.shape[2] // qk_ref.shape[0]
    hold = HOLD
    tail = glu_ref[glu_ref.shape[0] - 1, length - hold :].astype(F32)[:, glu_ref.shape[2] - chan :]
    group = head_lanes // chan
    each = hold // group
    tail = jnp.concatenate([tail[g * each : (g + 1) * each] for g in range(group)], axis=1)
    kept = jnp.concatenate([kept[: width + 2], tail, kept[width + 2 + each :]], axis=0)
    kept = kept.astype(BF16)
    for j in range(out_ref.shape[0]):
        out_ref[j] = kept


def local_kernel(place_ref, qk_ref, v_ref, gate_ref, glu_ref, taps_ref, out_ref, conv_ref, q_ref):
    chunks, length = gate_ref.shape[1], gate_ref.shape[2]
    head = q_ref.shape[1]
    lanes = v_ref.shape[1]
    width = lanes // 2
    nx = chunks // glu_ref.shape[0]
    group = glu_ref.shape[0] * glu_ref.shape[1]
    glu = glu_ref[...].reshape(group, lanes).astype(F32)
    lane = lax.broadcasted_iota(jnp.int32, (HOLD, lanes), 1)
    before = pltpu.roll(glu[group - HOLD :], lanes // nx, 1)
    before = jnp.where(lane < lanes // nx, 0.0, before)
    weights = tap_rows(taps_ref, place_ref[1], place_ref[3], nx, lanes)
    conv_ref[...] = convolve(jnp.concatenate([before, glu], axis=0), weights)

    scale = head ** (-0.5)
    gate, forget = gate_ref[0], gate_ref[1]
    within = lane_cumsum(forget)
    turned = columns_of(jnp.concatenate([within, gate], axis=0))
    causal = lax.broadcasted_iota(jnp.int32, (length, length), 0) >= lax.broadcasted_iota(
        jnp.int32, (length, length), 1
    )
    lane = lax.broadcasted_iota(jnp.int32, (length, lanes), 1)
    state = jnp.zeros((lanes, head), F32)
    level = jnp.full((1, 1), LOW, F32)
    passed = jnp.zeros((1, 1), F32)
    for r in range(chunks):
        here = slice(r * length, (r + 1) * length)
        value = v_ref[here]
        query = joined(qk_ref, 0, width, r, length)
        key = joined(qk_ref, width, width, r, length)
        q_ref[here] = query
        within_row, gate_row = within[r : r + 1], gate[r : r + 1]
        within_col = turned[:, r : r + 1]
        gate_col = turned[:, chunks + r : chunks + r + 1]
        log_weight = jnp.where(causal, within_col - within_row + gate_row, -jnp.inf)
        carried = within_col + level
        top = jnp.maximum(carried, jnp.max(log_weight, axis=1, keepdims=True))
        weight = jnp.exp(log_weight - top)
        carried_weight = jnp.exp(carried - top) * scale
        scores = dot(query, key, NT) * (scale * weight)
        numer = dot(scores.astype(BF16), value, NN)
        denom = jnp.sum(scores, axis=1, keepdims=True)
        if r:
            older = dot(query, state.astype(BF16), NT)
            numer = numer + carried_weight * older
            denom = denom + carried_weight * older[:, width : width + 1]
        sent = jnp.where(lane == width, denom, numer)
        sent = jnp.where(lane == width + 1, top, sent)
        out_ref[here] = jnp.where(lane == width + 2, within_col + passed, sent)
        last = within_row[:, length - 1 :]
        passed = passed + last
        end_row = last - within_row + gate_row
        new_level = jnp.maximum(last + level, jnp.max(end_row, axis=1, keepdims=True))
        keep = jnp.exp(last + level - new_level)
        fresh = jnp.exp(last - within_col + gate_col - new_level)
        scaled = (fresh * key.astype(F32)).astype(BF16)
        state = keep * state + dot(value, scaled, TN)
        level = new_level


def cell_kernel(place_ref, far_ref, in_ref, q_ref, local_ref, conv_ref, taps_ref, out_ref):
    members, rows, head = in_ref.shape
    groups = far_ref.shape[0]
    nx, nc, ny, _, lanes = out_ref.shape
    width, chan = lanes // 2, lanes // nx
    length = q_ref.shape[0] // (nx * nc)
    scale = head ** (-0.5)
    place = place_ref[0]
    at_far, at_close = lax.div(place, members), lax.rem(place, members)
    blocks = [far_ref[j] for j in range(groups)] + [in_ref[j] for j in range(members)]
    passed = [j < at_far for j in range(groups)] + [j < at_close for j in range(members)]
    state, level, _ = merged(blocks, passed, width)
    state = jnp.concatenate([state, jnp.zeros((lanes - rows, head), F32)], axis=0).astype(BF16)

    group = head // chan
    each = HOLD // group
    near_rows = in_ref[jnp.maximum(at_close - 1, 0), width : width + 8].astype(F32)
    far_rows = far_ref[jnp.maximum(at_far - 1, 0), width : width + 8].astype(F32)
    last_rows = jnp.where(at_close > 0, near_rows, jnp.where(at_far > 0, far_rows, 0.0))
    last_rows = last_rows[2 : 2 + each]
    prior = jnp.concatenate([last_rows[:, g * chan : (g + 1) * chan] for g in range(group)], axis=0)
    prior = jnp.concatenate([prior, jnp.zeros((HOLD, lanes - chan), F32)], axis=1)
    weights = tap_rows(taps_ref, place_ref[1], place_ref[3], nx, lanes)
    edge = convolve(jnp.concatenate([prior, jnp.zeros((HOLD, lanes), F32)], axis=0), weights)
    half, quarter = length // 2, length // 4
    for r in range(nx * nc):
        here = slice(r * length, (r + 1) * length)
        local = local_ref[here]
        top_here, since = local[:, width + 1 : width + 2], local[:, width + 2 : width + 3]
        carried = since + level
        top = jnp.maximum(carried, top_here)
        local_weight = jnp.exp(top_here - top)
        carried_weight = jnp.exp(carried - top) * scale
        mixed = local_weight * local + carried_weight * dot(q_ref[here], state, NT)
        denom = mixed[:, width : width + 1]
        result = mixed[:, :width] / jnp.maximum(jnp.abs(denom), 1.0)
        x, c = r // nc, r % nc
        memory = jnp.concatenate([result[:half], result[half:]], axis=1)
        branch = []
        for g in range(4):
            at = c * length + g * quarter
            part = conv_ref[at : at + quarter]
            if at == 0:
                part = part + edge
            branch.append(part[:, x * chan : (x + 1) * chan])
        sent = jnp.concatenate([memory, jnp.concatenate(branch, axis=1)], axis=0).astype(BF16)
        for y in range(ny):
            out_ref[x, c, y] = sent


def vmem(count):
    return [pl.BlockSpec(memory_space=pltpu.VMEM)] * count


def layer(
    tokens,
    conv_value_weight,
    conv_gate_weight,
    conv_kernel,
    conv_norm_gain,
    query_weight,
    key_weight,
    value_weight,
    input_gate_weight,
    forget_gate_weight,
    input_offset,
    forget_offset,
    memory_norm_gain,
    conv_out_weight,
    memory_out_weight,
):
    nzh, nzl, nx, nc, ny = (size(a) for a in AXES)
    xi, ci, yi = lax.axis_index("x"), lax.axis_index("c"), lax.axis_index("tp")
    members = nzh * nzl
    zi = lax.axis_index("zh") * nzl + lax.axis_index("zl")
    length, part = tokens.shape
    slab = length * nx * nc
    head = query_weight.shape[1] // nc
    width = head // nx
    chan = conv_value_weight.shape[1] // nc // nx
    rows = query_weight.shape[0]
    wide = 3 * width + 2 * chan

    def from_z(value, ahead):
        return lax.ppermute(value, Z, [(j, (j - ahead) % members) for j in range(members)])

    deep = memory_out_weight.shape[0] + conv_out_weight.shape[0]
    pieces, out_rows = pl.pallas_call(
        piece_kernel,
        out_shape=(
            jax.ShapeDtypeStruct((nx, nc, rows, wide), BF16),
            jax.ShapeDtypeStruct((deep // wide * rows, wide), BF16),
        ),
        in_specs=vmem(7),
        out_specs=vmem(2),
        interpret=INTERPRET,
        name="pieces",
    )(
        query_weight,
        key_weight,
        value_weight,
        conv_value_weight,
        conv_gate_weight,
        memory_out_weight.T,
        conv_out_weight.T,
    )
    offsets = jnp.concatenate([input_offset.T, forget_offset.T], axis=0)
    call_pack = pl.pallas_call(
        pack_kernel,
        out_shape=jax.ShapeDtypeStruct((nx * ny, length + 8, part), BF16),
        in_specs=vmem(4),
        out_specs=pl.BlockSpec(memory_space=pltpu.VMEM),
        interpret=INTERPRET,
        name="pack",
    )
    sent = call_pack(tokens, offsets, conv_norm_gain[None], memory_norm_gain[None])
    mine = exchange(pieces.reshape(nx * nc, rows, wide), ("x", "c"))
    mine = jnp.concatenate([mine.reshape(nx * nc * rows, wide), out_rows], axis=0)
    step = members // 4
    opposite = from_z(mine, 2 * step)
    far = [from_z(mine, -step), mine, from_z(mine, step), opposite]
    own = exchange(sent, ("x", "tp")).reshape(nx, ny, length + 8, part)
    near = jnp.stack(far, axis=0)
    halves = near[1:3], near[:2]
    sets = [near, from_z(near, 1), from_z(near, -1)]
    sets += [from_z(halves[0], 2), from_z(halves[1], -2)]
    other = swapped(own, "c")

    gate_weight = jnp.pad(
        jnp.concatenate([input_gate_weight, forget_gate_weight], axis=1), ((0, 0), (0, 124))
    )
    place = jnp.stack([zi, ci, yi, xi])
    smem = pl.BlockSpec(memory_space=pltpu.SMEM)
    qk, value, packed, gates, memory_gain, conv_gain, out_part = pl.pallas_call(
        project_kernel,
        out_shape=(
            jax.ShapeDtypeStruct((nx, nx, nc, length, 2 * width), BF16),
            jax.ShapeDtypeStruct((nx, nc, length, 2 * width), BF16),
            jax.ShapeDtypeStruct((nc, length, nx * chan), BF16),
            jax.ShapeDtypeStruct((2, nx * nc, length), F32),
            jax.ShapeDtypeStruct((ny, memory_norm_gain.shape[0]), F32),
            jax.ShapeDtypeStruct((ny, conv_norm_gain.shape[0]), F32),
            jax.ShapeDtypeStruct((nzh, nzl, rows, deep), BF16),
        ),
        in_specs=[smem] + vmem(8),
        out_specs=vmem(7),
        interpret=INTERPRET,
        name="project",
    )(place, own, other, *sets, gate_weight)
    value = value.reshape(slab, 2 * width)
    all_qk = exchange(qk.reshape(nx, slab, 2 * width), "x")
    out_part = [out_part[0]] + [
        lax.ppermute(out_part[ahead], "tp", [(j, (j + ahead) % ny) for j in range(ny)])
        for ahead in range(1, ny)
    ]
    out_part = jnp.stack(out_part, axis=0)

    def from_x(value, ahead):
        return lax.ppermute(value, "x", [(j, (j - ahead) % nx) for j in range(nx)])

    out_parts = [out_part, from_x(out_part, 1)]
    from_last = from_x(out_part, 3)
    out_parts += [from_x(out_part, 2), from_last]
    other_parts = [swapped(out, "c") for out in out_parts[:2]]
    other_parts += [swapped(out, "c") for out in out_parts[2:]]

    state_rows = width + 8
    keys = all_qk.reshape(nx, slab, 2 * width)
    call_slab = pl.pallas_call(
        slab_kernel,
        out_shape=jax.ShapeDtypeStruct((nzl, state_rows, head), BF16),
        in_specs=vmem(4),
        out_specs=pl.BlockSpec(memory_space=pltpu.VMEM),
        interpret=INTERPRET,
        name="slab_state",
    )
    states = call_slab(keys, value, gates, packed)
    states = exchange(states, "zl")
    call_group = pl.pallas_call(
        group_kernel,
        out_shape=jax.ShapeDtypeStruct((nzh, state_rows, head), BF16),
        in_specs=vmem(1),
        out_specs=pl.BlockSpec(memory_space=pltpu.VMEM),
        interpret=INTERPRET,
        name="group",
    )
    groups = call_group(states)
    groups = exchange(groups, "zh")
    call_local = pl.pallas_call(
        local_kernel,
        out_shape=(
            jax.ShapeDtypeStruct((slab, 2 * width), F32),
            jax.ShapeDtypeStruct((nc * length, nx * chan), F32),
            jax.ShapeDtypeStruct((slab, head), BF16),
        ),
        in_specs=[smem] + vmem(5),
        out_specs=vmem(3),
        interpret=INTERPRET,
        name="local",
    )
    local, conv, query = call_local(place, keys, value, gates, packed, conv_kernel)
    call_cell = pl.pallas_call(
        cell_kernel,
        out_shape=jax.ShapeDtypeStruct((nx, nc, ny, length // 4 * 3, 2 * width), BF16),
        in_specs=[smem] + vmem(6),
        out_specs=pl.BlockSpec(memory_space=pltpu.VMEM),
        interpret=INTERPRET,
        name="cell",
    )
    last = call_cell(place, groups, states, query, local, conv, conv_kernel)
    arrived = exchange(last.reshape(nx * nc * ny, length // 4 * 3, -1), ("x", "c", "tp"))
    arrived = arrived.reshape(nx, nc, ny, length // 4 * 3, -1)
    call_assemble = pl.pallas_call(
        assemble_kernel,
        out_shape=jax.ShapeDtypeStruct((ny, nzl, nx, nc, rows, deep), BF16),
        in_specs=[smem] + vmem(2 * nx),
        out_specs=pl.BlockSpec(memory_space=pltpu.VMEM),
        interpret=INTERPRET,
        name="assemble",
    )
    out_weight = call_assemble(place, *out_parts, *other_parts)
    return pl.pallas_call(
        finish_kernel,
        out_shape=jax.ShapeDtypeStruct((length, part), BF16),
        in_specs=vmem(4),
        out_specs=pl.BlockSpec(memory_space=pltpu.VMEM),
        interpret=INTERPRET,
        name="finish",
    )(arrived, out_weight, memory_gain, conv_gain)


def solution(mesh):
    shape = mesh.shape
    depth = shape["sp"] // 32
    split = Mesh(mesh.devices.reshape(4, depth, 4, 2, shape["tp"]), AXES)
    in_specs = (
        P(SP, "tp"),
        P(SP, "tp"),
        P(SP, "tp"),
        P(None, "tp"),
        P("tp"),
        P(SP, "tp"),
        P(SP, "tp"),
        P(SP, "tp"),
        P(None, "tp"),
        P(None, "tp"),
        P(SP, "tp"),
        P(SP, "tp"),
        P("tp"),
        P("tp", SP),
        P("tp", SP),
    )
    return jax.shard_map(
        layer, mesh=split, in_specs=in_specs, out_specs=P(SP, "tp"), check_vma=False
    )
```

```python
import jax
import jax.numpy as jnp
from jax import lax
from jax.experimental import pallas as pl
from jax.experimental.pallas import tpu as pltpu
from jax.sharding import Mesh
from jax.sharding import PartitionSpec as P

AXES = ("zh", "zl", "x", "c", "tp")
Z = ("zh", "zl")
SP = ("zh", "zl", "x", "c")
EPS = 1e-06
LOW = -1e30
F32 = jnp.float32
BF16 = jnp.bfloat16
INTERPRET = False


def size(axis):
    return lax.axis_size(axis)


def exchange(pieces, axes):
    return lax.all_to_all(pieces, axes, split_axis=0, concat_axis=0, tiled=True)


def swapped(value, axis):
    return lax.ppermute(value, axis, [(0, 1), (1, 0)])


def lane_cumsum(rows):
    lane = lax.broadcasted_iota(jnp.int32, rows.shape, 1)
    step = 1
    while step < rows.shape[1]:
        moved = pltpu.roll(rows, step, 1)
        rows = rows + jnp.where(lane >= step, moved, 0.0)
        step *= 2
    return rows


def columns_of(rows):
    count, length = rows.shape
    square = jnp.concatenate([rows, jnp.zeros((length - count, length), F32)], axis=0)
    return square.T


def dot(a, b, dims):
    return lax.dot_general(a, b, (dims, ((), ())), preferred_element_type=F32)


NN = ((1,), (0,))
NT = ((1,), (1,))
TN = ((0,), (0,))


def joined(parts_ref, start, width, chunk, length):
    picked = [
        parts_ref[j, chunk * length : (chunk + 1) * length, start : start + width]
        for j in range(parts_ref.shape[0])
    ]
    return jnp.concatenate(picked, axis=1)


def three_parts(value):
    high = value.astype(BF16).astype(F32)
    mid = (value - high).astype(BF16).astype(F32)
    return high, mid, value - high - mid


def pack_kernel(tokens_ref, offsets_ref, conv_gain_ref, memory_gain_ref, out_ref):
    length = tokens_ref.shape[0]
    offsets = three_parts(offsets_ref[...])
    conv_gain = three_parts(conv_gain_ref[...])
    memory_gain = three_parts(memory_gain_ref[...])
    rows = [jnp.concatenate([p[k : k + 1] for k in range(p.shape[0])], axis=1) for p in offsets]
    rows += memory_gain
    rows.append(jnp.concatenate(conv_gain[:2], axis=1))
    rows.append(jnp.concatenate([conv_gain[2], jnp.zeros_like(conv_gain[2])], axis=1))
    extra = jnp.concatenate(rows, axis=0).astype(BF16)
    tokens = tokens_ref[...]
    for j in range(out_ref.shape[0]):
        out_ref[j, :length] = tokens
        out_ref[j, length:] = extra


def piece_kernel(
    query_ref, key_ref, value_ref, left_ref, right_ref, memory_ref, conv_ref, out_ref, turn_ref
):
    nx, nc = out_ref.shape[0], out_ref.shape[1]
    rows = memory_ref.shape[0]
    whole = jnp.concatenate([memory_ref[...], conv_ref[...]], axis=1)
    wide = out_ref.shape[3]
    for j in range(whole.shape[1] // wide):
        turn_ref[j * rows : (j + 1) * rows] = whole[:, j * wide : (j + 1) * wide]
    for x in range(nx):
        for c in range(nc):
            at = c * nx + x
            parts = []
            for ref in (query_ref, key_ref, value_ref, left_ref, right_ref):
                width = ref.shape[1] // (nx * nc)
                parts.append(ref[:, at * width : (at + 1) * width])
            out_ref[x, c] = jnp.concatenate(parts, axis=1)


def assemble_kernel(place_ref, *refs):
    out_ref = refs[-1]
    nx, ny = out_ref.shape[2], out_ref.shape[0]
    core, column, x_at = place_ref[1], place_ref[2], place_ref[3]
    for ahead in range(nx):
        x = lax.rem(x_at + ahead, nx)
        for c, ref in ((core, refs[ahead]), (1 - core, refs[nx + ahead])):
            for b in range(ny):
                at = lax.rem(column + ny - b, ny)
                for near in range(ref.shape[1]):
                    out_ref[pl.ds(at, 1), near, pl.ds(x, 1), pl.ds(c, 1)] = ref[b, near][
                        None, None, None
                    ]


def project_kernel(
    place_ref, own_ref, other_ref,
    w0_ref, w1_ref, w3_ref, low_ref, high_ref, gate_ref,
    qk_ref, v_ref, glu_ref, gates_ref, memory_gain_ref, conv_gain_ref, out_weight_ref,
):
    nx, ny, _, part = own_ref.shape
    far, tall, wide = w0_ref.shape
    depth, chunks = out_weight_ref.shape[2], out_weight_ref.shape[3] // wide
    rows = tall - depth * chunks
    close = part // rows
    length = glu_ref.shape[1]
    place, core, column = place_ref[0], place_ref[1], place_ref[2]
    tokens_rows = nx * length
    width = qk_ref.shape[4] // 2
    chan = glu_ref.shape[2] // nx
    lane = lax.broadcasted_iota(jnp.int32, (length, width), 1)
    ones = jnp.where(lane == 0, 1.0, 0.0).astype(BF16)
    row = lax.broadcasted_iota(jnp.int32, (2 * nx, length), 0)
    gate_in = jnp.zeros((2 * nx, length), F32)
    forget = jnp.zeros((2 * nx, length), F32)

    members = far * close
    blocks = [
        (ref, i, ahead + close * (i - 1))
        for ref, ahead in ((w0_ref, 0), (w1_ref, 1), (w3_ref, -1))
        for i in range(far)
    ]
    blocks += [(low_ref, i, 2 + close * i) for i in range(far // 2)]
    blocks += [(high_ref, i, -2 + close * (i - 1)) for i in range(far // 2)]
    homes = []
    for ref, i, ahead in blocks:
        home = lax.rem(place + (ahead + members), members)
        y = lax.div(home, close)
        homes.append((y, lax.rem(home, close)))
        behind = lax.rem(y + ny - column, ny)
        out_weight_ref[pl.ds(behind, 1), pl.ds(homes[-1][1], 1)] = jnp.concatenate(
            [ref[i, rows + j * depth : rows + (j + 1) * depth] for j in range(chunks)], axis=1
        )[None, None]
    right = []
    for (w_ref, i, _), (y, z) in zip(blocks, homes):
        start = pl.multiple_of(y * part + z * rows, rows)
        right.append(jnp.concatenate([w_ref[i, :rows], gate_ref[pl.ds(start, rows)]], axis=1))
    right = jnp.concatenate(right, axis=0)
    for half, ref in enumerate((own_ref, other_ref)):
        home = core if half == 0 else 1 - core
        left = []
        for y, z in homes:
            lanes = pl.ds(pl.multiple_of(z * rows, rows), rows)
            left.append(ref[:, pl.ds(y, 1), :length, lanes].reshape(tokens_rows, rows))
        acc = dot(jnp.concatenate(left, axis=1), right, NN)
        pre = acc[:, wide:]
        glu = []
        for x in range(nx):
            mine = acc[x * length : (x + 1) * length]
            qk = mine[:, : 2 * width].astype(BF16)[None]
            for j in range(qk_ref.shape[0]):
                qk_ref[j, x, pl.ds(home, 1)] = qk
            v_ref[x, pl.ds(home, 1)] = jnp.concatenate(
                [mine[:, 2 * width : 3 * width].astype(BF16), ones], axis=1
            )[None]
            left = mine[:, 3 * width : 3 * width + chan]
            gates_side = mine[:, 3 * width + chan : wide]
            glu.append(left / (1.0 + jnp.exp(-gates_side)))
        glu_ref[pl.ds(home, 1)] = jnp.concatenate(glu, axis=1).astype(BF16)[None]
        for x in range(nx):
            turned = pre[x * length : (x + 1) * length].T
            extra = ref[x, column, length : length + 8].astype(F32)
            values = extra[0:1] + extra[1:2] + extra[2:3]
            offsets = jnp.where(core == 0, values[:, :length], values[:, length : 2 * length])
            offsets_f = jnp.where(
                core == 0, values[:, 2 * length : 3 * length], values[:, 3 * length : 4 * length]
            )
            at = row == 2 * x + home
            gate_pre = jnp.where(core == 0, turned[0:1], turned[1:2])
            forget_pre = jnp.where(core == 0, turned[2:3], turned[3:4])
            gate_in = jnp.where(at, gate_pre + offsets, gate_in)
            forget = jnp.where(at, forget_pre + offsets_f, forget)
    for b in range(ny):
        extra = own_ref[0, b, length : length + 8].astype(F32)
        memory_gain_ref[b : b + 1] = extra[3:4] + extra[4:5] + extra[5:6]
        half = part // 2
        conv_gain_ref[b : b + 1] = extra[6:7, :half] + extra[6:7, half:] + extra[7:8, :half]
    y = jnp.exp(-jnp.abs(forget))
    small = y * (1.0 - y * (1 / 2 - y * (1 / 3 - y * (1 / 4 - y * (1 / 5)))))
    gates_ref[0] = gate_in
    gates_ref[1] = jnp.minimum(forget, 0.0) - jnp.where(y < 0.03, small, jnp.log(1.0 + y))


def finish_kernel(arrived_ref, weight_ref, memory_gain_ref, conv_gain_ref, out_ref):
    nx, nc, ny, _, lanes = arrived_ref.shape
    width = lanes // 2
    chan = width // 2
    length, part = out_ref.shape
    half = length // 2
    memory, conv = [], []
    for b in range(ny):
        blocks = [arrived_ref[x, c, b].astype(F32) for c in range(nc) for x in range(nx)]
        upper = jnp.concatenate([got[:half, :width] for got in blocks], axis=1)
        lower = jnp.concatenate([got[:half, width:] for got in blocks], axis=1)
        memory.append(jnp.concatenate([upper, lower], axis=0))
        quarters = [
            jnp.concatenate([got[half:, k * chan : (k + 1) * chan] for got in blocks], axis=1)
            for k in range(4)
        ]
        conv.append(jnp.concatenate(quarters, axis=0))

    def mean_of(arrays):
        each = sum(arrays)
        return jnp.sum(each, axis=1, keepdims=True) / (ny * each.shape[1])

    scale = lax.rsqrt(mean_of([m * m for m in memory]) + EPS)
    mean = mean_of(conv)
    spread = lax.rsqrt(mean_of([t * t for t in conv]) - mean * mean + EPS)
    deep = weight_ref.shape[5]
    total = jnp.zeros((length, part), F32)
    for b in range(ny):
        scaled = memory[b] * scale * memory_gain_ref[b : b + 1]
        normed = (conv[b] - mean) * spread * conv_gain_ref[b : b + 1]
        branch = normed / (1.0 + jnp.exp(-normed))
        both = jnp.concatenate([scaled.astype(BF16), branch.astype(BF16)], axis=1)
        total = total + dot(both, weight_ref[b].reshape(part, deep), NT)
    out_ref[...] = total.astype(BF16)


HOLD = 32


def tap_rows(taps_ref, core, x_at, nx, lanes):
    chan = lanes // nx
    weights = taps_ref[...].astype(F32)
    weights = jnp.where(core == 0, weights[:, :lanes], weights[:, lanes:])
    weights = pltpu.roll(weights, lax.rem(lanes - chan * x_at, lanes), 1)
    weights = jnp.where(lax.broadcasted_iota(jnp.int32, weights.shape, 1) < chan, weights, 0.0)
    return sum(pltpu.roll(weights, chan * k, 1) for k in range(1, nx)) + weights


def convolve(extended, weights):
    taps = weights.shape[0]
    length = extended.shape[0] - HOLD
    total = jnp.zeros((length, extended.shape[1]), F32)
    first = HOLD - (taps - 1)
    for shift in range(8):
        moved = extended[shift : shift + length + HOLD - 8] if shift else extended
        for j in range(taps):
            at = first + j
            if at % 8 == shift:
                total = total + moved[at - shift : at - shift + length] * weights[j : j + 1]
    return total


def with_logs(kept, width, level, total):
    row = lax.broadcasted_iota(jnp.int32, kept.shape, 0)
    lane = lax.broadcasted_iota(jnp.int32, kept.shape, 1)
    for at, value in ((0, level), (3, total)):
        for k, part in enumerate(three_parts(value)):
            kept = jnp.where((row == width + 1) & (lane == at + k), part, kept)
    return kept


def read_logs(block, width):
    line = block[width + 1 : width + 2, :128].astype(F32)
    level = line[:, 0:1] + line[:, 1:2] + line[:, 2:3]
    return level, line[:, 3:4] + line[:, 4:5] + line[:, 5:6]


def merged(blocks, passed, width):
    acc = jnp.zeros((1, 1), F32)
    logs = []
    for block, use in zip(blocks[::-1], passed[::-1]):
        level, total = read_logs(block, width)
        logs.insert(0, jnp.where(use, level + acc, LOW))
        acc = acc + jnp.where(use, total, 0.0)
    level = logs[0]
    for log in logs[1:]:
        level = jnp.maximum(level, log)
    state = jnp.zeros(blocks[0].shape, F32)
    for block, use, log in zip(blocks, passed, logs):
        state = state + jnp.where(use, jnp.exp(log - level), 0.0) * block.astype(F32)
    return state, level, acc


def group_kernel(in_ref, out_ref):
    members, rows, _ = in_ref.shape
    width = rows - 8
    blocks = [in_ref[j] for j in range(members)]
    state, level, total = merged(blocks, [True] * members, width)
    last = blocks[-1].astype(F32)
    kept = jnp.concatenate([state[: width + 2], last[width + 2 :]], axis=0)
    kept = with_logs(kept, width, level, total).astype(BF16)
    for j in range(out_ref.shape[0]):
        out_ref[j] = kept


def slab_kernel(
    qk_ref, v_ref, gate_ref, glu_ref, out_ref,
):
    chunks, length = gate_ref.shape[1], gate_ref.shape[2]
    width = qk_ref.shape[2] // 2
    gate, forget = gate_ref[0], gate_ref[1]
    within = lane_cumsum(forget)
    ends = [within[r : r + 1, length - 1 :] for r in range(chunks)]
    after = [jnp.zeros((1, 1), F32)]
    for r in range(chunks - 1, 0, -1):
        after.insert(0, after[0] + ends[r])
    total = after[0] + ends[0]
    to_end = jnp.concatenate([e + a for e, a in zip(ends, after)], axis=0)
    end_log = to_end - within + gate
    level = jnp.max(jnp.max(end_log, axis=1, keepdims=True), axis=0, keepdims=True)
    fresh = columns_of(jnp.exp(end_log - level))
    state = jnp.zeros((2 * width, width * qk_ref.shape[0]), F32)
    for r in range(chunks):
        key = joined(qk_ref, width, width, r, length)
        scaled = (fresh[:, r : r + 1] * key.astype(F32)).astype(BF16)
        state = state + dot(v_ref[r * length : (r + 1) * length], scaled, TN)
    rows, head_lanes = out_ref.shape[1], out_ref.shape[2]
    kept = state[:rows]
    kept = with_logs(kept, width, level, total)
    chan = glu_ref.shape[2] // qk_ref.shape[0]
    hold = HOLD
    tail = glu_ref[glu_ref.shape[0] - 1, length - hold :].astype(F32)[:, glu_ref.shape[2] - chan :]
    group = head_lanes // chan
    each = hold // group
    tail = jnp.concatenate([tail[g * each : (g + 1) * each] for g in range(group)], axis=1)
    kept = jnp.concatenate([kept[: width + 2], tail, kept[width + 2 + each :]], axis=0)
    kept = kept.astype(BF16)
    for j in range(out_ref.shape[0]):
        out_ref[j] = kept


def local_kernel(place_ref, qk_ref, v_ref, gate_ref, glu_ref, taps_ref, out_ref, conv_ref, q_ref):
    chunks, length = gate_ref.shape[1], gate_ref.shape[2]
    head = q_ref.shape[1]
    lanes = v_ref.shape[1]
    width = lanes // 2
    nx = chunks // glu_ref.shape[0]
    group = glu_ref.shape[0] * glu_ref.shape[1]
    glu = glu_ref[...].reshape(group, lanes).astype(F32)
    lane = lax.broadcasted_iota(jnp.int32, (HOLD, lanes), 1)
    before = pltpu.roll(glu[group - HOLD :], lanes // nx, 1)
    before = jnp.where(lane < lanes // nx, 0.0, before)
    weights = tap_rows(taps_ref, place_ref[1], place_ref[3], nx, lanes)
    conv_ref[...] = convolve(jnp.concatenate([before, glu], axis=0), weights)

    scale = head ** (-0.5)
    gate, forget = gate_ref[0], gate_ref[1]
    within = lane_cumsum(forget)
    turned = columns_of(jnp.concatenate([within, gate], axis=0))
    causal = lax.broadcasted_iota(jnp.int32, (length, length), 0) >= lax.broadcasted_iota(
        jnp.int32, (length, length), 1
    )
    lane = lax.broadcasted_iota(jnp.int32, (length, lanes), 1)
    state = jnp.zeros((lanes, head), F32)
    level = jnp.full((1, 1), LOW, F32)
    passed = jnp.zeros((1, 1), F32)
    for r in range(chunks):
        here = slice(r * length, (r + 1) * length)
        value = v_ref[here]
        query = joined(qk_ref, 0, width, r, length)
        key = joined(qk_ref, width, width, r, length)
        q_ref[here] = query
        within_row, gate_row = within[r : r + 1], gate[r : r + 1]
        within_col = turned[:, r : r + 1]
        gate_col = turned[:, chunks + r : chunks + r + 1]
        log_weight = jnp.where(causal, within_col - within_row + gate_row, -jnp.inf)
        carried = within_col + level
        top = jnp.maximum(carried, jnp.max(log_weight, axis=1, keepdims=True))
        weight = jnp.exp(log_weight - top)
        carried_weight = jnp.exp(carried - top) * scale
        scores = dot(query, key, NT) * (scale * weight)
        numer = dot(scores.astype(BF16), value, NN)
        denom = jnp.sum(scores, axis=1, keepdims=True)
        if r:
            older = dot(query, state.astype(BF16), NT)
            numer = numer + carried_weight * older
            denom = denom + carried_weight * older[:, width : width + 1]
        sent = jnp.where(lane == width, denom, numer)
        sent = jnp.where(lane == width + 1, top, sent)
        out_ref[here] = jnp.where(lane == width + 2, within_col + passed, sent)
        last = within_row[:, length - 1 :]
        passed = passed + last
        end_row = last - within_row + gate_row
        new_level = jnp.maximum(last + level, jnp.max(end_row, axis=1, keepdims=True))
        keep = jnp.exp(last + level - new_level)
        fresh = jnp.exp(last - within_col + gate_col - new_level)
        scaled = (fresh * key.astype(F32)).astype(BF16)
        state = keep * state + dot(value, scaled, TN)
        level = new_level


def cell_kernel(place_ref, far_ref, in_ref, q_ref, local_ref, conv_ref, taps_ref, out_ref):
    members, rows, head = in_ref.shape
    groups = far_ref.shape[0]
    nx, nc, ny, _, lanes = out_ref.shape
    width, chan = lanes // 2, lanes // nx
    length = q_ref.shape[0] // (nx * nc)
    scale = head ** (-0.5)
    place = place_ref[0]
    at_far, at_close = lax.div(place, members), lax.rem(place, members)
    blocks = [far_ref[j] for j in range(groups)] + [in_ref[j] for j in range(members)]
    passed = [j < at_far for j in range(groups)] + [j < at_close for j in range(members)]
    state, level, _ = merged(blocks, passed, width)
    state = jnp.concatenate([state, jnp.zeros((lanes - rows, head), F32)], axis=0).astype(BF16)

    group = head // chan
    each = HOLD // group
    near_rows = in_ref[jnp.maximum(at_close - 1, 0), width : width + 8].astype(F32)
    far_rows = far_ref[jnp.maximum(at_far - 1, 0), width : width + 8].astype(F32)
    last_rows = jnp.where(at_close > 0, near_rows, jnp.where(at_far > 0, far_rows, 0.0))
    last_rows = last_rows[2 : 2 + each]
    prior = jnp.concatenate([last_rows[:, g * chan : (g + 1) * chan] for g in range(group)], axis=0)
    prior = jnp.concatenate([prior, jnp.zeros((HOLD, lanes - chan), F32)], axis=1)
    weights = tap_rows(taps_ref, place_ref[1], place_ref[3], nx, lanes)
    edge = convolve(jnp.concatenate([prior, jnp.zeros((HOLD, lanes), F32)], axis=0), weights)
    half, quarter = length // 2, length // 4
    for r in range(nx * nc):
        here = slice(r * length, (r + 1) * length)
        local = local_ref[here]
        top_here, since = local[:, width + 1 : width + 2], local[:, width + 2 : width + 3]
        carried = since + level
        top = jnp.maximum(carried, top_here)
        local_weight = jnp.exp(top_here - top)
        carried_weight = jnp.exp(carried - top) * scale
        mixed = local_weight * local + carried_weight * dot(q_ref[here], state, NT)
        denom = mixed[:, width : width + 1]
        result = mixed[:, :width] / jnp.maximum(jnp.abs(denom), 1.0)
        x, c = r // nc, r % nc
        memory = jnp.concatenate([result[:half], result[half:]], axis=1)
        branch = []
        for g in range(4):
            at = c * length + g * quarter
            part = conv_ref[at : at + quarter]
            if at == 0:
                part = part + edge
            branch.append(part[:, x * chan : (x + 1) * chan])
        sent = jnp.concatenate([memory, jnp.concatenate(branch, axis=1)], axis=0).astype(BF16)
        for y in range(ny):
            out_ref[x, c, y] = sent


def vmem(count):
    return [pl.BlockSpec(memory_space=pltpu.VMEM)] * count


def layer(
    tokens,
    conv_value_weight,
    conv_gate_weight,
    conv_kernel,
    conv_norm_gain,
    query_weight,
    key_weight,
    value_weight,
    input_gate_weight,
    forget_gate_weight,
    input_offset,
    forget_offset,
    memory_norm_gain,
    conv_out_weight,
    memory_out_weight,
):
    nzh, nzl, nx, nc, ny = (size(a) for a in AXES)
    xi, ci, yi = lax.axis_index("x"), lax.axis_index("c"), lax.axis_index("tp")
    members = nzh * nzl
    zi = lax.axis_index("zh") * nzl + lax.axis_index("zl")
    length, part = tokens.shape
    slab = length * nx * nc
    head = query_weight.shape[1] // nc
    width = head // nx
    chan = conv_value_weight.shape[1] // nc // nx
    rows = query_weight.shape[0]
    wide = 3 * width + 2 * chan

    def from_z(value, ahead):
        return lax.ppermute(value, Z, [(j, (j - ahead) % members) for j in range(members)])

    deep = memory_out_weight.shape[0] + conv_out_weight.shape[0]
    pieces, out_rows = pl.pallas_call(
        piece_kernel,
        out_shape=(
            jax.ShapeDtypeStruct((nx, nc, rows, wide), BF16),
            jax.ShapeDtypeStruct((deep // wide * rows, wide), BF16),
        ),
        in_specs=vmem(7),
        out_specs=vmem(2),
        interpret=INTERPRET,
        name="pieces",
    )(
        query_weight,
        key_weight,
        value_weight,
        conv_value_weight,
        conv_gate_weight,
        memory_out_weight.T,
        conv_out_weight.T,
    )
    offsets = jnp.concatenate([input_offset.T, forget_offset.T], axis=0)
    call_pack = pl.pallas_call(
        pack_kernel,
        out_shape=jax.ShapeDtypeStruct((nx * ny, length + 8, part), BF16),
        in_specs=vmem(4),
        out_specs=pl.BlockSpec(memory_space=pltpu.VMEM),
        interpret=INTERPRET,
        name="pack",
    )
    sent = call_pack(tokens, offsets, conv_norm_gain[None], memory_norm_gain[None])
    mine = exchange(pieces.reshape(nx * nc, rows, wide), ("x", "c"))
    mine = jnp.concatenate([mine.reshape(nx * nc * rows, wide), out_rows], axis=0)
    step = members // 4
    opposite = from_z(mine, 2 * step)
    far = [from_z(mine, -step), mine, from_z(mine, step), opposite]
    own = exchange(sent, ("x", "tp")).reshape(nx, ny, length + 8, part)
    near = jnp.stack(far, axis=0)
    halves = jnp.stack(far[1:3], axis=0), jnp.stack(far[:2], axis=0)
    sets = [near, from_z(near, 1), from_z(near, -1)]
    sets += [from_z(halves[0], 2), from_z(halves[1], -2)]
    other = swapped(own, "c")

    gate_weight = jnp.pad(
        jnp.concatenate([input_gate_weight, forget_gate_weight], axis=1), ((0, 0), (0, 124))
    )
    place = jnp.stack([zi, ci, yi, xi])
    smem = pl.BlockSpec(memory_space=pltpu.SMEM)
    qk, value, packed, gates, memory_gain, conv_gain, out_part = pl.pallas_call(
        project_kernel,
        out_shape=(
            jax.ShapeDtypeStruct((nx, nx, nc, length, 2 * width), BF16),
            jax.ShapeDtypeStruct((nx, nc, length, 2 * width), BF16),
            jax.ShapeDtypeStruct((nc, length, nx * chan), BF16),
            jax.ShapeDtypeStruct((2, nx * nc, length), F32),
            jax.ShapeDtypeStruct((ny, memory_norm_gain.shape[0]), F32),
            jax.ShapeDtypeStruct((ny, conv_norm_gain.shape[0]), F32),
            jax.ShapeDtypeStruct((nzh, nzl, rows, deep), BF16),
        ),
        in_specs=[smem] + vmem(8),
        out_specs=vmem(7),
        interpret=INTERPRET,
        name="project",
    )(place, own, other, *sets, gate_weight)
    value = value.reshape(slab, 2 * width)
    all_qk = exchange(qk.reshape(nx, slab, 2 * width), "x")
    out_part = [out_part[0]] + [
        lax.ppermute(out_part[ahead], "tp", [(j, (j + ahead) % ny) for j in range(ny)])
        for ahead in range(1, ny)
    ]
    out_part = jnp.stack(out_part, axis=0)

    def from_x(value, ahead):
        return lax.ppermute(value, "x", [(j, (j - ahead) % nx) for j in range(nx)])

    out_parts = [out_part, from_x(out_part, 1)]
    from_last = from_x(out_part, 3)
    out_parts += [from_x(out_part, 2), from_last]
    other_parts = [swapped(out, "c") for out in out_parts[:1]]
    other_parts += [swapped(out, "c") for out in out_parts[1:]]

    state_rows = width + 8
    keys = all_qk.reshape(nx, slab, 2 * width)
    call_slab = pl.pallas_call(
        slab_kernel,
        out_shape=jax.ShapeDtypeStruct((nzl, state_rows, head), BF16),
        in_specs=vmem(4),
        out_specs=pl.BlockSpec(memory_space=pltpu.VMEM),
        interpret=INTERPRET,
        name="slab_state",
    )
    states = call_slab(keys, value, gates, packed)
    states = exchange(states, "zl")
    call_group = pl.pallas_call(
        group_kernel,
        out_shape=jax.ShapeDtypeStruct((nzh, state_rows, head), BF16),
        in_specs=vmem(1),
        out_specs=pl.BlockSpec(memory_space=pltpu.VMEM),
        interpret=INTERPRET,
        name="group",
    )
    groups = call_group(states)
    groups = exchange(groups, "zh")
    call_local = pl.pallas_call(
        local_kernel,
        out_shape=(
            jax.ShapeDtypeStruct((slab, 2 * width), F32),
            jax.ShapeDtypeStruct((nc * length, nx * chan), F32),
            jax.ShapeDtypeStruct((slab, head), BF16),
        ),
        in_specs=[smem] + vmem(5),
        out_specs=vmem(3),
        interpret=INTERPRET,
        name="local",
    )
    local, conv, query = call_local(place, keys, value, gates, packed, conv_kernel)
    call_cell = pl.pallas_call(
        cell_kernel,
        out_shape=jax.ShapeDtypeStruct((nx, nc, ny, length // 4 * 3, 2 * width), BF16),
        in_specs=[smem] + vmem(6),
        out_specs=pl.BlockSpec(memory_space=pltpu.VMEM),
        interpret=INTERPRET,
        name="cell",
    )
    last = call_cell(place, groups, states, query, local, conv, conv_kernel)
    arrived = exchange(last.reshape(nx * nc * ny, length // 4 * 3, -1), ("x", "c", "tp"))
    arrived = arrived.reshape(nx, nc, ny, length // 4 * 3, -1)
    call_assemble = pl.pallas_call(
        assemble_kernel,
        out_shape=jax.ShapeDtypeStruct((ny, nzl, nx, nc, rows, deep), BF16),
        in_specs=[smem] + vmem(2 * nx),
        out_specs=pl.BlockSpec(memory_space=pltpu.VMEM),
        interpret=INTERPRET,
        name="assemble",
    )
    out_weight = call_assemble(place, *out_parts, *other_parts)
    return pl.pallas_call(
        finish_kernel,
        out_shape=jax.ShapeDtypeStruct((length, part), BF16),
        in_specs=vmem(4),
        out_specs=pl.BlockSpec(memory_space=pltpu.VMEM),
        interpret=INTERPRET,
        name="finish",
    )(arrived, out_weight, memory_gain, conv_gain)


def solution(mesh):
    shape = mesh.shape
    depth = shape["sp"] // 32
    split = Mesh(mesh.devices.reshape(4, depth, 4, 2, shape["tp"]), AXES)
    in_specs = (
        P(SP, "tp"),
        P(SP, "tp"),
        P(SP, "tp"),
        P(None, "tp"),
        P("tp"),
        P(SP, "tp"),
        P(SP, "tp"),
        P(SP, "tp"),
        P(None, "tp"),
        P(None, "tp"),
        P(SP, "tp"),
        P(SP, "tp"),
        P("tp"),
        P("tp", SP),
        P("tp", SP),
    )
    return jax.shard_map(
        layer, mesh=split, in_specs=in_specs, out_specs=P(SP, "tp"), check_vma=False
    )
```
